256 devices in a mesh: kv: 32 (over z, x), tp: 8 (over y, core).
Axes of the slice: x: 4, y: 4, z: 8, core: 2. Of those that a mesh axis runs over, the one named last changes fastest.
Arguments:
- inputs: bfloat16 [8192, 2048], P('kv', 'tp'), may hold values from -6 to 6
- queries: bfloat16 [8192, 2048], P('kv', 'tp'), may hold values from -8 to 8
- key_vectors: bfloat16 [8192, 512], P('kv', 'tp'), may hold values from -8 to 8
- value_rows_by_head: bfloat16 [8192, 512], P('kv', 'tp'), may hold values from -6 to 6
- out_grad: bfloat16 [8192, 2048], P('kv', 'tp'), may hold values from -6 to 6
- chosen: int32 [64, 16], replicated, may hold values from 0 to 127, as said below
Outputs:
- query_grad: bfloat16 [8192, 2048], P('kv', 'tp')
- key_grad: bfloat16 [8192, 512], P('kv', 'tp')
- value_grad: bfloat16 [8192, 512], P('kv', 'tp')
- weight_grad: float32 [2048, 2048], P('kv', 'tp')
The draws below stay inside these ranges and needn't reach their ends.
Inputs may be any that keep to these rules, and one draw needn't show every extreme that they name: `chosen`: row r holds 16 distinct key-block numbers, among them every key block that intersects query block r. The rows of one device (aligned runs of 2 rows) name at most 2 distinct key blocks that lie on any one other device (aligned runs of 4 key blocks), and exactly 2 at some other device for some devices.
All inputs are finite; a program needn't handle non-finite values.
Results may differ from the reference program's by a relative error of at most 0.015.
The reference program's roundings to bfloat16 on the way (of `probs_half` and `score_grad`) count: a program that leaves them out, or rounds other values in their place, can miss the bound.
Values may be sent and summed in bfloat16 or wider, within the bound.
A program may use at most 128 MiB of HBM per device.

```python
import jax
import jax.numpy as jnp
from jax import lax

D = 2048
QUERY_HEADS = 32
KEY_VALUE_HEADS = 8
HEAD_SIZE = 64
QB = 128
KB = 64
NSEL = 16
TOK_DEV = 256
SEQUENCE_TOKENS = 8192


def draw_queries(key, part):
    final_result = jnp.clip(jax.random.normal(jax.random.fold_in(key, 1), (SEQUENCE_TOKENS, QUERY_HEADS * HEAD_SIZE), jnp.float32), -6.0, 6.0)
    return final_result.astype(jnp.bfloat16)


def draw_key_vectors(key, part):
    final_result = jnp.clip(jax.random.normal(jax.random.fold_in(key, 2), (SEQUENCE_TOKENS, KEY_VALUE_HEADS * HEAD_SIZE), jnp.float32), -6.0, 6.0)
    return final_result.astype(jnp.bfloat16)


def draw_chosen(key, part):
    q_count = SEQUENCE_TOKENS // QB
    k_count = SEQUENCE_TOKENS // KB
    ratio = QB // KB
    owner_blocks = TOK_DEV // KB
    local_blocks = TOK_DEV // QB
    n_dev = SEQUENCE_TOKENS // TOK_DEV
    q_index = jnp.arange(q_count, dtype=jnp.int32)[:, None]
    k_index = jnp.arange(k_count, dtype=jnp.int32)[None, :]
    dev_grid = jnp.arange(n_dev, dtype=jnp.int32)[:, None]
    own_grid = jnp.arange(n_dev, dtype=jnp.int32)[None, :]
    random_phase = jax.random.randint(jax.random.fold_in(key, 7), (n_dev, n_dev), 0, ratio)
    phase = jnp.where(own_grid == (dev_grid - 1) % n_dev, ratio - 1, jnp.where(own_grid == (dev_grid - n_dev // 2) % n_dev, 0, random_phase))
    query_dev = q_index // local_blocks
    key_owner = k_index // owner_blocks
    key_offset = k_index % owner_blocks
    permitted = (key_owner == query_dev) | (key_offset % ratio == phase[query_dev, key_owner])
    own_block = k_index // ratio == q_index
    forced = (k_index == q_index * ratio - 1) | (k_index == q_index * ratio - k_count // 2)
    causal = k_index < q_index * ratio
    tier = jnp.where(own_block, 3, jnp.where(forced, 2, jnp.where(causal, 1, 0)))
    tier = jnp.where(permitted, tier, -1)
    popular = jax.random.randint(jax.random.fold_in(key, 5), (k_count,), 0, 2) * 7
    row_keys = jax.random.split(jax.random.fold_in(key, 6), q_count)
    noise = jax.vmap(lambda one_key: jax.random.permutation(one_key, k_count))(row_keys)
    ranking = tier * (k_count * 8) + popular[None, :] * k_count + noise
    _, picked = lax.top_k(ranking, NSEL)
    return picked.astype(jnp.int32)


def levels(rng, dims, shards, least, largest):
    loudness = 1.0
    for dim, parts in shards:
        draws = jax.random.uniform(jax.random.fold_in(jax.random.fold_in(rng, 6), dim), (parts,), jnp.float32, least / len(shards), largest / len(shards))
        loudness = loudness * jnp.repeat(jnp.exp(draws), dims[dim] // parts).reshape((-1,) + (1,) * (len(dims) - 1 - dim))
    return loudness


def centred(stream_key, dims, deviation, limit, shards=(), kind=jnp.bfloat16):
    level = levels(stream_key, dims, shards, -0.22, 0.18) if shards else 1.0
    entries = jax.random.normal(stream_key, dims, jnp.float32) * deviation * level
    return jnp.minimum(jnp.maximum(entries, -limit), limit).astype(kind)


def setup_inputs(seed: int = 0) -> dict:
    streams_of = jax.random.split(jax.random.key(seed), 7)
    inputs = centred(streams_of[0], (SEQUENCE_TOKENS, D), 1.0, 6.0, ((0, 32), (1, 8)))
    queries = draw_queries(jax.random.fold_in(streams_of[6], 71), 0)
    key_vectors = draw_key_vectors(jax.random.fold_in(streams_of[6], 71), 0)
    value_rows_by_head = centred(streams_of[3], (SEQUENCE_TOKENS, KEY_VALUE_HEADS * HEAD_SIZE), 1.0, 6.0, ((0, 32), (1, 8)))
    out_grad = centred(streams_of[4], (SEQUENCE_TOKENS, QUERY_HEADS * HEAD_SIZE), 1.0, 6.0, ((0, 32), (1, 8)))
    chosen = draw_chosen(jax.random.fold_in(streams_of[6], 71), 0)
    return dict(inputs=inputs, queries=queries, key_vectors=key_vectors, value_rows_by_head=value_rows_by_head, out_grad=out_grad, chosen=chosen)


def round_trip(values_in):
    halved = lax.optimization_barrier(values_in.astype(jnp.bfloat16))
    return halved.astype(jnp.float32)


def reference(inputs, queries, key_vectors, value_rows_by_head, out_grad, chosen):
    total = queries.shape[0]
    q_heads = queries.shape[1] // HEAD_SIZE
    kv_heads = key_vectors.shape[1] // HEAD_SIZE
    group_size = q_heads // kv_heads
    score_scale = HEAD_SIZE ** -0.5
    offsets = jnp.arange(KB, dtype=jnp.int32)

    def step(state_pair, q_blk):
        acc_k, acc_v = state_pair
        first = q_blk * QB
        q_block = lax.dynamic_slice_in_dim(queries, first, QB, 0).astype(jnp.float32).reshape(QB, kv_heads, group_size, HEAD_SIZE)
        g_block = lax.dynamic_slice_in_dim(out_grad, first, QB, 0).astype(jnp.float32).reshape(QB, kv_heads, group_size, HEAD_SIZE)
        key_rows = (chosen[q_blk][:, None] * KB + offsets[None, :]).reshape(-1).astype(jnp.int32)
        key_sel = key_vectors[key_rows].astype(jnp.float32).reshape(-1, kv_heads, HEAD_SIZE)
        val_sel = value_rows_by_head[key_rows].astype(jnp.float32).reshape(-1, kv_heads, HEAD_SIZE)
        positions = first + jnp.arange(QB, dtype=jnp.int32)
        allowed = key_rows[None, :] <= positions[:, None]
        scores = jnp.einsum('tkgd,skd->kgts', q_block, key_sel) * score_scale
        scores = jnp.where(allowed, scores, -1e30)
        row_max = jnp.max(scores, axis=-1, keepdims=True)
        log_sum = row_max + jnp.log(jnp.sum(jnp.exp(scores - row_max), axis=-1, keepdims=True))
        probs = jnp.exp(scores - log_sum)
        probs_half = round_trip(probs)
        attended = jnp.einsum('kgts,skd->tkgd', probs_half, val_sel)
        row_dot = jnp.einsum('tkgd,tkgd->kgt', g_block, attended)
        prob_grad = jnp.einsum('tkgd,skd->kgts', g_block, val_sel)
        score_grad = round_trip(probs * (prob_grad - row_dot[..., None]))
        d_query = jnp.einsum('kgts,skd->tkgd', score_grad, key_sel) * score_scale
        d_key = jnp.einsum('kgts,tkgd->skd', score_grad, q_block) * score_scale
        d_value = jnp.einsum('kgts,tkgd->skd', probs_half, g_block)
        acc_k = acc_k.at[key_rows].add(d_key.reshape(-1, kv_heads * HEAD_SIZE))
        acc_v = acc_v.at[key_rows].add(d_value.reshape(-1, kv_heads * HEAD_SIZE))
        return (acc_k, acc_v), d_query.reshape(QB, q_heads * HEAD_SIZE)

    zeros = jnp.zeros((total, kv_heads * HEAD_SIZE), jnp.float32)
    (acc_k, acc_v), query_blocks = lax.scan(step, (zeros, zeros), jnp.arange(total // QB, dtype=jnp.int32))
    query_grad = query_blocks.reshape(total, q_heads * HEAD_SIZE).astype(jnp.bfloat16)
    weight_grad = jnp.dot(inputs.T, query_grad, preferred_element_type=jnp.float32)
    return query_grad, acc_k.astype(jnp.bfloat16), acc_v.astype(jnp.bfloat16), weight_grad
```

```python
import functools

import jax
import jax.numpy as jnp
from jax import lax
from jax.experimental import pallas as pl
from jax.experimental.pallas import tpu as pltpu
from jax.sharding import PartitionSpec as P

HEAD = 64
QB = 128
KB = 64
NSEL = 16
Z, X, TP = 8, 4, 8
TOK = 256
GROUP = 4
SCALE = HEAD**-0.5
ORDER = (0, 1, 7, 2, 6, 3, 5, 4)
PLACE = {d: p for p, d in enumerate(ORDER)}
NEG = -1e30
MESH = pl.DeviceIdType.MESH
F32, BF16 = jnp.float32, jnp.bfloat16
ZERO_D = 2 * NSEL
T_LOC, T_BLK, T_FWD, T_SEND, T_OWN, T_RECV, T_END = 0, 32, 64, 112, 208, 272, 368


def place_of(distance):
    return jnp.where(
        distance == 0,
        0,
        jnp.where(distance < 4, 2 * distance - 1, jnp.where(distance == 4, 7, 2 * (8 - distance))),
    )


def index_table(chosen):
    kv = lax.axis_index("kv")
    z, x = kv // X, kv % X
    rows = lax.dynamic_slice_in_dim(chosen, z * 2 * X, 2 * X, 0).reshape(X, 2 * NSEL)
    by_dx = lax.dynamic_slice_in_dim(jnp.concatenate([rows, rows], 0), x, X, 0)
    own = by_dx[0]
    owner, off = own // 4, own % 4
    zr, dx = (owner // X - z) % Z, (owner % X - x) % X
    p = place_of(zr)
    smaller = jnp.any((owner[:, None] == owner[None, :]) & (off[None, :] < off[:, None]), axis=1)
    loc = jnp.where(dx == 0, p * 4 + off, 32 + ((dx - 1) * Z + p) * 2 + smaller.astype(jnp.int32))
    order = (jnp.arange(Z) + 1) // 2
    order = jnp.where(jnp.arange(Z) % 2 == 1, order, Z - order) % Z
    order = jnp.where(jnp.arange(Z) == 7, 4, order)
    zs = (z + order) % Z
    rel = by_dx[1:, None, :] - (zs * 16 + x * 4)[None, :, None]
    ok = (rel >= 0) & (rel < 4)
    o0 = jnp.min(jnp.where(ok, rel, 3), axis=2)
    o1 = jnp.max(jnp.where(ok, rel, 0), axis=2)
    fwd = jnp.stack([o0, o1], 2)
    base = zs[None, :] * 16 + ((x + jnp.arange(1, X)) % X)[:, None] * 4
    rel = own[None, None, :] - base[:, :, None]
    ok = (rel >= 0) & (rel < 4)
    m0 = jnp.min(jnp.where(ok, rel, 3), axis=2)
    m1 = jnp.max(jnp.where(ok, rel, 0), axis=2)
    send_blk = base[:, :, None] + jnp.stack([m0, m1], 2)
    own_blk = (zs * 16 + x * 4)[:, None] + jnp.arange(4)[None, :]
    blks = jnp.concatenate([send_blk.reshape(-1), own_blk.reshape(-1)])
    hit = blks[:, None] == own[None, :]
    js = jnp.where(hit, jnp.arange(2 * NSEL)[None, :], ZERO_D).reshape(-1, 2, NSEL)
    inverse = jnp.min(js, axis=2).reshape(-1)
    o = jnp.arange(4)[None, None, :]
    recv = jnp.where(o == o0[:, :, None], 0, jnp.where(o == o1[:, :, None], 1, 2))
    parts = [loc, own, fwd.reshape(-1), inverse, recv.reshape(-1)]
    return jnp.concatenate([part.astype(jnp.int32) for part in parts])


def kernel(
    tab, in_ref, q_ref, k_ref, v_ref, g_ref,
    dq_out, dk_out, dv_out, w_out,
    kvt, xsel, in_t, xt, at, kvs, qp, gp, s_scr, pg_scr, p_scr, ds_scr,
    dsel, dxs, rbuf, acc, zs_send, zr_buf, dqg, wp, w_send, w_recv,
    z_ss, z_rs, x_ss, x_rs, i_ss, i_rs, y_ss, y_rs, dq_ss, dq_rs, dx_ss, dx_rs, w_ss, w_rs, dz_ss, dz_rs,
):
    kv, tp = lax.axis_index("kv"), lax.axis_index("tp")
    z, x = kv // X, kv % X

    def at_z(d):
        return (lax.rem(z + d, Z) * X + x, tp)

    def at_x(d):
        return (z * X + lax.rem(x + d, X), tp)

    def at_tp(d):
        return (kv, lax.rem(tp + d, TP))

    def remote(src, dst, ss, rs, dev):
        return pltpu.make_async_remote_copy(
            src_ref=src, dst_ref=dst, send_sem=ss, recv_sem=rs, device_id=dev, device_id_type=MESH
        )

    sent = []
    barrier = pltpu.get_barrier_semaphore()
    peers = [at_z(d) for d in range(1, Z)] + [at_x(d) for d in range(1, X)] + [at_tp(d) for d in range(1, TP)]
    for dev in peers:
        pl.semaphore_signal(barrier, inc=1, device_id=dev, device_id_type=MESH)
    kvt[0:4] = jnp.concatenate([k_ref[...], v_ref[...]], axis=1).reshape(4, KB, 128)
    in_t[...] = in_ref[...].T.reshape(X, HEAD, TOK)
    dsel[ZERO_D] = jnp.zeros((KB, 128), F32)
    pl.semaphore_wait(barrier, len(peers))

    zc = []
    for p in range(1, Z):
        there = PLACE[(Z - ORDER[p]) % Z]
        c = remote(kvt.at[pl.ds(0, 4)], kvt.at[pl.ds(4 * there, 4)], z_ss.at[p], z_rs.at[there], at_z(ORDER[p]))
        c.start()
        zc.append(c)
        sent.append(c)
    ic = []
    for d in range(1, X):
        col = lax.rem(x + d, X)
        c = remote(in_t.at[col], xt.at[:, pl.ds((X - d) * TOK, TOK)], i_ss.at[d], i_rs.at[X - d], at_x(d))
        c.start()
        ic.append(c)
        sent.append(c)
    xt[:, 0:TOK] = in_t[x]

    xc = []
    yc = []
    for p in range(Z):
        if p > 0:
            zin = remote(kvt.at[pl.ds(0, 4)], kvt.at[pl.ds(4 * p, 4)], z_ss.at[p], z_rs.at[p], at_z(ORDER[p]))
            zin.wait_recv()
        four = [kvt[4 * p + o] for o in range(4)]
        for d in range(1, X):
            for s in range(2):
                n = ((d - 1) * Z + p) * 2 + s
                o = tab[T_FWD + n]
                low = jnp.where(o == 0, four[0], four[1])
                high = jnp.where(o == 2, four[2], four[3])
                xsel[n] = jnp.where(o < 2, low, high)
        for d in range(1, X):
            mine, there = ((d - 1) * Z + p) * 2, 32 + ((X - d - 1) * Z + p) * 2
            c = remote(
                xsel.at[pl.ds(mine, 2)], kvt.at[pl.ds(there, 2)],
                x_ss.at[(d - 1) * Z + p], x_rs.at[(X - d - 1) * Z + p], at_x(d),
            )
            c.start()
            xc.append(c)
            sent.append(c)
        if p == 1:
            for c in ic:
                c.wait_recv()
            for d in range(1, TP):
                c = remote(xt, at.at[tp], y_ss.at[d], y_rs.at[TP - d], at_tp(d))
                c.start()
                yc.append(c)
                sent.append(c)
            at[tp] = xt[...]
    for c in xc:
        c.wait_recv()

    lane_t = lax.broadcasted_iota(jnp.int32, (KB, GROUP * QB), 1) % QB
    diff = lax.broadcasted_iota(jnp.int32, (KB, GROUP * QB), 0) - lane_t
    zeros = jnp.zeros((QB, HEAD), BF16)
    nt = (((1,), (1,)), ((), ()))
    nn = (((1,), (0,)), ((), ()))

    def fold(t, op):
        return op(t.reshape(8, 8, GROUP * QB), axis=0)

    for r in range(2):
        rows = pl.ds(r * QB, QB)
        for h in range(GROUP):
            cols = slice(h * HEAD, (h + 1) * HEAD)
            qp[h * QB : (h + 1) * QB, :] = jnp.concatenate([q_ref[rows, cols], zeros], axis=1)
            gp[h * QB : (h + 1) * QB, :] = jnp.concatenate([zeros, g_ref[rows, cols]], axis=1)
        for j in range(NSEL):
            kvs[j * KB : (j + 1) * KB, :] = kvt[tab[T_LOC + r * NSEL + j]]
        s_scr[...] = lax.dot_general(kvs[...], qp[...], nt, preferred_element_type=F32)
        pg_scr[...] = lax.dot_general(kvs[...], gp[...], nt, preferred_element_type=F32)

        def mask_step(j, m):
            at_j = pl.ds(pl.multiple_of(j * KB, KB), KB)
            limit = kv * TOK + r * QB - tab[T_BLK + r * NSEL + j] * KB
            s = jnp.where(diff <= limit, s_scr[at_j, :] * SCALE, NEG)
            s_scr[at_j, :] = s
            return jnp.maximum(m, fold(s, jnp.max))

        m = lax.fori_loop(0, NSEL, mask_step, jnp.full((8, GROUP * QB), NEG, F32))
        m = jnp.max(m, axis=0, keepdims=True)

        def exp_step(j, total):
            at_j = pl.ds(pl.multiple_of(j * KB, KB), KB)
            e = jnp.exp(s_scr[at_j, :] - m)
            s_scr[at_j, :] = e
            return total + fold(e, jnp.sum)

        total = lax.fori_loop(0, NSEL, exp_step, jnp.zeros((8, GROUP * QB), F32))
        inv = 1.0 / jnp.sum(total, axis=0, keepdims=True)

        def half_step(j, dot):
            at_j = pl.ds(pl.multiple_of(j * KB, KB), KB)
            half = (s_scr[at_j, :] * inv).astype(BF16)
            p_scr[at_j, :] = half
            return dot + fold(half.astype(F32) * pg_scr[at_j, :], jnp.sum)

        dot = lax.fori_loop(0, NSEL, half_step, jnp.zeros((8, GROUP * QB), F32))
        dot = jnp.sum(dot, axis=0, keepdims=True)

        def grad_step(j, carry):
            at_j = pl.ds(pl.multiple_of(j * KB, KB), KB)
            ds_scr[at_j, :] = ((s_scr[at_j, :] * inv) * (pg_scr[at_j, :] - dot)).astype(BF16)
            return carry

        lax.fori_loop(0, NSEL, grad_step, 0)
        dq_t = lax.dot_general(kvs[...].T[:HEAD], ds_scr[...], nn, preferred_element_type=F32) * SCALE
        stacked = jnp.concatenate([dq_t[:, h * QB : (h + 1) * QB] for h in range(GROUP)], axis=0)
        dqg[rows, :] = stacked.T.astype(BF16)
        dkv = lax.dot_general(ds_scr[...], qp[...], nn, preferred_element_type=F32)
        dkv += lax.dot_general(p_scr[...], gp[...], nn, preferred_element_type=F32)
        dsel[pl.ds(r * NSEL, NSEL)] = dkv.reshape(NSEL, KB, 128)
        for d in range(1, X):
            c = remote(
                dqg.at[rows], dqg.at[pl.ds((X - d) * TOK + r * QB, QB)],
                dq_ss.at[r * X + d], dq_rs.at[r * X + X - d], at_x(d),
            )
            c.start()
            sent.append(c)
    dq_out[...] = dqg[0:TOK, :]

    for p in reversed(range(Z)):
        for d in range(1, X):
            for s in range(2):
                n = ((d - 1) * Z + p) * 2 + s
                dxs[n] = (dsel[tab[T_SEND + 2 * n]] + dsel[tab[T_SEND + 2 * n + 1]]).astype(BF16)
        for d in range(1, X):
            mine, there = (d - 1) * Z + p, (X - d - 1) * Z + p
            c = remote(
                dxs.at[pl.ds(2 * mine, 2)], rbuf.at[pl.ds(2 * there, 2)],
                dx_ss.at[mine], dx_rs.at[there], at_x(d),
            )
            c.start()
            sent.append(c)

    for c in yc:
        c.wait_recv()
    for r in range(2):
        for d in range(1, X):
            src = dqg.at[pl.ds(r * QB, QB)]
            dst = dqg.at[pl.ds(d * TOK + r * QB, QB)]
            remote(src, dst, dq_ss.at[r * X + d], dq_rs.at[r * X + d], at_x(d)).wait_recv()
    wp[...] = lax.dot_general(
        at[...].reshape(TP * HEAD, X * TOK), dqg[...], nn, preferred_element_type=F32
    ).reshape(TP, HEAD, TOK)
    w_send[...] = wp[...].astype(BF16)
    wc = []
    for p in reversed(range(1, Z)):
        there = PLACE[(Z - ORDER[p]) % Z]
        c = remote(w_send.at[lax.rem(z + ORDER[p], Z)], w_recv.at[there], w_ss.at[p], w_rs.at[there], at_z(ORDER[p]))
        c.start()
        wc.append(c)
        sent.append(c)

    dzc = []
    for p in reversed(range(Z)):
        for d in range(1, X):
            mine = (d - 1) * Z + p
            remote(
                dxs.at[pl.ds(2 * mine, 2)], rbuf.at[pl.ds(2 * mine, 2)],
                dx_ss.at[mine], dx_rs.at[mine], at_x(d),
            ).wait_recv()
        for o in range(4):
            n = T_OWN + (p * 4 + o) * 2
            term = dsel[tab[n]] + dsel[tab[n + 1]]
            for d in range(1, X):
                mine = (d - 1) * Z + p
                which = tab[T_RECV + mine * 4 + o]
                slot = jnp.where(which == 0, rbuf[2 * mine], rbuf[2 * mine + 1])
                term += jnp.where(which < 2, slot.astype(F32), 0.0)
            if p > 0:
                zs_send[p * 4 + o] = term.astype(BF16)
            else:
                acc[o] = term
        if p > 0:
            there = PLACE[(Z - ORDER[p]) % Z]
            c = remote(
                zs_send.at[pl.ds(4 * p, 4)], zr_buf.at[pl.ds(4 * there, 4)],
                dz_ss.at[p], dz_rs.at[there], at_z(ORDER[p]),
            )
            c.start()
            dzc.append(c)
            sent.append(c)
    for c in wc:
        c.wait_recv()
    w = wp[z]
    for p in range(1, Z):
        w += w_recv[p].astype(F32)
    w_out[...] = w
    for c in dzc:
        c.wait_recv()
    both = acc[...]
    for p in range(1, Z):
        both += zr_buf[4 * p : 4 * p + 4].astype(F32)
    both = both.reshape(TOK, 128)
    dk_out[...] = (both[:, :HEAD] * SCALE).astype(BF16)
    dv_out[...] = both[:, HEAD:].astype(BF16)
    for c in sent:
        c.wait_send()


def body(inputs, queries, key_vectors, value_rows_by_head, out_grad, chosen):
    tab = index_table(chosen)
    dma = pltpu.SemaphoreType.DMA
    vmem = pl.BlockSpec(memory_space=pltpu.VMEM)
    dq, dk, dv, w = pl.pallas_call(
        kernel,
        out_shape=(
            jax.ShapeDtypeStruct((TOK, GROUP * HEAD), BF16),
            jax.ShapeDtypeStruct((TOK, HEAD), BF16),
            jax.ShapeDtypeStruct((TOK, HEAD), BF16),
            jax.ShapeDtypeStruct((HEAD, GROUP * HEAD), F32),
        ),
        in_specs=[pl.BlockSpec(memory_space=pltpu.SMEM)] + [vmem] * 5,
        out_specs=(vmem,) * 4,
        scratch_shapes=[
            pltpu.VMEM((32 + 48, KB, 128), BF16),
            pltpu.VMEM((48, KB, 128), BF16),
            pltpu.VMEM((X, HEAD, TOK), BF16),
            pltpu.VMEM((HEAD, X * TOK), BF16),
            pltpu.VMEM((TP, HEAD, X * TOK), BF16),
            pltpu.VMEM((NSEL * KB, 128), BF16),
            pltpu.VMEM((GROUP * QB, 128), BF16),
            pltpu.VMEM((GROUP * QB, 128), BF16),
            pltpu.VMEM((NSEL * KB, GROUP * QB), F32),
            pltpu.VMEM((NSEL * KB, GROUP * QB), F32),
            pltpu.VMEM((NSEL * KB, GROUP * QB), BF16),
            pltpu.VMEM((NSEL * KB, GROUP * QB), BF16),
            pltpu.VMEM((2 * NSEL + 1, KB, 128), F32),
            pltpu.VMEM((48, KB, 128), BF16),
            pltpu.VMEM((48, KB, 128), BF16),
            pltpu.VMEM((4, KB, 128), F32),
            pltpu.VMEM((32, KB, 128), BF16),
            pltpu.VMEM((32, KB, 128), BF16),
            pltpu.VMEM((X * TOK, GROUP * HEAD), BF16),
            pltpu.VMEM((TP, HEAD, TOK), F32),
            pltpu.VMEM((TP, HEAD, TOK), BF16),
            pltpu.VMEM((Z, HEAD, TOK), BF16),
            dma((Z,)), dma((Z,)),
            dma((24,)), dma((24,)),
            dma((X,)), dma((X,)),
            dma((TP,)), dma((TP,)),
            dma((2 * X,)), dma((2 * X,)),
            dma((24,)), dma((24,)),
            dma((Z,)), dma((Z,)),
            dma((Z,)), dma((Z,)),
        ],
        compiler_params=pltpu.CompilerParams(
            collective_id=0, has_side_effects=True, vmem_limit_bytes=60000 * 1024
        ),
        name="fused_backward",
    )(tab, inputs, queries, key_vectors, value_rows_by_head, out_grad)
    return dq, dk, dv, w


def solution(mesh):
    spec = P("kv", "tp")
    return jax.shard_map(
        body, mesh=mesh, in_specs=(spec,) * 5 + (P(),), out_specs=(spec,) * 4, check_vma=False
    )
```

```python
import functools

import jax
import jax.numpy as jnp
from jax import lax
from jax.experimental import pallas as pl
from jax.experimental.pallas import tpu as pltpu
from jax.sharding import PartitionSpec as P

HEAD = 64
QB = 128
KB = 64
NSEL = 16
Z, X, TP = 8, 4, 8
TOK = 256
GROUP = 4
SCALE = HEAD**-0.5
ORDER = (0, 1, 7, 2, 6, 3, 5, 4)
PLACE = {d: p for p, d in enumerate(ORDER)}
NEG = -1e30
MESH = pl.DeviceIdType.MESH
F32, BF16 = jnp.float32, jnp.bfloat16
ZERO_D = 2 * NSEL
T_LOC, T_BLK, T_FWD, T_SEND, T_OWN, T_RECV, T_END = 0, 32, 64, 112, 208, 272, 368


def place_of(distance):
    return jnp.where(
        distance == 0,
        0,
        jnp.where(distance < 4, 2 * distance - 1, jnp.where(distance == 4, 7, 2 * (8 - distance))),
    )


def index_table(chosen):
    kv = lax.axis_index("kv")
    z, x = kv // X, kv % X
    rows = lax.dynamic_slice_in_dim(chosen, z * 2 * X, 2 * X, 0).reshape(X, 2 * NSEL)
    by_dx = lax.dynamic_slice_in_dim(jnp.concatenate([rows, rows], 0), x, X, 0)
    own = by_dx[0]
    owner, off = own // 4, own % 4
    zr, dx = (owner // X - z) % Z, (owner % X - x) % X
    p = place_of(zr)
    smaller = jnp.any((owner[:, None] == owner[None, :]) & (off[None, :] < off[:, None]), axis=1)
    loc = jnp.where(dx == 0, p * 4 + off, 32 + ((dx - 1) * Z + p) * 2 + smaller.astype(jnp.int32))
    order = (jnp.arange(Z) + 1) // 2
    order = jnp.where(jnp.arange(Z) % 2 == 1, order, Z - order) % Z
    order = jnp.where(jnp.arange(Z) == 7, 4, order)
    zs = (z + order) % Z
    rel = by_dx[1:, None, :] - (zs * 16 + x * 4)[None, :, None]
    ok = (rel >= 0) & (rel < 4)
    o0 = jnp.min(jnp.where(ok, rel, 3), axis=2)
    o1 = jnp.max(jnp.where(ok, rel, 0), axis=2)
    fwd = jnp.stack([o0, o1], 2)
    base = zs[None, :] * 16 + ((x + jnp.arange(1, X)) % X)[:, None] * 4
    rel = own[None, None, :] - base[:, :, None]
    ok = (rel >= 0) & (rel < 4)
    m0 = jnp.min(jnp.where(ok, rel, 3), axis=2)
    m1 = jnp.max(jnp.where(ok, rel, 0), axis=2)
    send_blk = base[:, :, None] + jnp.stack([m0, m1], 2)
    own_blk = (zs * 16 + x * 4)[:, None] + jnp.arange(4)[None, :]
    blks = jnp.concatenate([send_blk.reshape(-1), own_blk.reshape(-1)])
    hit = blks[:, None] == own[None, :]
    js = jnp.where(hit, jnp.arange(2 * NSEL)[None, :], ZERO_D).reshape(-1, 2, NSEL)
    inverse = jnp.min(js, axis=2).reshape(-1)
    o = jnp.arange(4)[None, None, :]
    recv = jnp.where(o == o0[:, :, None], 0, jnp.where(o == o1[:, :, None], 1, 2))
    parts = [loc, own, fwd.reshape(-1), inverse, recv.reshape(-1)]
    return jnp.concatenate([part.astype(jnp.int32) for part in parts])


def kernel(
    tab, in_ref, q_ref, k_ref, v_ref, g_ref,
    dq_out, dk_out, dv_out, w_out,
    kvt, xsel, in_t, xt, at, kvs, qp, gp, s_scr, pg_scr, p_scr, ds_scr,
    dsel, dxs, rbuf, acc, zs_send, zr_buf, dqg, wp, w_send, w_recv,
    z_ss, z_rs, x_ss, x_rs, i_ss, i_rs, y_ss, y_rs, dq_ss, dq_rs, dx_ss, dx_rs, w_ss, w_rs, dz_ss, dz_rs,
):
    kv, tp = lax.axis_index("kv"), lax.axis_index("tp")
    z, x = kv // X, kv % X

    def at_z(d):
        return (lax.rem(z + d, Z) * X + x, tp)

    def at_x(d):
        return (z * X + lax.rem(x + d, X), tp)

    def at_tp(d):
        return (kv, lax.rem(tp + d, TP))

    def remote(src, dst, ss, rs, dev):
        return pltpu.make_async_remote_copy(
            src_ref=src, dst_ref=dst, send_sem=ss, recv_sem=rs, device_id=dev, device_id_type=MESH
        )

    sent = []
    barrier = pltpu.get_barrier_semaphore()
    peers = [at_z(d) for d in range(1, Z)] + [at_x(d) for d in range(1, X)] + [at_tp(d) for d in range(1, TP)]
    for dev in peers:
        pl.semaphore_signal(barrier, inc=1, device_id=dev, device_id_type=MESH)
    kvt[0:4] = jnp.concatenate([k_ref[...], v_ref[...]], axis=0).T.reshape(4, KB, 128)
    in_t[...] = in_ref[...].T.reshape(X, HEAD, TOK)
    dsel[ZERO_D] = jnp.zeros((KB, 128), F32)
    pl.semaphore_wait(barrier, len(peers))

    zc = []
    for p in range(1, Z):
        there = PLACE[(Z - ORDER[p]) % Z]
        c = remote(kvt.at[pl.ds(0, 4)], kvt.at[pl.ds(4 * there, 4)], z_ss.at[p], z_rs.at[there], at_z(ORDER[p]))
        c.start()
        zc.append(c)
        sent.append(c)
    ic = []
    for d in range(1, X):
        col = lax.rem(x + d, X)
        c = remote(in_t.at[col], xt.at[:, pl.ds((X - d) * TOK, TOK)], i_ss.at[d], i_rs.at[X - d], at_x(d))
        c.start()
        ic.append(c)
        sent.append(c)
    xt[:, 0:TOK] = in_t[x]

    xc = []
    yc = []
    for p in range(Z):
        if p > 0:
            zin = remote(kvt.at[pl.ds(0, 4)], kvt.at[pl.ds(4 * p, 4)], z_ss.at[p], z_rs.at[p], at_z(ORDER[p]))
            zin.wait_recv()
        four = [kvt[4 * p + o] for o in range(4)]
        for d in range(1, X):
            for s in range(2):
                n = ((d - 1) * Z + p) * 2 + s
                o = tab[T_FWD + n]
                low = jnp.where(o == 0, four[0], four[1])
                high = jnp.where(o == 2, four[2], four[3])
                xsel[n] = jnp.where(o < 2, low, high)
        for d in range(1, X):
            mine, there = ((d - 1) * Z + p) * 2, 32 + ((X - d - 1) * Z + p) * 2
            c = remote(
                xsel.at[pl.ds(mine, 2)], kvt.at[pl.ds(there, 2)],
                x_ss.at[(d - 1) * Z + p], x_rs.at[(X - d - 1) * Z + p], at_x(d),
            )
            c.start()
            xc.append(c)
            sent.append(c)
        if p == 1:
            for c in ic:
                c.wait_recv()
            for d in range(1, TP):
                c = remote(xt, at.at[tp], y_ss.at[d], y_rs.at[TP - d], at_tp(d))
                c.start()
                yc.append(c)
                sent.append(c)
            at[tp] = xt[...]
    for c in xc:
        c.wait_recv()

    lane_t = lax.broadcasted_iota(jnp.int32, (KB, GROUP * QB), 1) % QB
    diff = lax.broadcasted_iota(jnp.int32, (KB, GROUP * QB), 0) - lane_t
    zeros = jnp.zeros((QB, HEAD), BF16)
    nt = (((1,), (1,)), ((), ()))
    nn = (((1,), (0,)), ((), ()))

    def fold(t, op):
        return op(t.reshape(8, 8, GROUP * QB), axis=0)

    for r in range(2):
        rows = pl.ds(r * QB, QB)
        for h in range(GROUP):
            cols = slice(h * HEAD, (h + 1) * HEAD)
            qp[h * QB : (h + 1) * QB, :] = jnp.concatenate([q_ref[rows, cols], zeros], axis=1)
            gp[h * QB : (h + 1) * QB, :] = jnp.concatenate([zeros, g_ref[rows, cols]], axis=1)
        for j in range(NSEL):
            kvs[j * KB : (j + 1) * KB, :] = kvt[tab[T_LOC + r * NSEL + j]]
        s_scr[...] = lax.dot_general(kvs[...], qp[...], nt, preferred_element_type=F32)
        pg_scr[...] = lax.dot_general(kvs[...], gp[...], nt, preferred_element_type=F32)

        def mask_step(j, m):
            at_j = pl.ds(pl.multiple_of(j * KB, KB), KB)
            limit = kv * TOK + r * QB - tab[T_BLK + r * NSEL + j] * KB
            s = jnp.where(diff <= limit, s_scr[at_j, :] * SCALE, NEG)
            s_scr[at_j, :] = s
            return jnp.maximum(m, fold(s, jnp.max))

        m = lax.fori_loop(0, NSEL, mask_step, jnp.full((8, GROUP * QB), NEG, F32))
        m = jnp.max(m, axis=0, keepdims=True)

        def exp_step(j, total):
            at_j = pl.ds(pl.multiple_of(j * KB, KB), KB)
            e = jnp.exp(s_scr[at_j, :] - m)
            s_scr[at_j, :] = e
            return total + fold(e, jnp.sum)

        total = lax.fori_loop(0, NSEL, exp_step, jnp.zeros((8, GROUP * QB), F32))
        inv = 1.0 / jnp.sum(total, axis=0, keepdims=True)

        def half_step(j, dot):
            at_j = pl.ds(pl.multiple_of(j * KB, KB), KB)
            half = (s_scr[at_j, :] * inv).astype(BF16)
            p_scr[at_j, :] = half
            return dot + fold(half.astype(F32) * pg_scr[at_j, :], jnp.sum)

        dot = lax.fori_loop(0, NSEL, half_step, jnp.zeros((8, GROUP * QB), F32))
        dot = jnp.sum(dot, axis=0, keepdims=True)

        def grad_step(j, carry):
            at_j = pl.ds(pl.multiple_of(j * KB, KB), KB)
            ds_scr[at_j, :] = ((s_scr[at_j, :] * inv) * (pg_scr[at_j, :] - dot)).astype(BF16)
            return carry

        lax.fori_loop(0, NSEL, grad_step, 0)
        dq_t = lax.dot_general(kvs[...].T[:HEAD], ds_scr[...], nn, preferred_element_type=F32) * SCALE
        stacked = jnp.concatenate([dq_t[:, h * QB : (h + 1) * QB] for h in range(GROUP)], axis=0)
        dqg[rows, :] = stacked.T.astype(BF16)
        dkv = lax.dot_general(ds_scr[...], qp[...], nn, preferred_element_type=F32)
        dkv += lax.dot_general(p_scr[...], gp[...], nn, preferred_element_type=F32)
        dsel[pl.ds(r * NSEL, NSEL)] = dkv.reshape(NSEL, KB, 128)
        for d in range(1, X):
            c = remote(
                dqg.at[rows], dqg.at[pl.ds((X - d) * TOK + r * QB, QB)],
                dq_ss.at[r * X + d], dq_rs.at[r * X + X - d], at_x(d),
            )
            c.start()
            sent.append(c)
    dq_out[...] = dqg[0:TOK, :]

    for p in reversed(range(Z)):
        for d in range(1, X):
            for s in range(2):
                n = ((d - 1) * Z + p) * 2 + s
                dxs[n] = (dsel[tab[T_SEND + 2 * n]] + dsel[tab[T_SEND + 2 * n + 1]]).astype(BF16)
        for d in range(1, X):
            mine, there = (d - 1) * Z + p, (X - d - 1) * Z + p
            c = remote(
                dxs.at[pl.ds(2 * mine, 2)], rbuf.at[pl.ds(2 * there, 2)],
                dx_ss.at[mine], dx_rs.at[there], at_x(d),
            )
            c.start()
            sent.append(c)

    for c in yc:
        c.wait_recv()
    for r in range(2):
        for d in range(1, X):
            src = dqg.at[pl.ds(r * QB, QB)]
            dst = dqg.at[pl.ds(d * TOK + r * QB, QB)]
            remote(src, dst, dq_ss.at[r * X + d], dq_rs.at[r * X + d], at_x(d)).wait_recv()
    wp[...] = lax.dot_general(
        at[...].reshape(TP * HEAD, X * TOK), dqg[...], nn, preferred_element_type=F32
    ).reshape(TP, HEAD, TOK)
    w_send[...] = wp[...].astype(BF16)
    wc = []
    for p in reversed(range(1, Z)):
        there = PLACE[(Z - ORDER[p]) % Z]
        c = remote(w_send.at[lax.rem(z + ORDER[p], Z)], w_recv.at[there], w_ss.at[p], w_rs.at[there], at_z(ORDER[p]))
        c.start()
        wc.append(c)
        sent.append(c)

    dzc = []
    for p in reversed(range(Z)):
        for d in range(1, X):
            mine = (d - 1) * Z + p
            remote(
                dxs.at[pl.ds(2 * mine, 2)], rbuf.at[pl.ds(2 * mine, 2)],
                dx_ss.at[mine], dx_rs.at[mine], at_x(d),
            ).wait_recv()
        for o in range(4):
            n = T_OWN + (p * 4 + o) * 2
            term = dsel[tab[n]] + dsel[tab[n + 1]]
            for d in range(1, X):
                mine = (d - 1) * Z + p
                which = tab[T_RECV + mine * 4 + o]
                slot = jnp.where(which == 0, rbuf[2 * mine], rbuf[2 * mine + 1])
                term += jnp.where(which < 2, slot.astype(F32), 0.0)
            if p > 0:
                zs_send[p * 4 + o] = term.astype(BF16)
            else:
                acc[o] = term
        if p > 0:
            there = PLACE[(Z - ORDER[p]) % Z]
            c = remote(
                zs_send.at[pl.ds(4 * p, 4)], zr_buf.at[pl.ds(4 * there, 4)],
                dz_ss.at[p], dz_rs.at[there], at_z(ORDER[p]),
            )
            c.start()
            dzc.append(c)
            sent.append(c)
    for c in wc:
        c.wait_recv()
    w = wp[z]
    for p in range(1, Z):
        w += w_recv[p].astype(F32)
    w_out[...] = w
    for c in dzc:
        c.wait_recv()
    both = acc[...]
    for p in range(1, Z):
        both += zr_buf[4 * p : 4 * p + 4].astype(F32)
    both = both.reshape(TOK, 128).T
    dk_out[...] = (both[:HEAD] * SCALE).astype(BF16)
    dv_out[...] = both[HEAD:].astype(BF16)
    for c in sent:
        c.wait_send()


def body(inputs, queries, key_vectors, value_rows_by_head, out_grad, chosen):
    tab = index_table(chosen)
    dma = pltpu.SemaphoreType.DMA
    vmem = pl.BlockSpec(memory_space=pltpu.VMEM)
    dq, dk, dv, w = pl.pallas_call(
        kernel,
        out_shape=(
            jax.ShapeDtypeStruct((TOK, GROUP * HEAD), BF16),
            jax.ShapeDtypeStruct((HEAD, TOK), BF16),
            jax.ShapeDtypeStruct((HEAD, TOK), BF16),
            jax.ShapeDtypeStruct((HEAD, GROUP * HEAD), F32),
        ),
        in_specs=[pl.BlockSpec(memory_space=pltpu.SMEM)] + [vmem] * 5,
        out_specs=(vmem,) * 4,
        scratch_shapes=[
            pltpu.VMEM((32 + 48, KB, 128), BF16),
            pltpu.VMEM((48, KB, 128), BF16),
            pltpu.VMEM((X, HEAD, TOK), BF16),
            pltpu.VMEM((HEAD, X * TOK), BF16),
            pltpu.VMEM((TP, HEAD, X * TOK), BF16),
            pltpu.VMEM((NSEL * KB, 128), BF16),
            pltpu.VMEM((GROUP * QB, 128), BF16),
            pltpu.VMEM((GROUP * QB, 128), BF16),
            pltpu.VMEM((NSEL * KB, GROUP * QB), F32),
            pltpu.VMEM((NSEL * KB, GROUP * QB), F32),
            pltpu.VMEM((NSEL * KB, GROUP * QB), BF16),
            pltpu.VMEM((NSEL * KB, GROUP * QB), BF16),
            pltpu.VMEM((2 * NSEL + 1, KB, 128), F32),
            pltpu.VMEM((48, KB, 128), BF16),
            pltpu.VMEM((48, KB, 128), BF16),
            pltpu.VMEM((4, KB, 128), F32),
            pltpu.VMEM((32, KB, 128), BF16),
            pltpu.VMEM((32, KB, 128), BF16),
            pltpu.VMEM((X * TOK, GROUP * HEAD), BF16),
            pltpu.VMEM((TP, HEAD, TOK), F32),
            pltpu.VMEM((TP, HEAD, TOK), BF16),
            pltpu.VMEM((Z, HEAD, TOK), BF16),
            dma((Z,)), dma((Z,)),
            dma((24,)), dma((24,)),
            dma((X,)), dma((X,)),
            dma((TP,)), dma((TP,)),
            dma((2 * X,)), dma((2 * X,)),
            dma((24,)), dma((24,)),
            dma((Z,)), dma((Z,)),
            dma((Z,)), dma((Z,)),
        ],
        compiler_params=pltpu.CompilerParams(
            collective_id=0, has_side_effects=True, vmem_limit_bytes=60000 * 1024
        ),
        name="fused_backward",
    )(tab, inputs, queries, key_vectors.T, value_rows_by_head.T, out_grad)
    return dq, dk.T, dv.T, w


def solution(mesh):
    spec = P("kv", "tp")
    return jax.shard_map(
        body, mesh=mesh, in_specs=(spec,) * 5 + (P(),), out_specs=(spec,) * 4, check_vma=False
    )
```

```python
import functools

import jax
import jax.numpy as jnp
from jax import lax
from jax.experimental import pallas as pl
from jax.experimental.pallas import tpu as pltpu
from jax.sharding import PartitionSpec as P

HEAD = 64
QB = 128
KB = 64
NSEL = 16
Z, X, TP = 8, 4, 8
TOK = 256
GROUP = 4
SCALE = HEAD**-0.5
ORDER = (0, 1, 7, 2, 6, 3, 5, 4)
PLACE = {d: p for p, d in enumerate(ORDER)}
NEG = -1e30
MESH = pl.DeviceIdType.MESH
F32, BF16 = jnp.float32, jnp.bfloat16
ZERO_D = 2 * NSEL
T_FWD, T_SEND, T_OWN, T_LOC, T_BLK, T_ROWS = 0, 6, 18, 20, 21, 24


def place_of(distance):
    near = jnp.where(distance < 4, 2 * distance - 1, jnp.where(distance == 4, 7, 2 * (8 - distance)))
    return jnp.where(distance == 0, 0, near)


def fill_table(table, chosen_t, z, x):
    by_row = chosen_t[...]
    lane_r = lax.broadcasted_iota(jnp.int32, by_row.shape, 1)

    def column(d, e):
        row = z * 2 * X + 2 * lax.rem(x + d, X) + e
        return jnp.sum(jnp.where(lane_r == row, by_row, 0), axis=1, keepdims=True)

    cols = [[column(d, e) for e in range(2)] for d in range(X)]
    lane = lax.broadcasted_iota(jnp.int32, (1, 128), 1)
    sub = lax.broadcasted_iota(jnp.int32, (NSEL, 128), 0)

    def row_of_place(place):
        half = (place + 1) >> 1
        d = jnp.where((place & 1) == 1, half, Z - half)
        d = jnp.where(place == 7, 4, d)
        return (z + d) & 7

    def two_used(pair, base):
        low, high = 3, 0
        for col in pair:
            rel = col - base
            ok = (rel >= 0) & (rel < 4)
            low = jnp.minimum(low, jnp.min(jnp.where(ok, rel, 3), axis=0, keepdims=True))
            high = jnp.maximum(high, jnp.max(jnp.where(ok, rel, 0), axis=0, keepdims=True))
        return low, high

    def inverse(e, block):
        hit = cols[0][e] == block
        return jnp.min(jnp.where(hit, sub + NSEL * e, ZERO_D), axis=0, keepdims=True)

    at_place = row_of_place(lane & 7) * 16
    for d in range(1, X):
        low, high = two_used(cols[d], at_place + x * 4)
        n = (d - 1) * 2
        table[T_FWD + n : T_FWD + n + 1] = low
        table[T_FWD + n + 1 : T_FWD + n + 2] = high
        base = at_place + lax.rem(x + d, X) * 4
        for s, o in enumerate(two_used(cols[0], base)):
            for e in range(2):
                m = T_SEND + ((d - 1) * 2 + s) * 2 + e
                table[m : m + 1] = inverse(e, base + o)
    mine = row_of_place((lane >> 2) & 7) * 16 + x * 4 + (lane & 3)
    for e in range(2):
        table[T_OWN + e : T_OWN + e + 1] = inverse(e, mine)
    diag = sub == (lane & (NSEL - 1))
    flat = [jnp.sum(jnp.where(diag, cols[0][e], 0), axis=0, keepdims=True) for e in range(2)]
    block = jnp.where(lane < NSEL, flat[0], flat[1])
    owner, off = block >> 2, block & 3
    place = place_of(((owner >> 2) - z) & 7)
    dx = ((owner & 3) - x) & 3
    earlier = 0
    for e in range(2):
        same = ((cols[0][e] >> 2) == owner) & ((cols[0][e] & 3) < off)
        earlier = jnp.maximum(earlier, jnp.max(jnp.where(same, 1, 0), axis=0, keepdims=True))
    loc = jnp.where(dx == 0, place * 4 + off, 32 + ((dx - 1) * Z + place) * 2 + earlier)
    table[T_LOC : T_LOC + 1] = jnp.where(owner > z * X + x, 0, loc)
    table[T_BLK : T_BLK + 1] = block


def kernel(
    chosen_t, in_ref, q_ref, k_ref, v_ref, g_ref,
    dq_out, dk_out, dv_out, w_out,
    tab_v, tab, kvt, xsel, in_t, xt, at, kvs, qp, gp, s_scr, pg_scr, p_scr, ds_scr,
    dsel, dxs, rbuf, acc, zs_send, zr_buf, dqg, wp, w_send, w_recv,
    t_sem, z_ss, z_rs, x_ss, x_rs, i_ss, i_rs, y_ss, y_rs, dq_ss, dq_rs, dx_ss, dx_rs, w_ss, w_rs, dz_ss, dz_rs,
):
    kv, tp = lax.axis_index("kv"), lax.axis_index("tp")
    z, x = kv // X, lax.rem(kv, X)

    def row(p):
        return lax.rem(z + ORDER[p], Z)

    def at_z(p):
        return (row(p) * X + x, tp)

    def at_x(d):
        return (z * X + lax.rem(x + d, X), tp)

    def at_tp(d):
        return (kv, lax.rem(tp + d, TP))

    def remote(src, dst, ss, rs, dev):
        return pltpu.make_async_remote_copy(
            src_ref=src, dst_ref=dst, send_sem=ss, recv_sem=rs, device_id=dev, device_id_type=MESH
        )

    def opposite(p):
        return PLACE[(Z - ORDER[p]) % Z]

    def column(d):
        return lax.rem(x + d, X)

    with jax.named_scope("bar"):
        barrier = pltpu.get_barrier_semaphore()
        peers = [at_z(p) for p in range(1, Z)] + [at_x(d) for d in range(1, X)] + [at_tp(d) for d in range(1, TP)]
        for dev in peers:
            pl.semaphore_signal(barrier, inc=1, device_id=dev, device_id_type=MESH)
        kvt[0:4] = jnp.concatenate([k_ref[...], v_ref[...]], axis=0).T.reshape(4, KB, 128)
        in_t[...] = in_ref[...].T.reshape(X, HEAD, TOK)
        fill_table(tab_v, chosen_t, z, x)
        dsel[ZERO_D] = jnp.zeros((KB, 128), F32)
        t_copy = pltpu.make_async_copy(tab_v, tab, t_sem)
        t_copy.start()
        xt[:, 0:TOK] = in_t[x]
        pl.semaphore_wait(barrier, len(peers))

    def z_keys(p):
        there = opposite(p)
        return remote(kvt.at[pl.ds(0, 4)], kvt.at[pl.ds(4 * there, 4)], z_ss.at[p], z_rs.at[there], at_z(p))

    for p in range(1, Z):
        pl.when(row(p) > z)(z_keys(p).start)

    def x_inputs(d):
        return remote(
            in_t.at[column(d)], xt.at[:, pl.ds((X - d) * TOK, TOK)], i_ss.at[d], i_rs.at[X - d], at_x(d)
        )

    for d in range(1, X):
        x_inputs(d).start()

    def tp_inputs(d):
        return remote(xt, at.at[tp], y_ss.at[d], y_rs.at[TP - d], at_tp(d))

    def x_keys(p, d):
        mine, there = ((d - 1) * Z + p) * 2, 32 + ((X - d - 1) * Z + p) * 2
        return remote(
            xsel.at[pl.ds(mine, 2)], kvt.at[pl.ds(there, 2)],
            x_ss.at[(d - 1) * Z + p], x_rs.at[(X - d - 1) * Z + p], at_x(d),
        )

    def x_keys_in(p, d):
        there = 32 + ((d - 1) * Z + p) * 2
        n = (d - 1) * Z + p
        return remote(xsel.at[pl.ds(2 * n, 2)], kvt.at[pl.ds(there, 2)], x_ss.at[n], x_rs.at[n], at_x(d))

    def forward(p):
        four = [kvt[4 * p + o] for o in range(4)]
        for d in range(1, X):
            for s in range(2):
                o = tab[T_FWD + (d - 1) * 2 + s, p]
                low = jnp.where(o == 0, four[0], four[1])
                high = jnp.where(o == 2, four[2], four[3])
                xsel[((d - 1) * Z + p) * 2 + s] = jnp.where(o < 2, low, high)
        for d in range(1, X):
            if p > 0:
                x_keys(p, d).start()
            else:
                pl.when(column(d) > x)(x_keys(p, d).start)

    with jax.named_scope("sel"):
        t_copy.wait()
        forward(0)
        for p in range(1, Z):
            @pl.when(row(p) < z)
            def _(p=p):
                remote(
                    kvt.at[pl.ds(0, 4)], kvt.at[pl.ds(4 * p, 4)], z_ss.at[p], z_rs.at[p], at_z(p)
                ).wait_recv()
                forward(p)

            if p == 2:
                for d in range(1, X):
                    x_inputs(d).wait_recv()
                for d in range(1, TP):
                    tp_inputs(d).start()
                at[tp] = xt[...]
    with jax.named_scope("xwait"):
        for p in range(1, Z):
            @pl.when(row(p) < z)
            def _(p=p):
                for d in range(1, X):
                    x_keys_in(p, d).wait_recv()
        for d in range(1, X):
            pl.when(column(d) < x)(x_keys_in(0, d).wait_recv)

    lanes = 2 * QB
    lane_t = lax.broadcasted_iota(jnp.int32, (KB, lanes), 1) % QB
    diff = lax.broadcasted_iota(jnp.int32, (KB, lanes), 0) - lane_t
    zeros = jnp.zeros((QB, HEAD), BF16)
    nt = (((1,), (1,)), ((), ()))
    nn = (((1,), (0,)), ((), ()))

    def fold(t, op):
        return op(t.reshape(KB // 8, 8, lanes), axis=0)

    def x_dq(r, hp, d):
        cols = pl.ds(hp * 2 * HEAD, 2 * HEAD)
        n = (r * 2 + hp) * X
        return remote(
            dqg.at[pl.ds(r * QB, QB), cols], dqg.at[pl.ds((X - d) * TOK + r * QB, QB), cols],
            dq_ss.at[n + d], dq_rs.at[n + X - d], at_x(d),
        )

    units = [(r, hp) for r in range(2) for hp in range(2)]
    for r, hp in units:
        scope = jax.named_scope(f"attn{r}{hp}")
        scope.__enter__()
        rows = pl.ds(r * QB, QB)
        if hp == 0:
            for j in range(NSEL):
                kvs[j * KB : (j + 1) * KB, :] = kvt[tab[T_LOC, r * NSEL + j]]
        for h in range(2):
            cols = slice((hp * 2 + h) * HEAD, (hp * 2 + h + 1) * HEAD)
            qp[h * QB : (h + 1) * QB, :] = jnp.concatenate([q_ref[rows, cols], zeros], axis=1)
            gp[h * QB : (h + 1) * QB, :] = jnp.concatenate([zeros, g_ref[rows, cols]], axis=1)
        s_scr[...] = lax.dot_general(kvs[...], qp[...], nt, preferred_element_type=F32)
        pg_scr[...] = lax.dot_general(kvs[...], gp[...], nt, preferred_element_type=F32)

        def mask_step(j, m):
            at_j = pl.ds(pl.multiple_of(j * KB, KB), KB)
            limit = kv * TOK + r * QB - tab[T_BLK, r * NSEL + j] * KB
            s = jnp.where(diff <= limit, s_scr[at_j, :] * SCALE, NEG)
            s_scr[at_j, :] = s
            return jnp.maximum(m, fold(s, jnp.max))

        m = lax.fori_loop(0, NSEL, mask_step, jnp.full((8, lanes), NEG, F32), unroll=4)
        m = jnp.max(m, axis=0, keepdims=True)

        def exp_step(j, total):
            at_j = pl.ds(pl.multiple_of(j * KB, KB), KB)
            e = jnp.exp(s_scr[at_j, :] - m)
            s_scr[at_j, :] = e
            return total + fold(e, jnp.sum)

        total = lax.fori_loop(0, NSEL, exp_step, jnp.zeros((8, lanes), F32), unroll=4)
        inv = 1.0 / jnp.sum(total, axis=0, keepdims=True)

        def half_step(j, dot):
            at_j = pl.ds(pl.multiple_of(j * KB, KB), KB)
            half = (s_scr[at_j, :] * inv).astype(BF16)
            p_scr[at_j, :] = half
            return dot + fold(half.astype(F32) * pg_scr[at_j, :], jnp.sum)

        dot = lax.fori_loop(0, NSEL, half_step, jnp.zeros((8, lanes), F32), unroll=4)
        dot = jnp.sum(dot, axis=0, keepdims=True)

        def grad_step(j, carry):
            at_j = pl.ds(pl.multiple_of(j * KB, KB), KB)
            ds_scr[at_j, :] = ((s_scr[at_j, :] * inv) * (pg_scr[at_j, :] - dot)).astype(BF16)
            return carry

        lax.fori_loop(0, NSEL, grad_step, 0, unroll=4)
        dq_t = lax.dot_general(kvs[...].T[:HEAD], ds_scr[...], nn, preferred_element_type=F32) * SCALE
        stacked = jnp.concatenate([dq_t[:, :QB], dq_t[:, QB:]], axis=0)
        dqg[rows, hp * 2 * HEAD : (hp + 1) * 2 * HEAD] = stacked.T.astype(BF16)
        dkv = lax.dot_general(ds_scr[...], qp[...], nn, preferred_element_type=F32)
        dkv += lax.dot_general(p_scr[...], gp[...], nn, preferred_element_type=F32)
        if hp == 0:
            dsel[pl.ds(r * NSEL, NSEL)] = dkv.reshape(NSEL, KB, 128)
        else:
            dsel[pl.ds(r * NSEL, NSEL)] += dkv.reshape(NSEL, KB, 128)
        for d in range(1, X):
            x_dq(r, hp, d).start()
        scope.__exit__(None, None, None)
    dq_out[...] = dqg[0:TOK, :]

    def x_grads(p, d):
        mine, there = (d - 1) * Z + p, (X - d - 1) * Z + p
        return remote(
            dxs.at[pl.ds(2 * mine, 2)], rbuf.at[pl.ds(2 * there, 2)], dx_ss.at[mine], dx_rs.at[there], at_x(d)
        )

    def x_grads_in(p, d):
        mine = (d - 1) * Z + p
        return remote(
            dxs.at[pl.ds(2 * mine, 2)], rbuf.at[pl.ds(2 * mine, 2)], dx_ss.at[mine], dx_rs.at[mine], at_x(d)
        )

    with jax.named_scope("dxsend"):
        for p in reversed(range(Z)):
            @pl.when(row(p) <= z)
            def _(p=p):
                for d in range(1, X):
                    for s in range(2):
                        t = T_SEND + ((d - 1) * 2 + s) * 2
                        dxs[((d - 1) * Z + p) * 2 + s] = (dsel[tab[t, p]] + dsel[tab[t + 1, p]]).astype(BF16)
                for d in range(1, X):
                    if p > 0:
                        x_grads(p, d).start()
                    else:
                        pl.when(column(d) < x)(x_grads(p, d).start)

    def z_weight(p):
        there = opposite(p)
        return remote(w_send.at[row(p)], w_recv.at[there], w_ss.at[p], w_rs.at[there], at_z(p))

    with jax.named_scope("wgrad"):
        for d in range(1, TP):
            tp_inputs(d).wait_recv()
        for r, hp in units:
            for d in range(1, X):
                x_dq(r, hp, d).wait_recv()
        wp[...] = lax.dot_general(
            at[...].reshape(TP * HEAD, X * TOK), dqg[...], nn, preferred_element_type=F32
        ).reshape(TP, HEAD, TOK)
        w_send[...] = wp[...].astype(BF16)
        for p in reversed(range(1, Z)):
            z_weight(p).start()

    def z_grads(p):
        there = opposite(p)
        return remote(
            zs_send.at[pl.ds(4 * p, 4)], zr_buf.at[pl.ds(4 * there, 4)], dz_ss.at[p], dz_rs.at[there], at_z(p)
        )

    def relay(p, o):
        n = p * 4 + o
        term = dsel[tab[T_OWN, n]] + dsel[tab[T_OWN + 1, n]]
        for d in range(1, X):
            mine = (d - 1) * Z + p
            t = T_FWD + (d - 1) * 2
            first = tab[t, p] == o
            used = first | (tab[t + 1, p] == o)
            if p == 0:
                used = used & (column(d) > x)
            slot = jnp.where(first, rbuf[2 * mine], rbuf[2 * mine + 1]).astype(F32)
            term += jnp.where(used, slot, 0.0)
        return term

    with jax.named_scope("relay"):
        for p in reversed(range(1, Z)):
            @pl.when(row(p) < z)
            def _(p=p):
                for d in range(1, X):
                    x_grads_in(p, d).wait_recv()
                for o in range(4):
                    zs_send[p * 4 + o] = relay(p, o).astype(BF16)
                z_grads(p).start()

        for d in range(1, X):
            pl.when(column(d) > x)(x_grads_in(0, d).wait_recv)
        for o in range(4):
            acc[o] = relay(0, o)
    with jax.named_scope("wfin"):
        w = wp[z]
        for p in range(1, Z):
            z_weight(p).wait_recv()
        for p in range(1, Z):
            w += w_recv[p].astype(F32)
        w_out[...] = w
    with jax.named_scope("dzwait"):
        for p in range(1, Z):
            @pl.when(row(p) > z)
            def _(p=p):
                remote(
                    zs_send.at[pl.ds(4 * p, 4)], zr_buf.at[pl.ds(4 * p, 4)], dz_ss.at[p], dz_rs.at[p], at_z(p)
                ).wait_recv()
                acc[...] += zr_buf[4 * p : 4 * p + 4].astype(F32)
        both = acc[...].reshape(TOK, 128).T
        dk_out[...] = (both[:HEAD] * SCALE).astype(BF16)
        dv_out[...] = both[HEAD:].astype(BF16)
    with jax.named_scope("sentwait"):
        for p in range(1, Z):
            pl.when(row(p) > z)(z_keys(p).wait_send)
            pl.when(row(p) < z)(z_grads(p).wait_send)
            z_weight(p).wait_send()
            @pl.when(row(p) < z)
            def _(p=p):
                for d in range(1, X):
                    x_keys(p, d).wait_send()
                    x_grads(p, d).wait_send()
        for d in range(1, X):
            pl.when(column(d) > x)(x_keys(0, d).wait_send)
            pl.when(column(d) < x)(x_grads(0, d).wait_send)
            x_inputs(d).wait_send()
            for r, hp in units:
                x_dq(r, hp, d).wait_send()
        for d in range(1, TP):
            tp_inputs(d).wait_send()


def body(inputs, queries, key_vectors, value_rows_by_head, out_grad, chosen):
    dma = pltpu.SemaphoreType.DMA
    vmem = pl.BlockSpec(memory_space=pltpu.VMEM)
    dq, dk, dv, w = pl.pallas_call(
        kernel,
        out_shape=(
            jax.ShapeDtypeStruct((TOK, GROUP * HEAD), BF16),
            jax.ShapeDtypeStruct((HEAD, TOK), BF16),
            jax.ShapeDtypeStruct((HEAD, TOK), BF16),
            jax.ShapeDtypeStruct((HEAD, GROUP * HEAD), F32),
        ),
        in_specs=[vmem] * 6,
        out_specs=(vmem,) * 4,
        scratch_shapes=[
            pltpu.VMEM((T_ROWS, 128), jnp.int32),
            pltpu.SMEM((T_ROWS, 128), jnp.int32),
            pltpu.VMEM((32 + 48, KB, 128), BF16),
            pltpu.VMEM((48, KB, 128), BF16),
            pltpu.VMEM((X, HEAD, TOK), BF16),
            pltpu.VMEM((HEAD, X * TOK), BF16),
            pltpu.VMEM((TP, HEAD, X * TOK), BF16),
            pltpu.VMEM((NSEL * KB, 128), BF16),
            pltpu.VMEM((2 * QB, 128), BF16),
            pltpu.VMEM((2 * QB, 128), BF16),
            pltpu.VMEM((NSEL * KB, 2 * QB), F32),
            pltpu.VMEM((NSEL * KB, 2 * QB), F32),
            pltpu.VMEM((NSEL * KB, 2 * QB), BF16),
            pltpu.VMEM((NSEL * KB, 2 * QB), BF16),
            pltpu.VMEM((2 * NSEL + 1, KB, 128), F32),
            pltpu.VMEM((48, KB, 128), BF16),
            pltpu.VMEM((48, KB, 128), BF16),
            pltpu.VMEM((4, KB, 128), F32),
            pltpu.VMEM((32, KB, 128), BF16),
            pltpu.VMEM((32, KB, 128), BF16),
            pltpu.VMEM((X * TOK, GROUP * HEAD), BF16),
            pltpu.VMEM((TP, HEAD, TOK), F32),
            pltpu.VMEM((TP, HEAD, TOK), BF16),
            pltpu.VMEM((Z, HEAD, TOK), BF16),
            dma,
            dma((Z,)), dma((Z,)),
            dma((24,)), dma((24,)),
            dma((X,)), dma((X,)),
            dma((TP,)), dma((TP,)),
            dma((4 * X,)), dma((4 * X,)),
            dma((24,)), dma((24,)),
            dma((Z,)), dma((Z,)),
            dma((Z,)), dma((Z,)),
        ],
        compiler_params=pltpu.CompilerParams(
            collective_id=0, has_side_effects=True, vmem_limit_bytes=60000 * 1024
        ),
        name="fused_backward",
    )(chosen.T, inputs, queries, key_vectors.T, value_rows_by_head.T, out_grad)
    return dq, dk.T, dv.T, w


def solution(mesh):
    spec = P("kv", "tp")
    return jax.shard_map(
        body, mesh=mesh, in_specs=(spec,) * 5 + (P(),), out_specs=(spec,) * 4, check_vma=False
    )
```

```python
import functools

import jax
import jax.numpy as jnp
from jax import lax
from jax.experimental import pallas as pl
from jax.experimental.pallas import tpu as pltpu
from jax.sharding import PartitionSpec as P

HEAD = 64
QB = 128
KB = 64
NSEL = 16
Z, X, TP = 8, 4, 8
TOK = 256
GROUP = 4
SCALE = HEAD**-0.5
ORDER = (0, 1, 7, 2, 6, 3, 5, 4)
PLACE = {d: p for p, d in enumerate(ORDER)}
NEG = -1e30
MESH = pl.DeviceIdType.MESH
F32, BF16 = jnp.float32, jnp.bfloat16
ZERO_D = 2 * NSEL
T_FWD, T_SEND, T_OWN, T_LOC, T_BLK, T_ROWS = 0, 6, 18, 20, 21, 24


def place_of(distance):
    near = jnp.where(distance < 4, 2 * distance - 1, jnp.where(distance == 4, 7, 2 * (8 - distance)))
    return jnp.where(distance == 0, 0, near)


def fill_table(table, chosen_t, z, x):
    by_row = chosen_t[...]
    lane_r = lax.broadcasted_iota(jnp.int32, by_row.shape, 1)

    def column(d, e):
        row = z * 2 * X + 2 * lax.rem(x + d, X) + e
        return jnp.sum(jnp.where(lane_r == row, by_row, 0), axis=1, keepdims=True)

    cols = [[column(d, e) for e in range(2)] for d in range(X)]
    lane = lax.broadcasted_iota(jnp.int32, (1, 128), 1)
    sub = lax.broadcasted_iota(jnp.int32, (NSEL, 128), 0)

    def row_of_place(place):
        half = (place + 1) >> 1
        d = jnp.where((place & 1) == 1, half, Z - half)
        d = jnp.where(place == 7, 4, d)
        return (z + d) & 7

    def two_used(pair, base):
        low, high = 3, 0
        for col in pair:
            rel = col - base
            ok = (rel >= 0) & (rel < 4)
            low = jnp.minimum(low, jnp.min(jnp.where(ok, rel, 3), axis=0, keepdims=True))
            high = jnp.maximum(high, jnp.max(jnp.where(ok, rel, 0), axis=0, keepdims=True))
        return low, high

    def inverse(e, block):
        hit = cols[0][e] == block
        return jnp.min(jnp.where(hit, sub + NSEL * e, ZERO_D), axis=0, keepdims=True)

    at_place = row_of_place(lane & 7) * 16
    for d in range(1, X):
        low, high = two_used(cols[d], at_place + x * 4)
        n = (d - 1) * 2
        table[T_FWD + n : T_FWD + n + 1] = low
        table[T_FWD + n + 1 : T_FWD + n + 2] = high
        base = at_place + lax.rem(x + d, X) * 4
        for s, o in enumerate(two_used(cols[0], base)):
            for e in range(2):
                m = T_SEND + ((d - 1) * 2 + s) * 2 + e
                table[m : m + 1] = inverse(e, base + o)
    mine = row_of_place((lane >> 2) & 7) * 16 + x * 4 + (lane & 3)
    for e in range(2):
        table[T_OWN + e : T_OWN + e + 1] = inverse(e, mine)
    diag = sub == (lane & (NSEL - 1))
    flat = [jnp.sum(jnp.where(diag, cols[0][e], 0), axis=0, keepdims=True) for e in range(2)]
    block = jnp.where(lane < NSEL, flat[0], flat[1])
    owner, off = block >> 2, block & 3
    place = place_of(((owner >> 2) - z) & 7)
    dx = ((owner & 3) - x) & 3
    earlier = 0
    for e in range(2):
        same = ((cols[0][e] >> 2) == owner) & ((cols[0][e] & 3) < off)
        earlier = jnp.maximum(earlier, jnp.max(jnp.where(same, 1, 0), axis=0, keepdims=True))
    loc = jnp.where(dx == 0, place * 4 + off, 32 + ((dx - 1) * Z + place) * 2 + earlier)
    table[T_LOC : T_LOC + 1] = jnp.where(owner > z * X + x, 0, loc)
    table[T_BLK : T_BLK + 1] = block


def kernel(
    chosen_t, in_ref, q_ref, k_ref, v_ref, g_ref,
    dq_out, dk_out, dv_out, w_out,
    tab_v, tab, kvt, xsel, in_t, xt, at, kvs, qp, gp, s_scr, pg_scr, p_scr, ds_scr,
    dsel, dxs, rbuf, acc, zs_send, zr_buf, dqg, wp, w_send, w_recv,
    t_sem, z_ss, z_rs, x_ss, x_rs, i_ss, i_rs, y_ss, y_rs, dq_ss, dq_rs, dx_ss, dx_rs, w_ss, w_rs, dz_ss, dz_rs,
):
    kv, tp = lax.axis_index("kv"), lax.axis_index("tp")
    z, x = kv // X, lax.rem(kv, X)

    def row(p):
        return lax.rem(z + ORDER[p], Z)

    def at_z(p):
        return (row(p) * X + x, tp)

    def at_x(d):
        return (z * X + lax.rem(x + d, X), tp)

    def at_tp(d):
        return (kv, lax.rem(tp + d, TP))

    def remote(src, dst, ss, rs, dev):
        return pltpu.make_async_remote_copy(
            src_ref=src, dst_ref=dst, send_sem=ss, recv_sem=rs, device_id=dev, device_id_type=MESH
        )

    def opposite(p):
        return PLACE[(Z - ORDER[p]) % Z]

    def column(d):
        return lax.rem(x + d, X)

    with jax.named_scope("bar"):
        barrier = pltpu.get_barrier_semaphore()
        peers = [at_z(p) for p in range(1, Z)] + [at_x(d) for d in range(1, X)] + [at_tp(d) for d in range(1, TP)]
        for dev in peers:
            pl.semaphore_signal(barrier, inc=1, device_id=dev, device_id_type=MESH)
        kvt[0:4] = jnp.concatenate([k_ref[...], v_ref[...]], axis=0).T.reshape(4, KB, 128)
        in_t[...] = in_ref[...].T.reshape(X, HEAD, TOK)
        fill_table(tab_v, chosen_t, z, x)
        dsel[ZERO_D] = jnp.zeros((KB, 128), F32)
        t_copy = pltpu.make_async_copy(tab_v, tab, t_sem)
        t_copy.start()
        xt[:, 0:TOK] = in_t[x]
        pl.semaphore_wait(barrier, len(peers))

    def z_keys(hop, f, up):
        here = 0 if hop == 1 else PLACE[Z + 1 - hop if up else hop - 1]
        there = PLACE[Z - hop if up else hop]
        n = 2 * there + f
        to = (lax.rem(z + (1 if up else Z - 1), Z) * X + x, tp)
        return remote(
            kvt.at[pl.ds(4 * here + 2 * f, 2)], kvt.at[pl.ds(4 * there + 2 * f, 2)], z_ss.at[n], z_rs.at[n], to
        )

    def z_sends(hop, up):
        if up:
            return (z >= hop - 1) & (z < Z - 1)
        return lax.rem(z + hop - 1, Z) <= Z - 6

    def z_gets(hop, up):
        if up:
            return z >= hop
        return lax.rem(z + hop, Z) <= Z - 6

    HOPS = [(hop, up) for hop in range(1, 5) for up in (True, False) if up or hop < 4]
    for f in range(2):
        for up in (True, False):
            pl.when(z_sends(1, up))(z_keys(1, f, up).start)

    def x_inputs(d):
        return remote(
            in_t.at[column(d)], xt.at[:, pl.ds((X - d) * TOK, TOK)], i_ss.at[d], i_rs.at[X - d], at_x(d)
        )

    def tp_inputs(d):
        return remote(xt, at.at[tp], y_ss.at[d], y_rs.at[TP - d], at_tp(d))

    def x_keys(p, d):
        mine, there = ((d - 1) * Z + p) * 2, 32 + ((X - d - 1) * Z + p) * 2
        return remote(
            xsel.at[pl.ds(mine, 2)], kvt.at[pl.ds(there, 2)],
            x_ss.at[(d - 1) * Z + p], x_rs.at[(X - d - 1) * Z + p], at_x(d),
        )

    def x_keys_in(p, d):
        there = 32 + ((d - 1) * Z + p) * 2
        n = (d - 1) * Z + p
        return remote(xsel.at[pl.ds(2 * n, 2)], kvt.at[pl.ds(there, 2)], x_ss.at[n], x_rs.at[n], at_x(d))

    def forward(p):
        four = [kvt[4 * p + o] for o in range(4)]
        for d in range(1, X):
            for s in range(2):
                o = tab[T_FWD + (d - 1) * 2 + s, p]
                low = jnp.where(o == 0, four[0], four[1])
                high = jnp.where(o == 2, four[2], four[3])
                xsel[((d - 1) * Z + p) * 2 + s] = jnp.where(o < 2, low, high)
        for d in range(1, X):
            if p > 0:
                x_keys(p, d).start()
            else:
                pl.when(column(d) > x)(x_keys(p, d).start)

    with jax.named_scope("sel"):
        t_copy.wait()
        forward(0)
        for d in range(1, X):
            x_inputs(d).start()
        for hop, up in HOPS:
            @pl.when(z_gets(hop, up))
            def _(hop=hop, up=up):
                for f in range(2):
                    z_keys(hop, f, up).wait_recv()
                    if hop < (4 if up else 3):
                        pl.when(z_sends(hop + 1, up))(z_keys(hop + 1, f, up).start)
            p = PLACE[Z - hop if up else hop]
            pl.when(row(p) < z)(functools.partial(forward, p))
            if hop == 1 and not up:
                for d in range(1, X):
                    x_inputs(d).wait_recv()
                for d in range(1, TP):
                    tp_inputs(d).start()
                at[tp] = xt[...]
    with jax.named_scope("xwait"):
        for p in range(1, Z):
            @pl.when(row(p) < z)
            def _(p=p):
                for d in range(1, X):
                    x_keys_in(p, d).wait_recv()
        for d in range(1, X):
            pl.when(column(d) < x)(x_keys_in(0, d).wait_recv)

    lanes = 2 * QB
    lane_t = lax.broadcasted_iota(jnp.int32, (KB, lanes), 1) % QB
    diff = lax.broadcasted_iota(jnp.int32, (KB, lanes), 0) - lane_t
    zeros = jnp.zeros((QB, HEAD), BF16)
    nt = (((1,), (1,)), ((), ()))
    nn = (((1,), (0,)), ((), ()))

    def fold(t, op):
        return op(t.reshape(KB // 8, 8, lanes), axis=0)

    def x_dq(r, hp, d):
        cols = pl.ds(hp * 2 * HEAD, 2 * HEAD)
        n = (r * 2 + hp) * X
        return remote(
            dqg.at[pl.ds(r * QB, QB), cols], dqg.at[pl.ds((X - d) * TOK + r * QB, QB), cols],
            dq_ss.at[n + d], dq_rs.at[n + X - d], at_x(d),
        )

    units = [(r, hp) for r in range(2) for hp in range(2)]
    for r, hp in units:
        scope = jax.named_scope(f"attn{r}{hp}")
        scope.__enter__()
        rows = pl.ds(r * QB, QB)
        if hp == 0:
            for j in range(NSEL):
                kvs[j * KB : (j + 1) * KB, :] = kvt[tab[T_LOC, r * NSEL + j]]
        for h in range(2):
            cols = slice((hp * 2 + h) * HEAD, (hp * 2 + h + 1) * HEAD)
            qp[h * QB : (h + 1) * QB, :] = jnp.concatenate([q_ref[rows, cols], zeros], axis=1)
            gp[h * QB : (h + 1) * QB, :] = jnp.concatenate([zeros, g_ref[rows, cols]], axis=1)
        s_scr[...] = lax.dot_general(kvs[...], qp[...], nt, preferred_element_type=F32)
        pg_scr[...] = lax.dot_general(kvs[...], gp[...], nt, preferred_element_type=F32)

        def mask_step(j, m):
            at_j = pl.ds(pl.multiple_of(j * KB, KB), KB)
            limit = kv * TOK + r * QB - tab[T_BLK, r * NSEL + j] * KB
            s = jnp.where(diff <= limit, s_scr[at_j, :] * SCALE, NEG)
            s_scr[at_j, :] = s
            return jnp.maximum(m, fold(s, jnp.max))

        m = lax.fori_loop(0, NSEL, mask_step, jnp.full((8, lanes), NEG, F32), unroll=4)
        m = jnp.max(m, axis=0, keepdims=True)

        def exp_step(j, total):
            at_j = pl.ds(pl.multiple_of(j * KB, KB), KB)
            e = jnp.exp(s_scr[at_j, :] - m)
            s_scr[at_j, :] = e
            return total + fold(e, jnp.sum)

        total = lax.fori_loop(0, NSEL, exp_step, jnp.zeros((8, lanes), F32), unroll=4)
        inv = 1.0 / jnp.sum(total, axis=0, keepdims=True)

        def half_step(j, dot):
            at_j = pl.ds(pl.multiple_of(j * KB, KB), KB)
            half = (s_scr[at_j, :] * inv).astype(BF16)
            p_scr[at_j, :] = half
            return dot + fold(half.astype(F32) * pg_scr[at_j, :], jnp.sum)

        dot = lax.fori_loop(0, NSEL, half_step, jnp.zeros((8, lanes), F32), unroll=4)
        dot = jnp.sum(dot, axis=0, keepdims=True)

        def grad_step(j, carry):
            at_j = pl.ds(pl.multiple_of(j * KB, KB), KB)
            ds_scr[at_j, :] = ((s_scr[at_j, :] * inv) * (pg_scr[at_j, :] - dot)).astype(BF16)
            return carry

        lax.fori_loop(0, NSEL, grad_step, 0, unroll=4)
        dq_t = lax.dot_general(kvs[...].T[:HEAD], ds_scr[...], nn, preferred_element_type=F32) * SCALE
        stacked = jnp.concatenate([dq_t[:, :QB], dq_t[:, QB:]], axis=0)
        dqg[rows, hp * 2 * HEAD : (hp + 1) * 2 * HEAD] = stacked.T.astype(BF16)
        dkv = lax.dot_general(ds_scr[...], qp[...], nn, preferred_element_type=F32)
        dkv += lax.dot_general(p_scr[...], gp[...], nn, preferred_element_type=F32)
        if hp == 0:
            dsel[pl.ds(r * NSEL, NSEL)] = dkv.reshape(NSEL, KB, 128)
        else:
            dsel[pl.ds(r * NSEL, NSEL)] += dkv.reshape(NSEL, KB, 128)
        for d in range(1, X):
            x_dq(r, hp, d).start()
        scope.__exit__(None, None, None)
    dq_out[...] = dqg[0:TOK, :]

    def x_grads(p, d):
        mine, there = (d - 1) * Z + p, (X - d - 1) * Z + p
        return remote(
            dxs.at[pl.ds(2 * mine, 2)], rbuf.at[pl.ds(2 * there, 2)], dx_ss.at[mine], dx_rs.at[there], at_x(d)
        )

    def x_grads_in(p, d):
        mine = (d - 1) * Z + p
        return remote(
            dxs.at[pl.ds(2 * mine, 2)], rbuf.at[pl.ds(2 * mine, 2)], dx_ss.at[mine], dx_rs.at[mine], at_x(d)
        )

    with jax.named_scope("dxsend"):
        for p in reversed(range(Z)):
            @pl.when(row(p) <= z)
            def _(p=p):
                for d in range(1, X):
                    for s in range(2):
                        t = T_SEND + ((d - 1) * 2 + s) * 2
                        dxs[((d - 1) * Z + p) * 2 + s] = (dsel[tab[t, p]] + dsel[tab[t + 1, p]]).astype(BF16)
                for d in range(1, X):
                    if p > 0:
                        x_grads(p, d).start()
                    else:
                        pl.when(column(d) < x)(x_grads(p, d).start)

    def z_weight(p):
        there = opposite(p)
        return remote(w_send.at[row(p)], w_recv.at[there], w_ss.at[p], w_rs.at[there], at_z(p))

    with jax.named_scope("wgrad"):
        for d in range(1, TP):
            tp_inputs(d).wait_recv()
        for r, hp in units:
            for d in range(1, X):
                x_dq(r, hp, d).wait_recv()
        wp[...] = lax.dot_general(
            at[...].reshape(TP * HEAD, X * TOK), dqg[...], nn, preferred_element_type=F32
        ).reshape(TP, HEAD, TOK)
        w_send[...] = wp[...].astype(BF16)
        for p in reversed(range(1, Z)):
            z_weight(p).start()

    def z_grads(p):
        there = opposite(p)
        return remote(
            zs_send.at[pl.ds(4 * p, 4)], zr_buf.at[pl.ds(4 * there, 4)], dz_ss.at[p], dz_rs.at[there], at_z(p)
        )

    def relay(p, o):
        n = p * 4 + o
        term = dsel[tab[T_OWN, n]] + dsel[tab[T_OWN + 1, n]]
        for d in range(1, X):
            mine = (d - 1) * Z + p
            t = T_FWD + (d - 1) * 2
            first = tab[t, p] == o
            used = first | (tab[t + 1, p] == o)
            if p == 0:
                used = used & (column(d) > x)
            slot = jnp.where(first, rbuf[2 * mine], rbuf[2 * mine + 1]).astype(F32)
            term += jnp.where(used, slot, 0.0)
        return term

    with jax.named_scope("relay"):
        for p in reversed(range(1, Z)):
            @pl.when(row(p) < z)
            def _(p=p):
                for d in range(1, X):
                    x_grads_in(p, d).wait_recv()
                for o in range(4):
                    zs_send[p * 4 + o] = relay(p, o).astype(BF16)
                z_grads(p).start()

        for d in range(1, X):
            pl.when(column(d) > x)(x_grads_in(0, d).wait_recv)
        for o in range(4):
            acc[o] = relay(0, o)
    with jax.named_scope("wfin"):
        w = wp[z]
        for p in range(1, Z):
            z_weight(p).wait_recv()
        for p in range(1, Z):
            w += w_recv[p].astype(F32)
        w_out[...] = w
    with jax.named_scope("dzwait"):
        for p in range(1, Z):
            @pl.when(row(p) > z)
            def _(p=p):
                remote(
                    zs_send.at[pl.ds(4 * p, 4)], zr_buf.at[pl.ds(4 * p, 4)], dz_ss.at[p], dz_rs.at[p], at_z(p)
                ).wait_recv()
                acc[...] += zr_buf[4 * p : 4 * p + 4].astype(F32)
        both = acc[...].reshape(TOK, 128).T
        dk_out[...] = (both[:HEAD] * SCALE).astype(BF16)
        dv_out[...] = both[HEAD:].astype(BF16)
    with jax.named_scope("sentwait"):
        for hop, up in HOPS:
            for f in range(2):
                pl.when(z_sends(hop, up))(z_keys(hop, f, up).wait_send)
        for p in range(1, Z):
            pl.when(row(p) < z)(z_grads(p).wait_send)
            z_weight(p).wait_send()
            @pl.when(row(p) < z)
            def _(p=p):
                for d in range(1, X):
                    x_keys(p, d).wait_send()
                    x_grads(p, d).wait_send()
        for d in range(1, X):
            pl.when(column(d) > x)(x_keys(0, d).wait_send)
            pl.when(column(d) < x)(x_grads(0, d).wait_send)
            x_inputs(d).wait_send()
            for r, hp in units:
                x_dq(r, hp, d).wait_send()
        for d in range(1, TP):
            tp_inputs(d).wait_send()


def body(inputs, queries, key_vectors, value_rows_by_head, out_grad, chosen):
    dma = pltpu.SemaphoreType.DMA
    vmem = pl.BlockSpec(memory_space=pltpu.VMEM)
    dq, dk, dv, w = pl.pallas_call(
        kernel,
        out_shape=(
            jax.ShapeDtypeStruct((TOK, GROUP * HEAD), BF16),
            jax.ShapeDtypeStruct((HEAD, TOK), BF16),
            jax.ShapeDtypeStruct((HEAD, TOK), BF16),
            jax.ShapeDtypeStruct((HEAD, GROUP * HEAD), F32),
        ),
        in_specs=[vmem] * 6,
        out_specs=(vmem,) * 4,
        scratch_shapes=[
            pltpu.VMEM((T_ROWS, 128), jnp.int32),
            pltpu.SMEM((T_ROWS, 128), jnp.int32),
            pltpu.VMEM((32 + 48, KB, 128), BF16),
            pltpu.VMEM((48, KB, 128), BF16),
            pltpu.VMEM((X, HEAD, TOK), BF16),
            pltpu.VMEM((HEAD, X * TOK), BF16),
            pltpu.VMEM((TP, HEAD, X * TOK), BF16),
            pltpu.VMEM((NSEL * KB, 128), BF16),
            pltpu.VMEM((2 * QB, 128), BF16),
            pltpu.VMEM((2 * QB, 128), BF16),
            pltpu.VMEM((NSEL * KB, 2 * QB), F32),
            pltpu.VMEM((NSEL * KB, 2 * QB), F32),
            pltpu.VMEM((NSEL * KB, 2 * QB), BF16),
            pltpu.VMEM((NSEL * KB, 2 * QB), BF16),
            pltpu.VMEM((2 * NSEL + 1, KB, 128), F32),
            pltpu.VMEM((48, KB, 128), BF16),
            pltpu.VMEM((48, KB, 128), BF16),
            pltpu.VMEM((4, KB, 128), F32),
            pltpu.VMEM((32, KB, 128), BF16),
            pltpu.VMEM((32, KB, 128), BF16),
            pltpu.VMEM((X * TOK, GROUP * HEAD), BF16),
            pltpu.VMEM((TP, HEAD, TOK), F32),
            pltpu.VMEM((TP, HEAD, TOK), BF16),
            pltpu.VMEM((Z, HEAD, TOK), BF16),
            dma,
            dma((2 * Z,)), dma((2 * Z,)),
            dma((24,)), dma((24,)),
            dma((X,)), dma((X,)),
            dma((TP,)), dma((TP,)),
            dma((4 * X,)), dma((4 * X,)),
            dma((24,)), dma((24,)),
            dma((Z,)), dma((Z,)),
            dma((Z,)), dma((Z,)),
        ],
        compiler_params=pltpu.CompilerParams(
            collective_id=0, has_side_effects=True, vmem_limit_bytes=60000 * 1024
        ),
        name="fused_backward",
    )(chosen.T, inputs, queries, key_vectors.T, value_rows_by_head.T, out_grad)
    return dq, dk.T, dv.T, w


def solution(mesh):
    spec = P("kv", "tp")
    return jax.shard_map(
        body, mesh=mesh, in_specs=(spec,) * 5 + (P(),), out_specs=(spec,) * 4, check_vma=False
    )
```

```python
import functools

import jax
import jax.numpy as jnp
from jax import lax
from jax.experimental import pallas as pl
from jax.experimental.pallas import tpu as pltpu
from jax.sharding import PartitionSpec as P

HEAD = 64
QB = 128
KB = 64
NSEL = 16
Z, X, TP = 8, 4, 8
TOK = 256
SEQ = 8192
GROUP = 4
SCALE = HEAD**-0.5
ORDER = (0, 1, 7, 2, 6, 3, 5, 4)
PLACE = {d: p for p, d in enumerate(ORDER)}
NEG = -1e30
PARTS = 4
SIZE = 4 // PARTS
LEAVE = (7, 5, 6, 3, 4, 1, 2, 0)
MESH = pl.DeviceIdType.MESH
F32, BF16 = jnp.float32, jnp.bfloat16
ZERO_D = 2 * NSEL
T_FWD, T_SEND, T_OWN, T_LOC, T_BLK, T_ROWS = 0, 6, 18, 20, 21, 24


def place_of(distance):
    near = jnp.where(distance < 4, 2 * distance - 1, jnp.where(distance == 4, 7, 2 * (8 - distance)))
    return jnp.where(distance == 0, 0, near)


def fill_table(table, chosen_t, z, x):
    by_row = chosen_t[...]
    lane_r = lax.broadcasted_iota(jnp.int32, by_row.shape, 1)

    def column(d, e):
        row = z * 2 * X + 2 * lax.rem(x + d, X) + e
        return jnp.sum(jnp.where(lane_r == row, by_row, 0), axis=1, keepdims=True)

    cols = [[column(d, e) for e in range(2)] for d in range(X)]
    lane = lax.broadcasted_iota(jnp.int32, (1, 128), 1)
    sub = lax.broadcasted_iota(jnp.int32, (NSEL, 128), 0)

    def row_of_place(place):
        half = (place + 1) >> 1
        d = jnp.where((place & 1) == 1, half, Z - half)
        d = jnp.where(place == 7, 4, d)
        return (z + d) & 7

    def two_used(pair, base):
        low, high = 3, 0
        for col in pair:
            rel = col - base
            ok = (rel >= 0) & (rel < 4)
            low = jnp.minimum(low, jnp.min(jnp.where(ok, rel, 3), axis=0, keepdims=True))
            high = jnp.maximum(high, jnp.max(jnp.where(ok, rel, 0), axis=0, keepdims=True))
        return low, high

    def inverse(e, block):
        hit = cols[0][e] == block
        return jnp.min(jnp.where(hit, sub + NSEL * e, ZERO_D), axis=0, keepdims=True)

    at_place = row_of_place(lane & 7) * 16
    for d in range(1, X):
        low, high = two_used(cols[d], at_place + x * 4)
        n = (d - 1) * 2
        table[T_FWD + n : T_FWD + n + 1] = low
        table[T_FWD + n + 1 : T_FWD + n + 2] = high
        base = at_place + lax.rem(x + d, X) * 4
        for s, o in enumerate(two_used(cols[0], base)):
            for e in range(2):
                m = T_SEND + ((d - 1) * 2 + s) * 2 + e
                table[m : m + 1] = inverse(e, base + o)
    mine = row_of_place((lane >> 2) & 7) * 16 + x * 4 + (lane & 3)
    for e in range(2):
        table[T_OWN + e : T_OWN + e + 1] = inverse(e, mine)
    diag = sub == (lane & (NSEL - 1))
    flat = [jnp.sum(jnp.where(diag, cols[0][e], 0), axis=0, keepdims=True) for e in range(2)]
    block = jnp.where(lane < NSEL, flat[0], flat[1])
    owner, off = block >> 2, block & 3
    place = place_of(((owner >> 2) - z) & 7)
    dx = ((owner & 3) - x) & 3
    earlier = 0
    for e in range(2):
        same = ((cols[0][e] >> 2) == owner) & ((cols[0][e] & 3) < off)
        earlier = jnp.maximum(earlier, jnp.max(jnp.where(same, 1, 0), axis=0, keepdims=True))
    loc = jnp.where(dx == 0, place * 4 + off, 32 + ((dx - 1) * Z + place) * 2 + earlier)
    table[T_LOC : T_LOC + 1] = jnp.where(owner > z * X + x, 0, loc)
    table[T_BLK : T_BLK + 1] = block


def kernel(
    chosen_h, in_h, q_h, k_h, v_h, g_h,
    dq_out, dk_out, dv_out, w_out,
    chosen_t, in_ref, q_ref, k_ref, v_ref, g_ref, tab_v, tab, kvt, xsel, in_t, xt, at, kvs, qp, gp, s_scr, pg_scr, p_scr, ds_scr,
    dsel, dxs, rbuf, acc, zs_send, zr_buf, dqg, wp, w_send, w_recv,
    t_sem, h_sem, z_ss, z_rs, x_ss, x_rs, i_ss, i_rs, y_ss, y_rs, dq_ss, dq_rs, dx_ss, dx_rs, w_ss, w_rs, dz_ss, dz_rs,
):
    kv, tp = lax.axis_index("kv"), lax.axis_index("tp")
    z, x = kv // X, lax.rem(kv, X)

    def row(p):
        return lax.rem(z + ORDER[p], Z)

    def at_z(p):
        return (row(p) * X + x, tp)

    def at_x(d):
        return (z * X + lax.rem(x + d, X), tp)

    def at_tp(d):
        return (kv, lax.rem(tp + d, TP))

    def remote(src, dst, ss, rs, dev):
        return pltpu.make_async_remote_copy(
            src_ref=src, dst_ref=dst, send_sem=ss, recv_sem=rs, device_id=dev, device_id_type=MESH
        )

    def opposite(p):
        return PLACE[(Z - ORDER[p]) % Z]

    def column(d):
        return lax.rem(x + d, X)

    with jax.named_scope("bar"):
        barrier = pltpu.get_barrier_semaphore()
        peers = [at_z(p) for p in range(1, Z)] + [at_x(d) for d in range(1, X)] + [at_tp(d) for d in range(1, TP)]
        for dev in peers:
            pl.semaphore_signal(barrier, inc=1, device_id=dev, device_id_type=MESH)
        loads = [(k_h, k_ref), (v_h, v_ref), (chosen_h, chosen_t), (in_h, in_ref), (q_h, q_ref), (g_h, g_ref)]
        loads = [pltpu.make_async_copy(src, dst, h_sem.at[n]) for n, (src, dst) in enumerate(loads)]
        for c in loads:
            c.start()
        for c in loads[:4]:
            c.wait()
        kvt[0:4] = jnp.concatenate([k_ref[...], v_ref[...]], axis=0).T.reshape(4, KB, 128)
        in_t[...] = in_ref[...].T.reshape(X, HEAD, TOK)
        fill_table(tab_v, chosen_t, z, x)
        dsel[ZERO_D] = jnp.zeros((KB, 128), F32)
        t_copy = pltpu.make_async_copy(tab_v, tab, t_sem)
        t_copy.start()
        xt[:, 0:TOK] = in_t[x]
        for c in loads[4:]:
            c.wait()
        pl.semaphore_wait(barrier, len(peers))

    def z_keys(hop, f, up):
        here = 0 if hop == 1 else PLACE[Z + 1 - hop if up else hop - 1]
        there = PLACE[Z - hop if up else hop]
        n = PARTS * there + f
        to = (lax.rem(z + (1 if up else Z - 1), Z) * X + x, tp)
        return remote(
            kvt.at[pl.ds(4 * here + SIZE * f, SIZE)], kvt.at[pl.ds(4 * there + SIZE * f, SIZE)], z_ss.at[n], z_rs.at[n], to
        )

    def z_sends(hop, up):
        if up:
            return (z >= hop - 1) & (z < Z - 1)
        return lax.rem(z + hop - 1, Z) <= Z - 6

    def z_gets(hop, up):
        if up:
            return z >= hop
        return lax.rem(z + hop, Z) <= Z - 6

    HOPS = [(hop, up) for hop in range(1, 5) for up in (True, False) if up or hop < 4]
    for f in range(PARTS):
        for up in (True, False):
            pl.when(z_sends(1, up))(z_keys(1, f, up).start)

    def x_inputs(d):
        return remote(
            in_t.at[column(d)], xt.at[:, pl.ds((X - d) * TOK, TOK)], i_ss.at[d], i_rs.at[X - d], at_x(d)
        )

    def tp_inputs(d):
        return remote(xt, at.at[tp], y_ss.at[d], y_rs.at[TP - d], at_tp(d))

    def x_keys(p, d):
        mine, there = ((d - 1) * Z + p) * 2, 32 + ((X - d - 1) * Z + p) * 2
        return remote(
            xsel.at[pl.ds(mine, 2)], kvt.at[pl.ds(there, 2)],
            x_ss.at[(d - 1) * Z + p], x_rs.at[(X - d - 1) * Z + p], at_x(d),
        )

    def x_keys_in(p, d):
        there = 32 + ((d - 1) * Z + p) * 2
        n = (d - 1) * Z + p
        return remote(xsel.at[pl.ds(2 * n, 2)], kvt.at[pl.ds(there, 2)], x_ss.at[n], x_rs.at[n], at_x(d))

    def forward(p):
        four = [kvt[4 * p + o] for o in range(4)]
        for d in range(1, X):
            for s in range(2):
                o = tab[T_FWD + (d - 1) * 2 + s, p]
                low = jnp.where(o == 0, four[0], four[1])
                high = jnp.where(o == 2, four[2], four[3])
                xsel[((d - 1) * Z + p) * 2 + s] = jnp.where(o < 2, low, high)
        for d in range(1, X):
            if p > 0:
                x_keys(p, d).start()
            else:
                pl.when(column(d) > x)(x_keys(p, d).start)

    with jax.named_scope("sel"):
        t_copy.wait()
        forward(0)
        for d in range(1, X):
            x_inputs(d).start()
        for hop, up in HOPS:
            @pl.when(z_gets(hop, up))
            def _(hop=hop, up=up):
                for f in range(PARTS):
                    z_keys(hop, f, up).wait_recv()
                    if hop < (4 if up else 3):
                        pl.when(z_sends(hop + 1, up))(z_keys(hop + 1, f, up).start)
            p = PLACE[Z - hop if up else hop]
            pl.when(row(p) < z)(functools.partial(forward, p))
            if hop == 1 and not up:
                for d in range(1, X):
                    x_inputs(d).wait_recv()
                for d in range(1, TP):
                    tp_inputs(d).start()
                at[tp] = xt[...]
    with jax.named_scope("xwait"):
        for p in range(1, Z):
            @pl.when(row(p) < z)
            def _(p=p):
                for d in range(1, X):
                    x_keys_in(p, d).wait_recv()
        for d in range(1, X):
            pl.when(column(d) < x)(x_keys_in(0, d).wait_recv)

    lanes = 2 * QB
    lane_t = lax.broadcasted_iota(jnp.int32, (KB, lanes), 1) % QB
    diff = lax.broadcasted_iota(jnp.int32, (KB, lanes), 0) - lane_t
    zeros = jnp.zeros((QB, HEAD), BF16)
    nt = (((1,), (1,)), ((), ()))
    nn = (((1,), (0,)), ((), ()))

    def fold(t, op):
        return op(t.reshape(KB // 8, 8, lanes), axis=0)

    def x_dq(r, hp, d):
        cols = pl.ds(hp * 2 * HEAD, 2 * HEAD)
        n = (r * 2 + hp) * X
        return remote(
            dqg.at[pl.ds(r * QB, QB), cols], dqg.at[pl.ds((X - d) * TOK + r * QB, QB), cols],
            dq_ss.at[n + d], dq_rs.at[n + X - d], at_x(d),
        )

    units = [(r, hp) for r in range(2) for hp in range(2)]
    for r, hp in units:
        scope = jax.named_scope(f"attn{r}{hp}")
        scope.__enter__()
        rows = pl.ds(r * QB, QB)
        if hp == 0:
            for j in range(NSEL):
                kvs[j * KB : (j + 1) * KB, :] = kvt[tab[T_LOC, r * NSEL + j]]
        for h in range(2):
            cols = slice((hp * 2 + h) * HEAD, (hp * 2 + h + 1) * HEAD)
            qp[h * QB : (h + 1) * QB, :] = jnp.concatenate([q_ref[rows, cols], zeros], axis=1)
            gp[h * QB : (h + 1) * QB, :] = jnp.concatenate([zeros, g_ref[rows, cols]], axis=1)
        s_scr[...] = lax.dot_general(kvs[...], qp[...], nt, preferred_element_type=F32)
        pg_scr[...] = lax.dot_general(kvs[...], gp[...], nt, preferred_element_type=F32)

        def mask_step(j, m):
            at_j = pl.ds(pl.multiple_of(j * KB, KB), KB)
            limit = kv * TOK + r * QB - tab[T_BLK, r * NSEL + j] * KB
            s = jnp.where(diff <= limit, s_scr[at_j, :] * SCALE, NEG)
            s_scr[at_j, :] = s
            return jnp.maximum(m, fold(s, jnp.max))

        m = lax.fori_loop(0, NSEL, mask_step, jnp.full((8, lanes), NEG, F32), unroll=4)
        m = jnp.max(m, axis=0, keepdims=True)

        def exp_step(j, total):
            at_j = pl.ds(pl.multiple_of(j * KB, KB), KB)
            e = jnp.exp(s_scr[at_j, :] - m)
            s_scr[at_j, :] = e
            return total + fold(e, jnp.sum)

        total = lax.fori_loop(0, NSEL, exp_step, jnp.zeros((8, lanes), F32), unroll=4)
        inv = 1.0 / jnp.sum(total, axis=0, keepdims=True)

        def half_step(j, dot):
            at_j = pl.ds(pl.multiple_of(j * KB, KB), KB)
            half = (s_scr[at_j, :] * inv).astype(BF16)
            p_scr[at_j, :] = half
            return dot + fold(half.astype(F32) * pg_scr[at_j, :], jnp.sum)

        dot = lax.fori_loop(0, NSEL, half_step, jnp.zeros((8, lanes), F32), unroll=4)
        dot = jnp.sum(dot, axis=0, keepdims=True)

        def grad_step(j, carry):
            at_j = pl.ds(pl.multiple_of(j * KB, KB), KB)
            ds_scr[at_j, :] = ((s_scr[at_j, :] * inv) * (pg_scr[at_j, :] - dot)).astype(BF16)
            return carry

        lax.fori_loop(0, NSEL, grad_step, 0, unroll=4)
        dq_t = lax.dot_general(kvs[...].T[:HEAD], ds_scr[...], nn, preferred_element_type=F32) * SCALE
        stacked = jnp.concatenate([dq_t[:, :QB], dq_t[:, QB:]], axis=0)
        dqg[rows, hp * 2 * HEAD : (hp + 1) * 2 * HEAD] = stacked.T.astype(BF16)
        dkv = lax.dot_general(ds_scr[...], qp[...], nn, preferred_element_type=F32)
        dkv += lax.dot_general(p_scr[...], gp[...], nn, preferred_element_type=F32)
        if hp == 0:
            dsel[pl.ds(r * NSEL, NSEL)] = dkv.reshape(NSEL, KB, 128)
        else:
            dsel[pl.ds(r * NSEL, NSEL)] += dkv.reshape(NSEL, KB, 128)
        for d in range(1, X):
            x_dq(r, hp, d).start()
        scope.__exit__(None, None, None)
    dq_out[...] = dqg[0:TOK, :]

    def x_grads(p, d):
        mine, there = (d - 1) * Z + p, (X - d - 1) * Z + p
        return remote(
            dxs.at[pl.ds(2 * mine, 2)], rbuf.at[pl.ds(2 * there, 2)], dx_ss.at[mine], dx_rs.at[there], at_x(d)
        )

    def x_grads_in(p, d):
        mine = (d - 1) * Z + p
        return remote(
            dxs.at[pl.ds(2 * mine, 2)], rbuf.at[pl.ds(2 * mine, 2)], dx_ss.at[mine], dx_rs.at[mine], at_x(d)
        )

    with jax.named_scope("dxsend"):
        for p in LEAVE:
            @pl.when(row(p) <= z)
            def _(p=p):
                for d in range(1, X):
                    for s in range(2):
                        t = T_SEND + ((d - 1) * 2 + s) * 2
                        dxs[((d - 1) * Z + p) * 2 + s] = (dsel[tab[t, p]] + dsel[tab[t + 1, p]]).astype(BF16)
                for d in range(1, X):
                    if p > 0:
                        x_grads(p, d).start()
                    else:
                        pl.when(column(d) < x)(x_grads(p, d).start)

    def z_weight(p):
        there = opposite(p)
        return remote(w_send.at[row(p)], w_recv.at[there], w_ss.at[p], w_rs.at[there], at_z(p))

    with jax.named_scope("wgrad"):
        for d in range(1, TP):
            tp_inputs(d).wait_recv()
        for r, hp in units:
            for d in range(1, X):
                x_dq(r, hp, d).wait_recv()
        wp[...] = lax.dot_general(
            at[...].reshape(TP * HEAD, X * TOK), dqg[...], nn, preferred_element_type=F32
        ).reshape(TP, HEAD, TOK)
        w_send[...] = wp[...].astype(BF16)
        for p in reversed(range(1, Z)):
            z_weight(p).start()

    def z_copy(slot, step):
        return remote(
            zs_send.at[pl.ds(4 * slot, 4)], zr_buf.at[pl.ds(4 * slot, 4)], dz_ss.at[slot], dz_rs.at[slot],
            (lax.rem(z + step + Z, Z) * X + x, tp),
        )

    wraps = (z >= Z - 2) | (z == 0)
    returns = [
        (7, z >= 4, None, None, 0, -1),
        (5, z >= 5, None, None, 1, 1),
        (6, z >= 3, 0, (z >= 3) & (z <= 6), 2, -1),
        (3, wraps, 1, wraps, 3, 2),
        (4, z >= 2, 2, (z >= 2) & (z <= 6), 4, -2),
        (1, z == 7, None, None, 5, 1),
        (2, z >= 1, None, None, 6, -1),
    ]
    arrivals = [(3, z <= 2), (4, z <= 5), (5, z == 0), (6, z <= 6)]

    def relay(p, o):
        n = p * 4 + o
        term = dsel[tab[T_OWN, n]] + dsel[tab[T_OWN + 1, n]]
        for d in range(1, X):
            mine = (d - 1) * Z + p
            t = T_FWD + (d - 1) * 2
            first = tab[t, p] == o
            used = first | (tab[t + 1, p] == o)
            if p == 0:
                used = used & (column(d) > x)
            slot = jnp.where(first, rbuf[2 * mine], rbuf[2 * mine + 1]).astype(F32)
            term += jnp.where(used, slot, 0.0)
        return term

    with jax.named_scope("relay"):
        for p, sends, added, adds, slot, step in returns:
            @pl.when(sends)
            def _(p=p, added=added, adds=adds, slot=slot, step=step):
                @pl.when(row(p) < z)
                def _():
                    for d in range(1, X):
                        x_grads_in(p, d).wait_recv()

                if added is not None:
                    pl.when(adds)(z_copy(added, 0).wait_recv)
                for o in range(4):
                    term = jnp.where(row(p) < z, relay(p, o), 0.0)
                    if added is not None:
                        term += jnp.where(adds, zr_buf[added * 4 + o].astype(F32), 0.0)
                    zs_send[slot * 4 + o] = term.astype(BF16)
                z_copy(slot, step).start()

        for d in range(1, X):
            pl.when(column(d) > x)(x_grads_in(0, d).wait_recv)
        for o in range(4):
            acc[o] = relay(0, o)
    with jax.named_scope("wfin"):
        w = wp[z]
        for p in range(1, Z):
            z_weight(p).wait_recv()
        for p in range(1, Z):
            w += w_recv[p].astype(F32)
        w_out[...] = w
    with jax.named_scope("dzwait"):
        for slot, comes in arrivals:
            @pl.when(comes)
            def _(slot=slot):
                z_copy(slot, 0).wait_recv()
                acc[...] += zr_buf[4 * slot : 4 * slot + 4].astype(F32)
        both = acc[...].reshape(TOK, 128).T
        dk_out[...] = (both[:HEAD] * SCALE).astype(BF16)
        dv_out[...] = both[HEAD:].astype(BF16)
    with jax.named_scope("sentwait"):
        for hop, up in HOPS:
            for f in range(PARTS):
                pl.when(z_sends(hop, up))(z_keys(hop, f, up).wait_send)
        for p in range(1, Z):
            z_weight(p).wait_send()
            @pl.when(row(p) < z)
            def _(p=p):
                for d in range(1, X):
                    x_keys(p, d).wait_send()
                    x_grads(p, d).wait_send()
        for d in range(1, X):
            pl.when(column(d) > x)(x_keys(0, d).wait_send)
            pl.when(column(d) < x)(x_grads(0, d).wait_send)
            x_inputs(d).wait_send()
            for r, hp in units:
                x_dq(r, hp, d).wait_send()
        for d in range(1, TP):
            tp_inputs(d).wait_send()
        for p, sends, added, adds, slot, step in returns:
            pl.when(sends)(z_copy(slot, step).wait_send)


def body(inputs, queries, key_vectors, value_rows_by_head, out_grad, chosen):
    dma = pltpu.SemaphoreType.DMA
    vmem = pl.BlockSpec(memory_space=pltpu.VMEM)
    dq, dk, dv, w = pl.pallas_call(
        kernel,
        out_shape=(
            jax.ShapeDtypeStruct((TOK, GROUP * HEAD), BF16),
            jax.ShapeDtypeStruct((HEAD, TOK), BF16),
            jax.ShapeDtypeStruct((HEAD, TOK), BF16),
            jax.ShapeDtypeStruct((HEAD, GROUP * HEAD), F32),
        ),
        in_specs=[pl.BlockSpec(memory_space=pl.ANY)] * 6,
        out_specs=(vmem,) * 4,
        scratch_shapes=[
            pltpu.VMEM((NSEL, SEQ // QB), jnp.int32),
            pltpu.VMEM((TOK, TOK), BF16),
            pltpu.VMEM((TOK, GROUP * HEAD), BF16),
            pltpu.VMEM((HEAD, TOK), BF16),
            pltpu.VMEM((HEAD, TOK), BF16),
            pltpu.VMEM((TOK, GROUP * HEAD), BF16),
            pltpu.VMEM((T_ROWS, 128), jnp.int32),
            pltpu.SMEM((T_ROWS, 128), jnp.int32),
            pltpu.VMEM((32 + 48, KB, 128), BF16),
            pltpu.VMEM((48, KB, 128), BF16),
            pltpu.VMEM((X, HEAD, TOK), BF16),
            pltpu.VMEM((HEAD, X * TOK), BF16),
            pltpu.VMEM((TP, HEAD, X * TOK), BF16),
            pltpu.VMEM((NSEL * KB, 128), BF16),
            pltpu.VMEM((2 * QB, 128), BF16),
            pltpu.VMEM((2 * QB, 128), BF16),
            pltpu.VMEM((NSEL * KB, 2 * QB), F32),
            pltpu.VMEM((NSEL * KB, 2 * QB), F32),
            pltpu.VMEM((NSEL * KB, 2 * QB), BF16),
            pltpu.VMEM((NSEL * KB, 2 * QB), BF16),
            pltpu.VMEM((2 * NSEL + 1, KB, 128), F32),
            pltpu.VMEM((48, KB, 128), BF16),
            pltpu.VMEM((48, KB, 128), BF16),
            pltpu.VMEM((4, KB, 128), F32),
            pltpu.VMEM((28, KB, 128), BF16),
            pltpu.VMEM((28, KB, 128), BF16),
            pltpu.VMEM((X * TOK, GROUP * HEAD), BF16),
            pltpu.VMEM((TP, HEAD, TOK), F32),
            pltpu.VMEM((TP, HEAD, TOK), BF16),
            pltpu.VMEM((Z, HEAD, TOK), BF16),
            dma,
            dma((6,)),
            dma((PARTS * Z,)), dma((PARTS * Z,)),
            dma((24,)), dma((24,)),
            dma((X,)), dma((X,)),
            dma((TP,)), dma((TP,)),
            dma((4 * X,)), dma((4 * X,)),
            dma((24,)), dma((24,)),
            dma((Z,)), dma((Z,)),
            dma((Z,)), dma((Z,)),
        ],
        compiler_params=pltpu.CompilerParams(
            collective_id=0, has_side_effects=True, vmem_limit_bytes=60000 * 1024
        ),
        name="fused_backward",
    )(chosen.T, inputs, queries, key_vectors.T, value_rows_by_head.T, out_grad)
    return dq, dk.T, dv.T, w


def solution(mesh):
    spec = P("kv", "tp")
    return jax.shard_map(
        body, mesh=mesh, in_specs=(spec,) * 5 + (P(),), out_specs=(spec,) * 4, check_vma=False
    )
```

```python
import functools

import jax
import jax.numpy as jnp
from jax import lax
from jax.experimental import pallas as pl
from jax.experimental.pallas import tpu as pltpu
from jax.sharding import PartitionSpec as P

HEAD = 64
QB = 128
KB = 64
NSEL = 16
Z, X, TP = 8, 4, 8
TOK = 256
SEQ = 8192
GROUP = 4
SCALE = HEAD**-0.5
ORDER = (0, 1, 7, 2, 6, 3, 5, 4)
PLACE = {d: p for p, d in enumerate(ORDER)}
NEG = -1e30
PARTS = 4
SIZE = 4 // PARTS
LEAVE = (7, 5, 6, 3, 4, 1, 2, 0)
MESH = pl.DeviceIdType.MESH
F32, BF16 = jnp.float32, jnp.bfloat16
ZERO_D = 2 * NSEL
T_FWD, T_SEND, T_OWN, T_LOC, T_BLK, T_ROWS = 0, 6, 18, 20, 21, 24


def place_of(distance):
    near = jnp.where(distance < 4, 2 * distance - 1, jnp.where(distance == 4, 7, 2 * (8 - distance)))
    return jnp.where(distance == 0, 0, near)


def fill_table(table, chosen_t, z, x):
    by_row = chosen_t[...]
    lane_r = lax.broadcasted_iota(jnp.int32, by_row.shape, 1)

    def column(d, e):
        row = z * 2 * X + 2 * lax.rem(x + d, X) + e
        return jnp.sum(jnp.where(lane_r == row, by_row, 0), axis=1, keepdims=True)

    cols = [[column(d, e) for e in range(2)] for d in range(X)]
    lane = lax.broadcasted_iota(jnp.int32, (1, 128), 1)
    sub = lax.broadcasted_iota(jnp.int32, (NSEL, 128), 0)

    def row_of_place(place):
        half = (place + 1) >> 1
        d = jnp.where((place & 1) == 1, half, Z - half)
        d = jnp.where(place == 7, 4, d)
        return (z + d) & 7

    def two_used(pair, base):
        low, high = 3, 0
        for col in pair:
            rel = col - base
            ok = (rel >= 0) & (rel < 4)
            low = jnp.minimum(low, jnp.min(jnp.where(ok, rel, 3), axis=0, keepdims=True))
            high = jnp.maximum(high, jnp.max(jnp.where(ok, rel, 0), axis=0, keepdims=True))
        return low, high

    def inverse(e, block):
        hit = cols[0][e] == block
        return jnp.min(jnp.where(hit, sub + NSEL * e, ZERO_D), axis=0, keepdims=True)

    at_place = row_of_place(lane & 7) * 16
    for d in range(1, X):
        low, high = two_used(cols[d], at_place + x * 4)
        n = (d - 1) * 2
        table[T_FWD + n : T_FWD + n + 1] = low
        table[T_FWD + n + 1 : T_FWD + n + 2] = high
        base = at_place + lax.rem(x + d, X) * 4
        for s, o in enumerate(two_used(cols[0], base)):
            for e in range(2):
                m = T_SEND + ((d - 1) * 2 + s) * 2 + e
                table[m : m + 1] = inverse(e, base + o)
    mine = row_of_place((lane >> 2) & 7) * 16 + x * 4 + (lane & 3)
    for e in range(2):
        table[T_OWN + e : T_OWN + e + 1] = inverse(e, mine)
    diag = sub == (lane & (NSEL - 1))
    flat = [jnp.sum(jnp.where(diag, cols[0][e], 0), axis=0, keepdims=True) for e in range(2)]
    block = jnp.where(lane < NSEL, flat[0], flat[1])
    owner, off = block >> 2, block & 3
    place = place_of(((owner >> 2) - z) & 7)
    dx = ((owner & 3) - x) & 3
    earlier = 0
    for e in range(2):
        same = ((cols[0][e] >> 2) == owner) & ((cols[0][e] & 3) < off)
        earlier = jnp.maximum(earlier, jnp.max(jnp.where(same, 1, 0), axis=0, keepdims=True))
    loc = jnp.where(dx == 0, place * 4 + off, 32 + ((dx - 1) * Z + place) * 2 + earlier)
    table[T_LOC : T_LOC + 1] = jnp.where(owner > z * X + x, 0, loc)
    table[T_BLK : T_BLK + 1] = block


def kernel(
    chosen_h, in_h, q_h, k_h, v_h, g_h,
    dq_out, dk_out, dv_out, w_out,
    chosen_t, in_ref, q_ref, k_ref, v_ref, g_ref, tab_v, tab, kvt, xsel, in_t, xt, at, kvs, kst, qg, sg_scr, sp_scr,
    dsel, dxs, rbuf, acc, zs_send, zr_buf, dqg, wp, w_send, w_recv,
    t_sem, h_sem, z_ss, z_rs, x_ss, x_rs, i_ss, i_rs, y_ss, y_rs, dq_ss, dq_rs, dx_ss, dx_rs, w_ss, w_rs, dz_ss, dz_rs,
):
    kv, tp = lax.axis_index("kv"), lax.axis_index("tp")
    z, x = kv // X, lax.rem(kv, X)

    def row(p):
        return lax.rem(z + ORDER[p], Z)

    def at_z(p):
        return (row(p) * X + x, tp)

    def at_x(d):
        return (z * X + lax.rem(x + d, X), tp)

    def at_tp(d):
        return (kv, lax.rem(tp + d, TP))

    def remote(src, dst, ss, rs, dev):
        return pltpu.make_async_remote_copy(
            src_ref=src, dst_ref=dst, send_sem=ss, recv_sem=rs, device_id=dev, device_id_type=MESH
        )

    def opposite(p):
        return PLACE[(Z - ORDER[p]) % Z]

    def column(d):
        return lax.rem(x + d, X)

    with jax.named_scope("bar"):
        barrier = pltpu.get_barrier_semaphore()
        peers = [at_z(p) for p in range(1, Z)] + [at_x(d) for d in range(1, X)] + [at_tp(d) for d in range(1, TP)]
        for dev in peers:
            pl.semaphore_signal(barrier, inc=1, device_id=dev, device_id_type=MESH)
        loads = [(k_h, k_ref), (v_h, v_ref), (chosen_h, chosen_t), (in_h, in_ref), (q_h, q_ref), (g_h, g_ref)]
        loads = [pltpu.make_async_copy(src, dst, h_sem.at[n]) for n, (src, dst) in enumerate(loads)]
        for c in loads:
            c.start()
        for c in loads[:4]:
            c.wait()
        kvt[0:4] = jnp.concatenate([k_ref[...], v_ref[...]], axis=0).T.reshape(4, KB, 128)
        in_t[...] = in_ref[...].T.reshape(X, HEAD, TOK)
        fill_table(tab_v, chosen_t, z, x)
        dsel[ZERO_D] = jnp.zeros((KB, 128), F32)
        t_copy = pltpu.make_async_copy(tab_v, tab, t_sem)
        t_copy.start()
        xt[:, 0:TOK] = in_t[x]
        for c in loads[4:]:
            c.wait()
        pl.semaphore_wait(barrier, len(peers))

    def z_keys(hop, f, up):
        here = 0 if hop == 1 else PLACE[Z + 1 - hop if up else hop - 1]
        there = PLACE[Z - hop if up else hop]
        n = PARTS * there + f
        to = (lax.rem(z + (1 if up else Z - 1), Z) * X + x, tp)
        return remote(
            kvt.at[pl.ds(4 * here + SIZE * f, SIZE)], kvt.at[pl.ds(4 * there + SIZE * f, SIZE)], z_ss.at[n], z_rs.at[n], to
        )

    def z_sends(hop, up):
        if up:
            return (z >= hop - 1) & (z < Z - 1)
        return lax.rem(z + hop - 1, Z) <= Z - 6

    def z_gets(hop, up):
        if up:
            return z >= hop
        return lax.rem(z + hop, Z) <= Z - 6

    HOPS = [(hop, up) for hop in range(1, 5) for up in (True, False) if up or hop < 4]
    for f in range(PARTS):
        for up in (True, False):
            pl.when(z_sends(1, up))(z_keys(1, f, up).start)

    def x_inputs(d):
        return remote(
            in_t.at[column(d)], xt.at[:, pl.ds((X - d) * TOK, TOK)], i_ss.at[d], i_rs.at[X - d], at_x(d)
        )

    def tp_inputs(d):
        return remote(xt, at.at[tp], y_ss.at[d], y_rs.at[TP - d], at_tp(d))

    def x_keys(p, d):
        mine, there = ((d - 1) * Z + p) * 2, 32 + ((X - d - 1) * Z + p) * 2
        return remote(
            xsel.at[pl.ds(mine, 2)], kvt.at[pl.ds(there, 2)],
            x_ss.at[(d - 1) * Z + p], x_rs.at[(X - d - 1) * Z + p], at_x(d),
        )

    def x_keys_in(p, d):
        there = 32 + ((d - 1) * Z + p) * 2
        n = (d - 1) * Z + p
        return remote(xsel.at[pl.ds(2 * n, 2)], kvt.at[pl.ds(there, 2)], x_ss.at[n], x_rs.at[n], at_x(d))

    def forward(p):
        four = [kvt[4 * p + o] for o in range(4)]
        for d in range(1, X):
            for s in range(2):
                o = tab[T_FWD + (d - 1) * 2 + s, p]
                low = jnp.where(o == 0, four[0], four[1])
                high = jnp.where(o == 2, four[2], four[3])
                xsel[((d - 1) * Z + p) * 2 + s] = jnp.where(o < 2, low, high)
        for d in range(1, X):
            if p > 0:
                x_keys(p, d).start()
            else:
                pl.when(column(d) > x)(x_keys(p, d).start)

    with jax.named_scope("sel"):
        t_copy.wait()
        forward(0)
        for d in range(1, X):
            x_inputs(d).start()
        for hop, up in HOPS:
            @pl.when(z_gets(hop, up))
            def _(hop=hop, up=up):
                for f in range(PARTS):
                    z_keys(hop, f, up).wait_recv()
                    if hop < (4 if up else 3):
                        pl.when(z_sends(hop + 1, up))(z_keys(hop + 1, f, up).start)
            p = PLACE[Z - hop if up else hop]
            pl.when(row(p) < z)(functools.partial(forward, p))
            if hop == 1 and not up:
                for d in range(1, X):
                    x_inputs(d).wait_recv()
                for d in range(1, TP):
                    tp_inputs(d).start()
                at[tp] = xt[...]
    with jax.named_scope("xwait"):
        for p in range(1, Z):
            @pl.when(row(p) < z)
            def _(p=p):
                for d in range(1, X):
                    x_keys_in(p, d).wait_recv()
        for d in range(1, X):
            pl.when(column(d) < x)(x_keys_in(0, d).wait_recv)

    lanes = 2 * QB
    lane_t = lax.broadcasted_iota(jnp.int32, (KB, lanes), 1) % QB
    diff = lax.broadcasted_iota(jnp.int32, (KB, lanes), 0) - lane_t
    zeros = jnp.zeros((QB, HEAD), BF16)
    nt = (((1,), (1,)), ((), ()))
    nn = (((1,), (0,)), ((), ()))

    def fold(t, op):
        return op(t.reshape(KB // 8, 8, lanes), axis=0)

    def x_dq(r, hp, d):
        cols = pl.ds(hp * 2 * HEAD, 2 * HEAD)
        n = (r * 2 + hp) * X
        return remote(
            dqg.at[pl.ds(r * QB, QB), cols], dqg.at[pl.ds((X - d) * TOK + r * QB, QB), cols],
            dq_ss.at[n + d], dq_rs.at[n + X - d], at_x(d),
        )

    units = [(r, hp) for r in range(2) for hp in range(2)]
    for r, hp in units:
        scope = jax.named_scope(f"attn{r}{hp}")
        scope.__enter__()
        rows = pl.ds(r * QB, QB)
        if hp == 0:
            for j in range(NSEL):
                kvs[j * KB : (j + 1) * KB, :] = kvt[tab[T_LOC, r * NSEL + j]]
            kst[...] = kvs[...].T[:HEAD]
        first = r * 8 * QB + hp * 4 * QB
        for h in range(2):
            cols = slice((hp * 2 + h) * HEAD, (hp * 2 + h + 1) * HEAD)
            qg[first + h * QB : first + (h + 1) * QB, :] = jnp.concatenate([q_ref[rows, cols], zeros], axis=1)
            qg[first + (h + 2) * QB : first + (h + 3) * QB, :] = jnp.concatenate([zeros, g_ref[rows, cols]], axis=1)
        sg_scr[...] = lax.dot_general(kvs[...], qg[first : first + 4 * QB], nt, preferred_element_type=F32)
        s_lanes, g_lanes = slice(0, lanes), slice(lanes, 2 * lanes)
        ds_lanes = slice(hp * 2 * lanes, hp * 2 * lanes + lanes)
        p_lanes = slice(hp * 2 * lanes + lanes, hp * 2 * lanes + 2 * lanes)

        def mask_step(j, m):
            at_j = pl.ds(pl.multiple_of(j * KB, KB), KB)
            limit = kv * TOK + r * QB - tab[T_BLK, r * NSEL + j] * KB
            s = jnp.where(diff <= limit, sg_scr[at_j, s_lanes] * SCALE, NEG)
            sg_scr[at_j, s_lanes] = s
            return jnp.maximum(m, fold(s, jnp.max))

        m = lax.fori_loop(0, NSEL, mask_step, jnp.full((8, lanes), NEG, F32), unroll=4)
        m = jnp.max(m, axis=0, keepdims=True)

        def exp_step(j, total):
            at_j = pl.ds(pl.multiple_of(j * KB, KB), KB)
            e = jnp.exp(sg_scr[at_j, s_lanes] - m)
            sg_scr[at_j, s_lanes] = e
            return total + fold(e, jnp.sum)

        total = lax.fori_loop(0, NSEL, exp_step, jnp.zeros((8, lanes), F32), unroll=4)
        inv = 1.0 / jnp.sum(total, axis=0, keepdims=True)

        def half_step(j, dot):
            at_j = pl.ds(pl.multiple_of(j * KB, KB), KB)
            half = (sg_scr[at_j, s_lanes] * inv).astype(BF16)
            sp_scr[r, at_j, p_lanes] = half
            return dot + fold(half.astype(F32) * sg_scr[at_j, g_lanes], jnp.sum)

        dot = lax.fori_loop(0, NSEL, half_step, jnp.zeros((8, lanes), F32), unroll=4)
        dot = jnp.sum(dot, axis=0, keepdims=True)

        def grad_step(j, carry):
            at_j = pl.ds(pl.multiple_of(j * KB, KB), KB)
            grad = (sg_scr[at_j, s_lanes] * inv) * (sg_scr[at_j, g_lanes] - dot)
            sp_scr[r, at_j, ds_lanes] = grad.astype(BF16)
            return carry

        lax.fori_loop(0, NSEL, grad_step, 0, unroll=4)
        dq_t = lax.dot_general(kst[...], sp_scr[r, :, ds_lanes], nn, preferred_element_type=F32) * SCALE
        stacked = jnp.concatenate([dq_t[:, :QB], dq_t[:, QB:]], axis=0)
        dqg[rows, hp * 2 * HEAD : (hp + 1) * 2 * HEAD] = stacked.T.astype(BF16)
        for d in range(1, X):
            x_dq(r, hp, d).start()
        scope.__exit__(None, None, None)
    with jax.named_scope("dkv"):
        for r in range(2):
            dkv = lax.dot_general(
                sp_scr[r], qg[r * 8 * QB : (r + 1) * 8 * QB], nn, preferred_element_type=F32
            )
            dsel[pl.ds(r * NSEL, NSEL)] = dkv.reshape(NSEL, KB, 128)
        dq_out[...] = dqg[0:TOK, :]

    def x_grads(p, d):
        mine, there = (d - 1) * Z + p, (X - d - 1) * Z + p
        return remote(
            dxs.at[pl.ds(2 * mine, 2)], rbuf.at[pl.ds(2 * there, 2)], dx_ss.at[mine], dx_rs.at[there], at_x(d)
        )

    def x_grads_in(p, d):
        mine = (d - 1) * Z + p
        return remote(
            dxs.at[pl.ds(2 * mine, 2)], rbuf.at[pl.ds(2 * mine, 2)], dx_ss.at[mine], dx_rs.at[mine], at_x(d)
        )

    with jax.named_scope("dxsend"):
        for p in LEAVE:
            @pl.when(row(p) <= z)
            def _(p=p):
                for d in range(1, X):
                    for s in range(2):
                        t = T_SEND + ((d - 1) * 2 + s) * 2
                        dxs[((d - 1) * Z + p) * 2 + s] = (dsel[tab[t, p]] + dsel[tab[t + 1, p]]).astype(BF16)
                for d in range(1, X):
                    if p > 0:
                        x_grads(p, d).start()
                    else:
                        pl.when(column(d) < x)(x_grads(p, d).start)

    def z_weight(p):
        there = opposite(p)
        return remote(w_send.at[row(p)], w_recv.at[there], w_ss.at[p], w_rs.at[there], at_z(p))

    with jax.named_scope("wgrad"):
        for d in range(1, TP):
            tp_inputs(d).wait_recv()
        for r, hp in units:
            for d in range(1, X):
                x_dq(r, hp, d).wait_recv()
        wp[...] = lax.dot_general(
            at[...].reshape(TP * HEAD, X * TOK), dqg[...], nn, preferred_element_type=F32
        ).reshape(TP, HEAD, TOK)
        w_send[...] = wp[...].astype(BF16)
        for p in reversed(range(1, Z)):
            z_weight(p).start()

    def z_copy(slot, step):
        return remote(
            zs_send.at[pl.ds(4 * slot, 4)], zr_buf.at[pl.ds(4 * slot, 4)], dz_ss.at[slot], dz_rs.at[slot],
            (lax.rem(z + step + Z, Z) * X + x, tp),
        )

    wraps = (z >= Z - 2) | (z == 0)
    returns = [
        (7, z >= 4, None, None, 0, -1),
        (5, z >= 5, None, None, 1, 1),
        (6, z >= 3, 0, (z >= 3) & (z <= 6), 2, -1),
        (3, wraps, 1, wraps, 3, 2),
        (4, z >= 2, 2, (z >= 2) & (z <= 6), 4, -2),
        (1, z == 7, None, None, 5, 1),
        (2, z >= 1, None, None, 6, -1),
    ]
    arrivals = [(3, z <= 2), (4, z <= 5), (5, z == 0), (6, z <= 6)]

    def relay(p, o):
        n = p * 4 + o
        term = dsel[tab[T_OWN, n]] + dsel[tab[T_OWN + 1, n]]
        for d in range(1, X):
            mine = (d - 1) * Z + p
            t = T_FWD + (d - 1) * 2
            first = tab[t, p] == o
            used = first | (tab[t + 1, p] == o)
            if p == 0:
                used = used & (column(d) > x)
            slot = jnp.where(first, rbuf[2 * mine], rbuf[2 * mine + 1]).astype(F32)
            term += jnp.where(used, slot, 0.0)
        return term

    with jax.named_scope("relay"):
        for p, sends, added, adds, slot, step in returns:
            @pl.when(sends)
            def _(p=p, added=added, adds=adds, slot=slot, step=step):
                @pl.when(row(p) < z)
                def _():
                    for d in range(1, X):
                        x_grads_in(p, d).wait_recv()

                if added is not None:
                    pl.when(adds)(z_copy(added, 0).wait_recv)
                for o in range(4):
                    term = jnp.where(row(p) < z, relay(p, o), 0.0)
                    if added is not None:
                        term += jnp.where(adds, zr_buf[added * 4 + o].astype(F32), 0.0)
                    zs_send[slot * 4 + o] = term.astype(BF16)
                z_copy(slot, step).start()

        for d in range(1, X):
            pl.when(column(d) > x)(x_grads_in(0, d).wait_recv)
        for o in range(4):
            acc[o] = relay(0, o)
    with jax.named_scope("wfin"):
        w = wp[z]
        for p in range(1, Z):
            z_weight(p).wait_recv()
        for p in range(1, Z):
            w += w_recv[p].astype(F32)
        w_out[...] = w
    with jax.named_scope("dzwait"):
        for slot, comes in arrivals:
            @pl.when(comes)
            def _(slot=slot):
                z_copy(slot, 0).wait_recv()
                acc[...] += zr_buf[4 * slot : 4 * slot + 4].astype(F32)
        both = acc[...].reshape(TOK, 128).T
        dk_out[...] = (both[:HEAD] * SCALE).astype(BF16)
        dv_out[...] = both[HEAD:].astype(BF16)
    with jax.named_scope("sentwait"):
        for hop, up in HOPS:
            for f in range(PARTS):
                pl.when(z_sends(hop, up))(z_keys(hop, f, up).wait_send)
        for p in range(1, Z):
            z_weight(p).wait_send()
            @pl.when(row(p) < z)
            def _(p=p):
                for d in range(1, X):
                    x_keys(p, d).wait_send()
                    x_grads(p, d).wait_send()
        for d in range(1, X):
            pl.when(column(d) > x)(x_keys(0, d).wait_send)
            pl.when(column(d) < x)(x_grads(0, d).wait_send)
            x_inputs(d).wait_send()
            for r, hp in units:
                x_dq(r, hp, d).wait_send()
        for d in range(1, TP):
            tp_inputs(d).wait_send()
        for p, sends, added, adds, slot, step in returns:
            pl.when(sends)(z_copy(slot, step).wait_send)


def body(inputs, queries, key_vectors, value_rows_by_head, out_grad, chosen):
    dma = pltpu.SemaphoreType.DMA
    vmem = pl.BlockSpec(memory_space=pltpu.VMEM)
    dq, dk, dv, w = pl.pallas_call(
        kernel,
        out_shape=(
            jax.ShapeDtypeStruct((TOK, GROUP * HEAD), BF16),
            jax.ShapeDtypeStruct((HEAD, TOK), BF16),
            jax.ShapeDtypeStruct((HEAD, TOK), BF16),
            jax.ShapeDtypeStruct((HEAD, GROUP * HEAD), F32),
        ),
        in_specs=[pl.BlockSpec(memory_space=pl.ANY)] * 6,
        out_specs=(vmem,) * 4,
        scratch_shapes=[
            pltpu.VMEM((NSEL, SEQ // QB), jnp.int32),
            pltpu.VMEM((TOK, TOK), BF16),
            pltpu.VMEM((TOK, GROUP * HEAD), BF16),
            pltpu.VMEM((HEAD, TOK), BF16),
            pltpu.VMEM((HEAD, TOK), BF16),
            pltpu.VMEM((TOK, GROUP * HEAD), BF16),
            pltpu.VMEM((T_ROWS, 128), jnp.int32),
            pltpu.SMEM((T_ROWS, 128), jnp.int32),
            pltpu.VMEM((32 + 48, KB, 128), BF16),
            pltpu.VMEM((48, KB, 128), BF16),
            pltpu.VMEM((X, HEAD, TOK), BF16),
            pltpu.VMEM((HEAD, X * TOK), BF16),
            pltpu.VMEM((TP, HEAD, X * TOK), BF16),
            pltpu.VMEM((NSEL * KB, 128), BF16),
            pltpu.VMEM((HEAD, NSEL * KB), BF16),
            pltpu.VMEM((16 * QB, 128), BF16),
            pltpu.VMEM((NSEL * KB, 4 * QB), F32),
            pltpu.VMEM((2, NSEL * KB, 8 * QB), BF16),
            pltpu.VMEM((2 * NSEL + 1, KB, 128), F32),
            pltpu.VMEM((48, KB, 128), BF16),
            pltpu.VMEM((48, KB, 128), BF16),
            pltpu.VMEM((4, KB, 128), F32),
            pltpu.VMEM((28, KB, 128), BF16),
            pltpu.VMEM((28, KB, 128), BF16),
            pltpu.VMEM((X * TOK, GROUP * HEAD), BF16),
            pltpu.VMEM((TP, HEAD, TOK), F32),
            pltpu.VMEM((TP, HEAD, TOK), BF16),
            pltpu.VMEM((Z, HEAD, TOK), BF16),
            dma,
            dma((6,)),
            dma((PARTS * Z,)), dma((PARTS * Z,)),
            dma((24,)), dma((24,)),
            dma((X,)), dma((X,)),
            dma((TP,)), dma((TP,)),
            dma((4 * X,)), dma((4 * X,)),
            dma((24,)), dma((24,)),
            dma((Z,)), dma((Z,)),
            dma((Z,)), dma((Z,)),
        ],
        compiler_params=pltpu.CompilerParams(
            collective_id=0, has_side_effects=True, vmem_limit_bytes=60000 * 1024
        ),
        name="fused_backward",
    )(chosen.T, inputs, queries, key_vectors.T, value_rows_by_head.T, out_grad)
    return dq, dk.T, dv.T, w


def solution(mesh):
    spec = P("kv", "tp")
    return jax.shard_map(
        body, mesh=mesh, in_specs=(spec,) * 5 + (P(),), out_specs=(spec,) * 4, check_vma=False
    )
```

```python
import functools

import jax
import jax.numpy as jnp
from jax import lax
from jax.experimental import pallas as pl
from jax.experimental.pallas import tpu as pltpu
from jax.sharding import PartitionSpec as P

HEAD = 64
QB = 128
KB = 64
NSEL = 16
Z, X, TP = 8, 4, 8
TOK = 256
SEQ = 8192
GROUP = 4
SCALE = HEAD**-0.5
ORDER = (0, 1, 7, 2, 6, 3, 5, 4)
PLACE = {d: p for p, d in enumerate(ORDER)}
NEG = -1e30
PARTS = 4
SIZE = 4 // PARTS
LEAVE = (7, 5, 6, 3, 4, 1, 2, 0)
MESH = pl.DeviceIdType.MESH
F32, BF16 = jnp.float32, jnp.bfloat16
ZERO_D = 2 * NSEL
T_FWD, T_SEND, T_OWN, T_LOC, T_BLK, T_ROWS = 0, 6, 18, 20, 21, 24


def place_of(distance):
    near = jnp.where(distance < 4, 2 * distance - 1, jnp.where(distance == 4, 7, 2 * (8 - distance)))
    return jnp.where(distance == 0, 0, near)


def fill_table(table, chosen_t, z, x):
    by_row = chosen_t[...]
    lane_r = lax.broadcasted_iota(jnp.int32, by_row.shape, 1)

    def column(d, e):
        row = z * 2 * X + 2 * lax.rem(x + d, X) + e
        return jnp.sum(jnp.where(lane_r == row, by_row, 0), axis=1, keepdims=True)

    cols = [[column(d, e) for e in range(2)] for d in range(X)]
    lane = lax.broadcasted_iota(jnp.int32, (1, 128), 1)
    sub = lax.broadcasted_iota(jnp.int32, (NSEL, 128), 0)

    def row_of_place(place):
        half = (place + 1) >> 1
        d = jnp.where((place & 1) == 1, half, Z - half)
        d = jnp.where(place == 7, 4, d)
        return (z + d) & 7

    def two_used(pair, base):
        low, high = 3, 0
        for col in pair:
            rel = col - base
            ok = (rel >= 0) & (rel < 4)
            low = jnp.minimum(low, jnp.min(jnp.where(ok, rel, 3), axis=0, keepdims=True))
            high = jnp.maximum(high, jnp.max(jnp.where(ok, rel, 0), axis=0, keepdims=True))
        return low, high

    def inverse(e, block):
        hit = cols[0][e] == block
        return jnp.min(jnp.where(hit, sub + NSEL * e, ZERO_D), axis=0, keepdims=True)

    at_place = row_of_place(lane & 7) * 16
    for d in range(1, X):
        low, high = two_used(cols[d], at_place + x * 4)
        n = (d - 1) * 2
        table[T_FWD + n : T_FWD + n + 1] = low
        table[T_FWD + n + 1 : T_FWD + n + 2] = high
        base = at_place + lax.rem(x + d, X) * 4
        for s, o in enumerate(two_used(cols[0], base)):
            for e in range(2):
                m = T_SEND + ((d - 1) * 2 + s) * 2 + e
                table[m : m + 1] = inverse(e, base + o)
    mine = row_of_place((lane >> 2) & 7) * 16 + x * 4 + (lane & 3)
    for e in range(2):
        table[T_OWN + e : T_OWN + e + 1] = inverse(e, mine)
    diag = sub == (lane & (NSEL - 1))
    flat = [jnp.sum(jnp.where(diag, cols[0][e], 0), axis=0, keepdims=True) for e in range(2)]
    block = jnp.where(lane < NSEL, flat[0], flat[1])
    owner, off = block >> 2, block & 3
    place = place_of(((owner >> 2) - z) & 7)
    dx = ((owner & 3) - x) & 3
    earlier = 0
    for e in range(2):
        same = ((cols[0][e] >> 2) == owner) & ((cols[0][e] & 3) < off)
        earlier = jnp.maximum(earlier, jnp.max(jnp.where(same, 1, 0), axis=0, keepdims=True))
    loc = jnp.where(dx == 0, place * 4 + off, 32 + ((dx - 1) * Z + place) * 2 + earlier)
    table[T_LOC : T_LOC + 1] = jnp.where(owner > z * X + x, 0, loc)
    table[T_BLK : T_BLK + 1] = block


def kernel(
    chosen_h, in_h, q_h, k_h, v_h, g_h,
    dq_out, dk_out, dv_out, w_out,
    chosen_t, in_ref, q_ref, k_ref, v_ref, g_ref, tab_v, tab, kvt, xsel, in_t, xt, at, kvs, kst, qg, sg_scr, sp_scr,
    dsel, dxs, rbuf, acc, zs_send, zr_buf, dqg, wp, w_send, w_recv,
    t_sem, h_sem, z_ss, z_rs, x_ss, x_rs, i_ss, i_rs, y_ss, y_rs, dq_ss, dq_rs, dx_ss, dx_rs, w_ss, w_rs, dz_ss, dz_rs,
):
    kv, tp = lax.axis_index("kv"), lax.axis_index("tp")
    z, x = kv // X, lax.rem(kv, X)

    def row(p):
        return lax.rem(z + ORDER[p], Z)

    def at_z(p):
        return (row(p) * X + x, tp)

    def at_x(d):
        return (z * X + lax.rem(x + d, X), tp)

    def at_tp(d):
        return (kv, lax.rem(tp + d, TP))

    def remote(src, dst, ss, rs, dev):
        return pltpu.make_async_remote_copy(
            src_ref=src, dst_ref=dst, send_sem=ss, recv_sem=rs, device_id=dev, device_id_type=MESH
        )

    def opposite(p):
        return PLACE[(Z - ORDER[p]) % Z]

    def column(d):
        return lax.rem(x + d, X)

    with jax.named_scope("bar"):
        barrier = pltpu.get_barrier_semaphore()
        peers = [at_z(p) for p in range(1, Z)] + [at_x(d) for d in range(1, X)] + [at_tp(d) for d in range(1, TP)]
        for dev in peers:
            pl.semaphore_signal(barrier, inc=1, device_id=dev, device_id_type=MESH)
        loads = [(k_h, k_ref), (v_h, v_ref), (chosen_h, chosen_t), (in_h, in_ref), (q_h, q_ref), (g_h, g_ref)]
        loads = [pltpu.make_async_copy(src, dst, h_sem.at[n]) for n, (src, dst) in enumerate(loads)]
        for c in loads:
            c.start()
        for c in loads[:4]:
            c.wait()
        kvt[0:4] = jnp.concatenate([k_ref[...], v_ref[...]], axis=0).T.reshape(4, KB, 128)
        in_t[...] = in_ref[...].T.reshape(X, HEAD, TOK)
        fill_table(tab_v, chosen_t, z, x)
        dsel[ZERO_D] = jnp.zeros((KB, 128), F32)
        t_copy = pltpu.make_async_copy(tab_v, tab, t_sem)
        t_copy.start()
        xt[:, 0:TOK] = in_t[x]
        for c in loads[4:]:
            c.wait()
        pl.semaphore_wait(barrier, len(peers))

    def z_keys(hop, f, up):
        here = 0 if hop == 1 else PLACE[Z + 1 - hop if up else hop - 1]
        there = PLACE[Z - hop if up else hop]
        n = PARTS * there + f
        to = (lax.rem(z + (1 if up else Z - 1), Z) * X + x, tp)
        return remote(
            kvt.at[pl.ds(4 * here + SIZE * f, SIZE)], kvt.at[pl.ds(4 * there + SIZE * f, SIZE)], z_ss.at[n], z_rs.at[n], to
        )

    def z_sends(hop, up):
        if up:
            return (z >= hop - 1) & (z < Z - 1)
        return lax.rem(z + hop - 1, Z) <= Z - 6

    def z_gets(hop, up):
        if up:
            return z >= hop
        return lax.rem(z + hop, Z) <= Z - 6

    HOPS = [(hop, up) for hop in range(1, 5) for up in (True, False) if up or hop < 4]
    for f in range(PARTS):
        for up in (True, False):
            pl.when(z_sends(1, up))(z_keys(1, f, up).start)

    def x_inputs(d):
        return remote(
            in_t.at[column(d)], xt.at[:, pl.ds((X - d) * TOK, TOK)], i_ss.at[d], i_rs.at[X - d], at_x(d)
        )

    def tp_inputs(d):
        return remote(xt, at.at[tp], y_ss.at[d], y_rs.at[TP - d], at_tp(d))

    def x_keys(p, d):
        mine, there = ((d - 1) * Z + p) * 2, 32 + ((X - d - 1) * Z + p) * 2
        return remote(
            xsel.at[pl.ds(mine, 2)], kvt.at[pl.ds(there, 2)],
            x_ss.at[(d - 1) * Z + p], x_rs.at[(X - d - 1) * Z + p], at_x(d),
        )

    def x_keys_in(p, d):
        there = 32 + ((d - 1) * Z + p) * 2
        n = (d - 1) * Z + p
        return remote(xsel.at[pl.ds(2 * n, 2)], kvt.at[pl.ds(there, 2)], x_ss.at[n], x_rs.at[n], at_x(d))

    def forward(p):
        four = [kvt[4 * p + o] for o in range(4)]
        for d in range(1, X):
            for s in range(2):
                o = tab[T_FWD + (d - 1) * 2 + s, p]
                low = jnp.where(o == 0, four[0], four[1])
                high = jnp.where(o == 2, four[2], four[3])
                xsel[((d - 1) * Z + p) * 2 + s] = jnp.where(o < 2, low, high)
        for d in range(1, X):
            if p > 0:
                x_keys(p, d).start()
            else:
                pl.when(column(d) > x)(x_keys(p, d).start)

    with jax.named_scope("sel"):
        t_copy.wait()
        forward(0)
        for d in range(1, X):
            x_inputs(d).start()
        for hop, up in HOPS:
            @pl.when(z_gets(hop, up))
            def _(hop=hop, up=up):
                for f in range(PARTS):
                    z_keys(hop, f, up).wait_recv()
                    if hop < (4 if up else 3):
                        pl.when(z_sends(hop + 1, up))(z_keys(hop + 1, f, up).start)
            p = PLACE[Z - hop if up else hop]
            pl.when(row(p) < z)(functools.partial(forward, p))
            if hop == 1 and not up:
                for d in range(1, X):
                    x_inputs(d).wait_recv()
                for d in range(1, TP):
                    tp_inputs(d).start()
                at[tp] = xt[...]
    with jax.named_scope("xwait"):
        for p in range(1, Z):
            @pl.when(row(p) < z)
            def _(p=p):
                for d in range(1, X):
                    x_keys_in(p, d).wait_recv()
        for d in range(1, X):
            pl.when(column(d) < x)(x_keys_in(0, d).wait_recv)

    lanes = 2 * QB
    lane_t = lax.broadcasted_iota(jnp.int32, (KB, lanes), 1) % QB
    diff = lax.broadcasted_iota(jnp.int32, (KB, lanes), 0) - lane_t
    zeros = jnp.zeros((QB, HEAD), BF16)
    nt = (((1,), (1,)), ((), ()))
    nn = (((1,), (0,)), ((), ()))

    def fold(t, op):
        return op(t.reshape(KB // 8, 8, lanes), axis=0)

    def x_dq(r, hp, d):
        cols = pl.ds(hp * 2 * HEAD, 2 * HEAD)
        n = (r * 2 + hp) * X
        return remote(
            dqg.at[pl.ds(r * QB, QB), cols], dqg.at[pl.ds((X - d) * TOK + r * QB, QB), cols],
            dq_ss.at[n + d], dq_rs.at[n + X - d], at_x(d),
        )

    units = [(r, hp) for r in range(2) for hp in range(2)]
    for r, hp in units:
        scope = jax.named_scope(f"attn{r}{hp}")
        scope.__enter__()
        rows = pl.ds(r * QB, QB)
        if hp == 0:
            for j in range(NSEL):
                kvs[j * KB : (j + 1) * KB, :] = kvt[tab[T_LOC, r * NSEL + j]]
            kst[...] = kvs[...].T[:HEAD]
        first = r * 8 * QB + hp * 4 * QB
        for h in range(2):
            cols = slice((hp * 2 + h) * HEAD, (hp * 2 + h + 1) * HEAD)
            qg[first + h * QB : first + (h + 1) * QB, :] = jnp.concatenate([q_ref[rows, cols], zeros], axis=1)
            qg[first + (h + 2) * QB : first + (h + 3) * QB, :] = jnp.concatenate([zeros, g_ref[rows, cols]], axis=1)
        sg_scr[...] = lax.dot_general(kvs[...], qg[first : first + 4 * QB], nt, preferred_element_type=F32)
        s_lanes, g_lanes = slice(0, lanes), slice(lanes, 2 * lanes)
        ds_lanes = slice(hp * 2 * lanes, hp * 2 * lanes + lanes)
        p_lanes = slice(hp * 2 * lanes + lanes, hp * 2 * lanes + 2 * lanes)

        def mask_step(j, m):
            at_j = pl.ds(pl.multiple_of(j * KB, KB), KB)
            limit = kv * TOK + r * QB - tab[T_BLK, r * NSEL + j] * KB
            s = jnp.where(diff <= limit, sg_scr[at_j, s_lanes] * SCALE, NEG)
            sg_scr[at_j, s_lanes] = s
            return jnp.maximum(m, fold(s, jnp.max))

        m = lax.fori_loop(0, NSEL, mask_step, jnp.full((8, lanes), NEG, F32), unroll=4)
        m = jnp.max(m, axis=0, keepdims=True)

        def exp_step(j, total):
            at_j = pl.ds(pl.multiple_of(j * KB, KB), KB)
            e = jnp.exp(sg_scr[at_j, s_lanes] - m)
            sg_scr[at_j, s_lanes] = e
            return total + fold(e, jnp.sum)

        total = lax.fori_loop(0, NSEL, exp_step, jnp.zeros((8, lanes), F32), unroll=4)
        inv = 1.0 / jnp.sum(total, axis=0, keepdims=True)

        def half_step(j, dot):
            at_j = pl.ds(pl.multiple_of(j * KB, KB), KB)
            half = (sg_scr[at_j, s_lanes] * inv).astype(BF16)
            sp_scr[r, at_j, p_lanes] = half
            return dot + fold(half.astype(F32) * sg_scr[at_j, g_lanes], jnp.sum)

        dot = lax.fori_loop(0, NSEL, half_step, jnp.zeros((8, lanes), F32), unroll=4)
        dot = jnp.sum(dot, axis=0, keepdims=True)

        def grad_step(j, carry):
            at_j = pl.ds(pl.multiple_of(j * KB, KB), KB)
            grad = (sg_scr[at_j, s_lanes] * inv) * (sg_scr[at_j, g_lanes] - dot)
            sp_scr[r, at_j, ds_lanes] = grad.astype(BF16)
            return carry

        lax.fori_loop(0, NSEL, grad_step, 0, unroll=4)
        dq_t = lax.dot_general(kst[...], sp_scr[r, :, ds_lanes], nn, preferred_element_type=F32) * SCALE
        stacked = jnp.concatenate([dq_t[:, :QB], dq_t[:, QB:]], axis=0)
        dqg[rows, hp * 2 * HEAD : (hp + 1) * 2 * HEAD] = stacked.T.astype(BF16)
        for d in range(1, X):
            x_dq(r, hp, d).start()
        scope.__exit__(None, None, None)
    with jax.named_scope("dkv"):
        for r in range(2):
            dkv = lax.dot_general(
                sp_scr[r], qg[r * 8 * QB : (r + 1) * 8 * QB], nn, preferred_element_type=F32
            )
            dsel[pl.ds(r * NSEL, NSEL)] = dkv.reshape(NSEL, KB, 128)
        dq_out[...] = dqg[0:TOK, :]

    def x_grads(p, d):
        mine, there = (d - 1) * Z + p, (X - d - 1) * Z + p
        return remote(
            dxs.at[pl.ds(2 * mine, 2)], rbuf.at[pl.ds(2 * there, 2)], dx_ss.at[mine], dx_rs.at[there], at_x(d)
        )

    def x_grads_in(p, d):
        mine = (d - 1) * Z + p
        return remote(
            dxs.at[pl.ds(2 * mine, 2)], rbuf.at[pl.ds(2 * mine, 2)], dx_ss.at[mine], dx_rs.at[mine], at_x(d)
        )

    with jax.named_scope("dxsend"):
        for p in LEAVE:
            @pl.when(row(p) <= z)
            def _(p=p):
                for d in range(1, X):
                    for s in range(2):
                        t = T_SEND + ((d - 1) * 2 + s) * 2
                        dxs[((d - 1) * Z + p) * 2 + s] = (dsel[tab[t, p]] + dsel[tab[t + 1, p]]).astype(BF16)
                for d in range(1, X):
                    if p > 0:
                        x_grads(p, d).start()
                    else:
                        pl.when(column(d) < x)(x_grads(p, d).start)

    def z_weight(p):
        there = opposite(p)
        return remote(w_send.at[row(p)], w_recv.at[there], w_ss.at[p], w_rs.at[there], at_z(p))

    with jax.named_scope("wgrad"):
        for d in range(1, TP):
            tp_inputs(d).wait_recv()
        for r, hp in units:
            for d in range(1, X):
                x_dq(r, hp, d).wait_recv()
        wp[...] = lax.dot_general(
            at[...].reshape(TP * HEAD, X * TOK), dqg[...], nn, preferred_element_type=F32
        ).reshape(TP, HEAD, TOK)
        w_send[...] = wp[...].astype(BF16)
        @pl.when(z < Z // 2)
        def _():
            for p in reversed(range(1, Z)):
                z_weight(p).start()


    def z_copy(slot, step):
        return remote(
            zs_send.at[pl.ds(4 * slot, 4)], zr_buf.at[pl.ds(4 * slot, 4)], dz_ss.at[slot], dz_rs.at[slot],
            (lax.rem(z + step + Z, Z) * X + x, tp),
        )

    wraps = (z >= Z - 2) | (z == 0)
    returns = [
        (7, z >= 4, None, None, 0, -1),
        (5, z >= 5, None, None, 1, 1),
        (6, z >= 3, 0, (z >= 3) & (z <= 6), 2, -1),
        (3, wraps, 1, wraps, 3, 2),
        (4, z >= 2, 2, (z >= 2) & (z <= 6), 4, -2),
        (1, z == 7, None, None, 5, 1),
        (2, z >= 1, None, None, 6, -1),
    ]
    arrivals = [(3, z <= 2), (4, z <= 5), (5, z == 0), (6, z <= 6)]

    def relay(p, o):
        n = p * 4 + o
        term = dsel[tab[T_OWN, n]] + dsel[tab[T_OWN + 1, n]]
        for d in range(1, X):
            mine = (d - 1) * Z + p
            t = T_FWD + (d - 1) * 2
            first = tab[t, p] == o
            used = first | (tab[t + 1, p] == o)
            if p == 0:
                used = used & (column(d) > x)
            slot = jnp.where(first, rbuf[2 * mine], rbuf[2 * mine + 1]).astype(F32)
            term += jnp.where(used, slot, 0.0)
        return term

    with jax.named_scope("relay"):
        for p, sends, added, adds, slot, step in returns:
            @pl.when(sends)
            def _(p=p, added=added, adds=adds, slot=slot, step=step):
                @pl.when(row(p) < z)
                def _():
                    for d in range(1, X):
                        x_grads_in(p, d).wait_recv()

                if added is not None:
                    pl.when(adds)(z_copy(added, 0).wait_recv)
                for o in range(4):
                    term = jnp.where(row(p) < z, relay(p, o), 0.0)
                    if added is not None:
                        term += jnp.where(adds, zr_buf[added * 4 + o].astype(F32), 0.0)
                    zs_send[slot * 4 + o] = term.astype(BF16)
                z_copy(slot, step).start()

            pl.when(z >= Z // 2)(z_weight(Z - 1 - slot).start)

        for d in range(1, X):
            pl.when(column(d) > x)(x_grads_in(0, d).wait_recv)
        for o in range(4):
            acc[o] = relay(0, o)
    with jax.named_scope("wfin"):
        w = wp[z]
        for p in range(1, Z):
            z_weight(p).wait_recv()
        for p in range(1, Z):
            w += w_recv[p].astype(F32)
        w_out[...] = w
    with jax.named_scope("dzwait"):
        for slot, comes in arrivals:
            @pl.when(comes)
            def _(slot=slot):
                z_copy(slot, 0).wait_recv()
                acc[...] += zr_buf[4 * slot : 4 * slot + 4].astype(F32)
        both = acc[...].reshape(TOK, 128).T
        dk_out[...] = (both[:HEAD] * SCALE).astype(BF16)
        dv_out[...] = both[HEAD:].astype(BF16)
    with jax.named_scope("sentwait"):
        for hop, up in HOPS:
            for f in range(PARTS):
                pl.when(z_sends(hop, up))(z_keys(hop, f, up).wait_send)
        for p in range(1, Z):
            z_weight(p).wait_send()
            @pl.when(row(p) < z)
            def _(p=p):
                for d in range(1, X):
                    x_keys(p, d).wait_send()
                    x_grads(p, d).wait_send()
        for d in range(1, X):
            pl.when(column(d) > x)(x_keys(0, d).wait_send)
            pl.when(column(d) < x)(x_grads(0, d).wait_send)
            x_inputs(d).wait_send()
            for r, hp in units:
                x_dq(r, hp, d).wait_send()
        for d in range(1, TP):
            tp_inputs(d).wait_send()
        for p, sends, added, adds, slot, step in returns:
            pl.when(sends)(z_copy(slot, step).wait_send)


def copy_out(*refs):
    for src, dst in zip(refs[:4], refs[4:]):
        dst[...] = src[...]


def body(inputs, queries, key_vectors, value_rows_by_head, out_grad, chosen):
    dma = pltpu.SemaphoreType.DMA
    vmem = pl.BlockSpec(memory_space=pltpu.VMEM)
    dq, dk, dv, w = pl.pallas_call(
        kernel,
        out_shape=(
            jax.ShapeDtypeStruct((TOK, GROUP * HEAD), BF16),
            jax.ShapeDtypeStruct((HEAD, TOK), BF16),
            jax.ShapeDtypeStruct((HEAD, TOK), BF16),
            jax.ShapeDtypeStruct((HEAD, GROUP * HEAD), F32),
        ),
        in_specs=[pl.BlockSpec(memory_space=pl.ANY)] * 6,
        out_specs=(vmem,) * 4,
        scratch_shapes=[
            pltpu.VMEM((NSEL, SEQ // QB), jnp.int32),
            pltpu.VMEM((TOK, TOK), BF16),
            pltpu.VMEM((TOK, GROUP * HEAD), BF16),
            pltpu.VMEM((HEAD, TOK), BF16),
            pltpu.VMEM((HEAD, TOK), BF16),
            pltpu.VMEM((TOK, GROUP * HEAD), BF16),
            pltpu.VMEM((T_ROWS, 128), jnp.int32),
            pltpu.SMEM((T_ROWS, 128), jnp.int32),
            pltpu.VMEM((32 + 48, KB, 128), BF16),
            pltpu.VMEM((48, KB, 128), BF16),
            pltpu.VMEM((X, HEAD, TOK), BF16),
            pltpu.VMEM((HEAD, X * TOK), BF16),
            pltpu.VMEM((TP, HEAD, X * TOK), BF16),
            pltpu.VMEM((NSEL * KB, 128), BF16),
            pltpu.VMEM((HEAD, NSEL * KB), BF16),
            pltpu.VMEM((16 * QB, 128), BF16),
            pltpu.VMEM((NSEL * KB, 4 * QB), F32),
            pltpu.VMEM((2, NSEL * KB, 8 * QB), BF16),
            pltpu.VMEM((2 * NSEL + 1, KB, 128), F32),
            pltpu.VMEM((48, KB, 128), BF16),
            pltpu.VMEM((48, KB, 128), BF16),
            pltpu.VMEM((4, KB, 128), F32),
            pltpu.VMEM((28, KB, 128), BF16),
            pltpu.VMEM((28, KB, 128), BF16),
            pltpu.VMEM((X * TOK, GROUP * HEAD), BF16),
            pltpu.VMEM((TP, HEAD, TOK), F32),
            pltpu.VMEM((TP, HEAD, TOK), BF16),
            pltpu.VMEM((Z, HEAD, TOK), BF16),
            dma,
            dma((6,)),
            dma((PARTS * Z,)), dma((PARTS * Z,)),
            dma((24,)), dma((24,)),
            dma((X,)), dma((X,)),
            dma((TP,)), dma((TP,)),
            dma((4 * X,)), dma((4 * X,)),
            dma((24,)), dma((24,)),
            dma((Z,)), dma((Z,)),
            dma((Z,)), dma((Z,)),
        ],
        compiler_params=pltpu.CompilerParams(
            collective_id=0, has_side_effects=True, vmem_limit_bytes=60000 * 1024
        ),
        name="fused_backward",
    )(chosen.T, inputs, queries, key_vectors.T, value_rows_by_head.T, out_grad)
    dq, dk, dv, w = pl.pallas_call(
        copy_out,
        out_shape=tuple(jax.ShapeDtypeStruct(t.shape, t.dtype) for t in (dq, dk, dv, w)),
        in_specs=[vmem] * 4,
        out_specs=(vmem,) * 4,
        name="copy_out",
    )(dq, dk, dv, w)
    return dq, dk.T, dv.T, w


def solution(mesh):
    spec = P("kv", "tp")
    return jax.shard_map(
        body, mesh=mesh, in_specs=(spec,) * 5 + (P(),), out_specs=(spec,) * 4, check_vma=False
    )
```

```python
import functools

import jax
import jax.numpy as jnp
from jax import lax
from jax.experimental import pallas as pl
from jax.experimental.pallas import tpu as pltpu
from jax.sharding import PartitionSpec as P

HEAD = 64
QB = 128
KB = 64
NSEL = 16
Z, X, TP = 8, 4, 8
TOK = 256
SEQ = 8192
GROUP = 4
SCALE = HEAD**-0.5
ORDER = (0, 1, 7, 2, 6, 3, 5, 4)
PLACE = {d: p for p, d in enumerate(ORDER)}
NEG = -1e30
PARTS = 4
SIZE = 4 // PARTS
LEAVE = (7, 5, 6, 3, 4, 1, 2, 0)
MESH = pl.DeviceIdType.MESH
F32, BF16 = jnp.float32, jnp.bfloat16
ZERO_D = 2 * NSEL
T_FWD, T_SEND, T_OWN, T_LOC, T_BLK, T_ROWS = 0, 6, 18, 20, 21, 24


def place_of(distance):
    near = jnp.where(distance < 4, 2 * distance - 1, jnp.where(distance == 4, 7, 2 * (8 - distance)))
    return jnp.where(distance == 0, 0, near)


def fill_table(table, chosen_t, z, x):
    by_row = chosen_t[...]
    lane_r = lax.broadcasted_iota(jnp.int32, by_row.shape, 1)

    def column(d, e):
        row = z * 2 * X + 2 * lax.rem(x + d, X) + e
        return jnp.sum(jnp.where(lane_r == row, by_row, 0), axis=1, keepdims=True)

    cols = [[column(d, e) for e in range(2)] for d in range(X)]
    lane = lax.broadcasted_iota(jnp.int32, (1, 128), 1)
    sub = lax.broadcasted_iota(jnp.int32, (NSEL, 128), 0)

    def row_of_place(place):
        half = (place + 1) >> 1
        d = jnp.where((place & 1) == 1, half, Z - half)
        d = jnp.where(place == 7, 4, d)
        return (z + d) & 7

    def two_used(pair, base):
        low, high = 3, 0
        for col in pair:
            rel = col - base
            ok = (rel >= 0) & (rel < 4)
            low = jnp.minimum(low, jnp.min(jnp.where(ok, rel, 3), axis=0, keepdims=True))
            high = jnp.maximum(high, jnp.max(jnp.where(ok, rel, 0), axis=0, keepdims=True))
        return low, high

    def inverse(e, block):
        hit = cols[0][e] == block
        return jnp.min(jnp.where(hit, sub + NSEL * e, ZERO_D), axis=0, keepdims=True)

    at_place = row_of_place(lane & 7) * 16
    for d in range(1, X):
        low, high = two_used(cols[d], at_place + x * 4)
        n = (d - 1) * 2
        table[T_FWD + n : T_FWD + n + 1] = low
        table[T_FWD + n + 1 : T_FWD + n + 2] = high
        base = at_place + lax.rem(x + d, X) * 4
        for s, o in enumerate(two_used(cols[0], base)):
            for e in range(2):
                m = T_SEND + ((d - 1) * 2 + s) * 2 + e
                table[m : m + 1] = inverse(e, base + o)
    mine = row_of_place((lane >> 2) & 7) * 16 + x * 4 + (lane & 3)
    for e in range(2):
        table[T_OWN + e : T_OWN + e + 1] = inverse(e, mine)
    diag = sub == (lane & (NSEL - 1))
    flat = [jnp.sum(jnp.where(diag, cols[0][e], 0), axis=0, keepdims=True) for e in range(2)]
    block = jnp.where(lane < NSEL, flat[0], flat[1])
    owner, off = block >> 2, block & 3
    place = place_of(((owner >> 2) - z) & 7)
    dx = ((owner & 3) - x) & 3
    earlier = 0
    for e in range(2):
        same = ((cols[0][e] >> 2) == owner) & ((cols[0][e] & 3) < off)
        earlier = jnp.maximum(earlier, jnp.max(jnp.where(same, 1, 0), axis=0, keepdims=True))
    loc = jnp.where(dx == 0, place * 4 + off, 32 + ((dx - 1) * Z + place) * 2 + earlier)
    table[T_LOC : T_LOC + 1] = jnp.where(owner > z * X + x, 0, loc)
    table[T_BLK : T_BLK + 1] = block


def kernel(
    chosen_h, in_h, q_h, k_h, v_h, g_h,
    dq_out, dk_out, dv_out, w_out,
    chosen_t, in_ref, q_ref, k_ref, v_ref, g_ref, tab_v, tab, kvt, xsel, in_t, xt, at, kvs, kst, qg, sg_both, sp_scr,
    dsel, dxs, rbuf, acc, zs_send, zr_buf, dqg, wp, w_send, w_recv,
    t_sem, h_sem, z_ss, z_rs, x_ss, x_rs, i_ss, i_rs, y_ss, y_rs, dq_ss, dq_rs, dx_ss, dx_rs, w_ss, w_rs, dz_ss, dz_rs,
):
    kv, tp = lax.axis_index("kv"), lax.axis_index("tp")
    z, x = kv // X, lax.rem(kv, X)

    def row(p):
        return lax.rem(z + ORDER[p], Z)

    def at_z(p):
        return (row(p) * X + x, tp)

    def at_x(d):
        return (z * X + lax.rem(x + d, X), tp)

    def at_tp(d):
        return (kv, lax.rem(tp + d, TP))

    def remote(src, dst, ss, rs, dev):
        return pltpu.make_async_remote_copy(
            src_ref=src, dst_ref=dst, send_sem=ss, recv_sem=rs, device_id=dev, device_id_type=MESH
        )

    def opposite(p):
        return PLACE[(Z - ORDER[p]) % Z]

    def column(d):
        return lax.rem(x + d, X)

    with jax.named_scope("bar"):
        barrier = pltpu.get_barrier_semaphore()
        peers = [at_z(p) for p in range(1, Z)] + [at_x(d) for d in range(1, X)] + [at_tp(d) for d in range(1, TP)]
        for dev in peers:
            pl.semaphore_signal(barrier, inc=1, device_id=dev, device_id_type=MESH)
        loads = [(k_h, k_ref), (v_h, v_ref), (chosen_h, chosen_t), (in_h, in_ref), (q_h, q_ref), (g_h, g_ref)]
        loads = [pltpu.make_async_copy(src, dst, h_sem.at[n]) for n, (src, dst) in enumerate(loads)]
        for c in loads:
            c.start()
        for c in loads[:4]:
            c.wait()
        kvt[0:4] = jnp.concatenate([k_ref[...], v_ref[...]], axis=0).T.reshape(4, KB, 128)
        in_t[...] = in_ref[...].T.reshape(X, HEAD, TOK)
        fill_table(tab_v, chosen_t, z, x)
        dsel[ZERO_D] = jnp.zeros((KB, 128), F32)
        t_copy = pltpu.make_async_copy(tab_v, tab, t_sem)
        t_copy.start()
        xt[:, 0:TOK] = in_t[x]
        for c in loads[4:]:
            c.wait()
        pl.semaphore_wait(barrier, len(peers))

    def z_keys(hop, f, up):
        here = 0 if hop in (1, 4) else PLACE[Z + 1 - hop if up else hop - 1]
        there = PLACE[Z - hop if up else hop]
        n = PARTS * there + f
        step = 4 if hop == 4 else 1 if up else Z - 1
        to = (lax.rem(z + step, Z) * X + x, tp)
        return remote(
            kvt.at[pl.ds(4 * here + SIZE * f, SIZE)], kvt.at[pl.ds(4 * there + SIZE * f, SIZE)], z_ss.at[n], z_rs.at[n], to
        )

    def z_sends(hop, up):
        if hop == 4:
            return z < Z // 2
        if up:
            return (z >= hop - 1) & (z < Z - 1)
        return lax.rem(z + hop - 1, Z) <= Z - 6

    def z_gets(hop, up):
        if up:
            return z >= hop
        return lax.rem(z + hop, Z) <= Z - 6

    HOPS = [(hop, up) for hop in range(1, 5) for up in (True, False) if up or hop < 4]
    for f in range(PARTS):
        for up in (True, False):
            pl.when(z_sends(1, up))(z_keys(1, f, up).start)

    def x_inputs(d):
        return remote(
            in_t.at[column(d)], xt.at[:, pl.ds((X - d) * TOK, TOK)], i_ss.at[d], i_rs.at[X - d], at_x(d)
        )

    def tp_inputs(d):
        return remote(xt, at.at[tp], y_ss.at[d], y_rs.at[TP - d], at_tp(d))

    def x_keys(p, d):
        mine, there = ((d - 1) * Z + p) * 2, 32 + ((X - d - 1) * Z + p) * 2
        return remote(
            xsel.at[pl.ds(mine, 2)], kvt.at[pl.ds(there, 2)],
            x_ss.at[(d - 1) * Z + p], x_rs.at[(X - d - 1) * Z + p], at_x(d),
        )

    def x_keys_in(p, d):
        there = 32 + ((d - 1) * Z + p) * 2
        n = (d - 1) * Z + p
        return remote(xsel.at[pl.ds(2 * n, 2)], kvt.at[pl.ds(there, 2)], x_ss.at[n], x_rs.at[n], at_x(d))

    def forward(p):
        four = [kvt[4 * p + o] for o in range(4)]
        for d in range(1, X):
            for s in range(2):
                o = tab[T_FWD + (d - 1) * 2 + s, p]
                low = jnp.where(o == 0, four[0], four[1])
                high = jnp.where(o == 2, four[2], four[3])
                xsel[((d - 1) * Z + p) * 2 + s] = jnp.where(o < 2, low, high)
        for d in range(1, X):
            if p > 0:
                x_keys(p, d).start()
            else:
                pl.when(column(d) > x)(x_keys(p, d).start)

    with jax.named_scope("sel"):
        t_copy.wait()
        forward(0)
        for d in range(1, X):
            x_inputs(d).start()
        for hop in (1, 2, 4, 3):
            ways = [up for up in (True, False) if (hop, up) in HOPS]
            for f in range(PARTS):
                for up in ways:
                    @pl.when(z_gets(hop, up))
                    def _(f=f, up=up):
                        z_keys(hop, f, up).wait_recv()
                        if hop < 3:
                            pl.when(z_sends(hop + 1, up))(z_keys(hop + 1, f, up).start)

            if hop == 1:
                for f in range(PARTS):
                    pl.when(z_sends(4, True))(z_keys(4, f, True).start)
            for up in ways:
                p = PLACE[Z - hop if up else hop]
                pl.when(z_gets(hop, up) & (row(p) < z))(functools.partial(forward, p))
            if hop == 1:
                for d in range(1, X):
                    x_inputs(d).wait_recv()
                for d in range(1, TP):
                    tp_inputs(d).start()
                at[tp] = xt[...]
    with jax.named_scope("xwait"):
        for p in range(1, Z):
            @pl.when(row(p) < z)
            def _(p=p):
                for d in range(1, X):
                    x_keys_in(p, d).wait_recv()
        for d in range(1, X):
            pl.when(column(d) < x)(x_keys_in(0, d).wait_recv)

    lanes = 2 * QB
    lane_t = lax.broadcasted_iota(jnp.int32, (KB, lanes), 1) % QB
    diff = lax.broadcasted_iota(jnp.int32, (KB, lanes), 0) - lane_t
    zeros = jnp.zeros((QB, HEAD), BF16)
    nt = (((1,), (1,)), ((), ()))
    nn = (((1,), (0,)), ((), ()))

    def fold(t, op):
        return op(t.reshape(KB // 8, 8, lanes), axis=0)

    def x_dq(r, hp, d):
        cols = pl.ds(hp * 2 * HEAD, 2 * HEAD)
        n = (r * 2 + hp) * X
        return remote(
            dqg.at[pl.ds(r * QB, QB), cols], dqg.at[pl.ds((X - d) * TOK + r * QB, QB), cols],
            dq_ss.at[n + d], dq_rs.at[n + X - d], at_x(d),
        )

    units = [(r, hp) for r in range(2) for hp in range(2)]
    for r, hp in units:
        scope = jax.named_scope(f"attn{r}{hp}")
        scope.__enter__()
        rows = pl.ds(r * QB, QB)
        if hp == 0:
            for j in range(NSEL):
                kvs[j * KB : (j + 1) * KB, :] = kvt[tab[T_LOC, r * NSEL + j]]
            kst[...] = kvs[...].T[:HEAD]
        first = r * 8 * QB + hp * 4 * QB
        for h in range(2):
            cols = slice((hp * 2 + h) * HEAD, (hp * 2 + h + 1) * HEAD)
            qg[first + h * QB : first + (h + 1) * QB, :] = jnp.concatenate([q_ref[rows, cols], zeros], axis=1)
            qg[first + (h + 2) * QB : first + (h + 3) * QB, :] = jnp.concatenate([zeros, g_ref[rows, cols]], axis=1)
        sg_scr = sg_both.at[hp]
        sg_scr[...] = lax.dot_general(kvs[...], qg[first : first + 4 * QB], nt, preferred_element_type=F32)
        s_lanes, g_lanes = slice(0, lanes), slice(lanes, 2 * lanes)
        ds_lanes = slice(hp * 2 * lanes, hp * 2 * lanes + lanes)
        p_lanes = slice(hp * 2 * lanes + lanes, hp * 2 * lanes + 2 * lanes)

        def mask_step(j, m):
            at_j = pl.ds(pl.multiple_of(j * KB, KB), KB)
            limit = kv * TOK + r * QB - tab[T_BLK, r * NSEL + j] * KB
            s = jnp.where(diff <= limit, sg_scr[at_j, s_lanes] * SCALE, NEG)
            sg_scr[at_j, s_lanes] = s
            return jnp.maximum(m, fold(s, jnp.max))

        m = lax.fori_loop(0, NSEL, mask_step, jnp.full((8, lanes), NEG, F32), unroll=16)
        m = jnp.max(m, axis=0, keepdims=True)

        def exp_step(j, total):
            at_j = pl.ds(pl.multiple_of(j * KB, KB), KB)
            e = jnp.exp(sg_scr[at_j, s_lanes] - m)
            sg_scr[at_j, s_lanes] = e
            return total + fold(e, jnp.sum)

        total = lax.fori_loop(0, NSEL, exp_step, jnp.zeros((8, lanes), F32), unroll=16)
        inv = 1.0 / jnp.sum(total, axis=0, keepdims=True)

        def half_step(j, dot):
            at_j = pl.ds(pl.multiple_of(j * KB, KB), KB)
            half = (sg_scr[at_j, s_lanes] * inv).astype(BF16)
            sp_scr[r, at_j, p_lanes] = half
            return dot + fold(half.astype(F32) * sg_scr[at_j, g_lanes], jnp.sum)

        dot = lax.fori_loop(0, NSEL, half_step, jnp.zeros((8, lanes), F32), unroll=16)
        dot = jnp.sum(dot, axis=0, keepdims=True)

        def grad_step(j, carry):
            at_j = pl.ds(pl.multiple_of(j * KB, KB), KB)
            grad = (sg_scr[at_j, s_lanes] * inv) * (sg_scr[at_j, g_lanes] - dot)
            sp_scr[r, at_j, ds_lanes] = grad.astype(BF16)
            return carry

        lax.fori_loop(0, NSEL, grad_step, 0, unroll=16)
        dq_t = lax.dot_general(kst[...], sp_scr[r, :, ds_lanes], nn, preferred_element_type=F32) * SCALE
        stacked = jnp.concatenate([dq_t[:, :QB], dq_t[:, QB:]], axis=0)
        dqg[rows, hp * 2 * HEAD : (hp + 1) * 2 * HEAD] = stacked.T.astype(BF16)
        for d in range(1, X):
            x_dq(r, hp, d).start()
        scope.__exit__(None, None, None)
    with jax.named_scope("dkv"):
        for r in range(2):
            dkv = lax.dot_general(
                sp_scr[r], qg[r * 8 * QB : (r + 1) * 8 * QB], nn, preferred_element_type=F32
            )
            dsel[pl.ds(r * NSEL, NSEL)] = dkv.reshape(NSEL, KB, 128)
        dq_out[...] = dqg[0:TOK, :]

    def x_grads(p, d):
        mine, there = (d - 1) * Z + p, (X - d - 1) * Z + p
        return remote(
            dxs.at[pl.ds(2 * mine, 2)], rbuf.at[pl.ds(2 * there, 2)], dx_ss.at[mine], dx_rs.at[there], at_x(d)
        )

    def x_grads_in(p, d):
        mine = (d - 1) * Z + p
        return remote(
            dxs.at[pl.ds(2 * mine, 2)], rbuf.at[pl.ds(2 * mine, 2)], dx_ss.at[mine], dx_rs.at[mine], at_x(d)
        )

    with jax.named_scope("dxsend"):
        for p in LEAVE:
            @pl.when(row(p) <= z)
            def _(p=p):
                for d in range(1, X):
                    for s in range(2):
                        t = T_SEND + ((d - 1) * 2 + s) * 2
                        dxs[((d - 1) * Z + p) * 2 + s] = (dsel[tab[t, p]] + dsel[tab[t + 1, p]]).astype(BF16)
                for d in range(1, X):
                    if p > 0:
                        x_grads(p, d).start()
                    else:
                        pl.when(column(d) < x)(x_grads(p, d).start)

    def z_weight(p):
        there = opposite(p)
        return remote(w_send.at[row(p)], w_recv.at[there], w_ss.at[p], w_rs.at[there], at_z(p))

    with jax.named_scope("wgrad"):
        for d in range(1, TP):
            tp_inputs(d).wait_recv()
        for r, hp in units:
            for d in range(1, X):
                x_dq(r, hp, d).wait_recv()
        wp[...] = lax.dot_general(
            at[...].reshape(TP * HEAD, X * TOK), dqg[...], nn, preferred_element_type=F32
        ).reshape(TP, HEAD, TOK)
        w_send[...] = wp[...].astype(BF16)
        @pl.when(z < Z // 2)
        def _():
            for p in reversed(range(1, Z)):
                z_weight(p).start()


    def z_copy(slot, step):
        return remote(
            zs_send.at[pl.ds(4 * slot, 4)], zr_buf.at[pl.ds(4 * slot, 4)], dz_ss.at[slot], dz_rs.at[slot],
            (lax.rem(z + step + Z, Z) * X + x, tp),
        )

    wraps = (z >= Z - 2) | (z == 0)
    returns = [
        (7, z >= 4, None, None, 0, -1),
        (5, z >= 5, None, None, 1, 1),
        (6, z >= 3, 0, (z >= 3) & (z <= 6), 2, -1),
        (3, wraps, 1, wraps, 3, 2),
        (4, z >= 2, 2, (z >= 2) & (z <= 6), 4, -2),
        (1, z == 7, None, None, 5, 1),
        (2, z >= 1, None, None, 6, -1),
    ]
    arrivals = [(3, z <= 2), (4, z <= 5), (5, z == 0), (6, z <= 6)]

    def relay(p, o):
        n = p * 4 + o
        term = dsel[tab[T_OWN, n]] + dsel[tab[T_OWN + 1, n]]
        for d in range(1, X):
            mine = (d - 1) * Z + p
            t = T_FWD + (d - 1) * 2
            first = tab[t, p] == o
            used = first | (tab[t + 1, p] == o)
            if p == 0:
                used = used & (column(d) > x)
            slot = jnp.where(first, rbuf[2 * mine], rbuf[2 * mine + 1]).astype(F32)
            term += jnp.where(used, slot, 0.0)
        return term

    with jax.named_scope("relay"):
        for p, sends, added, adds, slot, step in returns:
            @pl.when(sends)
            def _(p=p, added=added, adds=adds, slot=slot, step=step):
                @pl.when(row(p) < z)
                def _():
                    for d in range(1, X):
                        x_grads_in(p, d).wait_recv()

                if added is not None:
                    pl.when(adds)(z_copy(added, 0).wait_recv)
                for o in range(4):
                    term = jnp.where(row(p) < z, relay(p, o), 0.0)
                    if added is not None:
                        term += jnp.where(adds, zr_buf[added * 4 + o].astype(F32), 0.0)
                    zs_send[slot * 4 + o] = term.astype(BF16)
                z_copy(slot, step).start()

            pl.when(z >= Z // 2)(z_weight(Z - 1 - slot).start)

        for d in range(1, X):
            pl.when(column(d) > x)(x_grads_in(0, d).wait_recv)
        for o in range(4):
            acc[o] = relay(0, o)
    with jax.named_scope("wfin"):
        w = wp[z]
        for p in range(1, Z):
            z_weight(p).wait_recv()
        for p in range(1, Z):
            w += w_recv[p].astype(F32)
        w_out[...] = w
    with jax.named_scope("dzwait"):
        for slot, comes in arrivals:
            @pl.when(comes)
            def _(slot=slot):
                z_copy(slot, 0).wait_recv()
                acc[...] += zr_buf[4 * slot : 4 * slot + 4].astype(F32)
        both = acc[...].reshape(TOK, 128).T
        dk_out[...] = (both[:HEAD] * SCALE).astype(BF16)
        dv_out[...] = both[HEAD:].astype(BF16)
    with jax.named_scope("sentwait"):
        for hop, up in HOPS:
            for f in range(PARTS):
                pl.when(z_sends(hop, up))(z_keys(hop, f, up).wait_send)
        for p in range(1, Z):
            z_weight(p).wait_send()
            @pl.when(row(p) < z)
            def _(p=p):
                for d in range(1, X):
                    x_keys(p, d).wait_send()
                    x_grads(p, d).wait_send()
        for d in range(1, X):
            pl.when(column(d) > x)(x_keys(0, d).wait_send)
            pl.when(column(d) < x)(x_grads(0, d).wait_send)
            x_inputs(d).wait_send()
            for r, hp in units:
                x_dq(r, hp, d).wait_send()
        for d in range(1, TP):
            tp_inputs(d).wait_send()
        for p, sends, added, adds, slot, step in returns:
            pl.when(sends)(z_copy(slot, step).wait_send)


def copy_out(*refs):
    for src, dst in zip(refs[:4], refs[4:]):
        dst[...] = src[...]


def body(inputs, queries, key_vectors, value_rows_by_head, out_grad, chosen):
    dma = pltpu.SemaphoreType.DMA
    vmem = pl.BlockSpec(memory_space=pltpu.VMEM)
    dq, dk, dv, w = pl.pallas_call(
        kernel,
        out_shape=(
            jax.ShapeDtypeStruct((TOK, GROUP * HEAD), BF16),
            jax.ShapeDtypeStruct((HEAD, TOK), BF16),
            jax.ShapeDtypeStruct((HEAD, TOK), BF16),
            jax.ShapeDtypeStruct((HEAD, GROUP * HEAD), F32),
        ),
        in_specs=[pl.BlockSpec(memory_space=pl.ANY)] * 6,
        out_specs=(vmem,) * 4,
        scratch_shapes=[
            pltpu.VMEM((NSEL, SEQ // QB), jnp.int32),
            pltpu.VMEM((TOK, TOK), BF16),
            pltpu.VMEM((TOK, GROUP * HEAD), BF16),
            pltpu.VMEM((HEAD, TOK), BF16),
            pltpu.VMEM((HEAD, TOK), BF16),
            pltpu.VMEM((TOK, GROUP * HEAD), BF16),
            pltpu.VMEM((T_ROWS, 128), jnp.int32),
            pltpu.SMEM((T_ROWS, 128), jnp.int32),
            pltpu.VMEM((32 + 48, KB, 128), BF16),
            pltpu.VMEM((48, KB, 128), BF16),
            pltpu.VMEM((X, HEAD, TOK), BF16),
            pltpu.VMEM((HEAD, X * TOK), BF16),
            pltpu.VMEM((TP, HEAD, X * TOK), BF16),
            pltpu.VMEM((NSEL * KB, 128), BF16),
            pltpu.VMEM((HEAD, NSEL * KB), BF16),
            pltpu.VMEM((16 * QB, 128), BF16),
            pltpu.VMEM((2, NSEL * KB, 4 * QB), F32),
            pltpu.VMEM((2, NSEL * KB, 8 * QB), BF16),
            pltpu.VMEM((2 * NSEL + 1, KB, 128), F32),
            pltpu.VMEM((48, KB, 128), BF16),
            pltpu.VMEM((48, KB, 128), BF16),
            pltpu.VMEM((4, KB, 128), F32),
            pltpu.VMEM((28, KB, 128), BF16),
            pltpu.VMEM((28, KB, 128), BF16),
            pltpu.VMEM((X * TOK, GROUP * HEAD), BF16),
            pltpu.VMEM((TP, HEAD, TOK), F32),
            pltpu.VMEM((TP, HEAD, TOK), BF16),
            pltpu.VMEM((Z, HEAD, TOK), BF16),
            dma,
            dma((6,)),
            dma((PARTS * Z,)), dma((PARTS * Z,)),
            dma((24,)), dma((24,)),
            dma((X,)), dma((X,)),
            dma((TP,)), dma((TP,)),
            dma((4 * X,)), dma((4 * X,)),
            dma((24,)), dma((24,)),
            dma((Z,)), dma((Z,)),
            dma((Z,)), dma((Z,)),
        ],
        compiler_params=pltpu.CompilerParams(
            collective_id=0, has_side_effects=True, vmem_limit_bytes=60000 * 1024
        ),
        name="fused_backward",
    )(chosen.T, inputs, queries, key_vectors.T, value_rows_by_head.T, out_grad)
    dq, dk, dv, w = pl.pallas_call(
        copy_out,
        out_shape=tuple(jax.ShapeDtypeStruct(t.shape, t.dtype) for t in (dq, dk, dv, w)),
        in_specs=[vmem] * 4,
        out_specs=(vmem,) * 4,
        name="copy_out",
    )(dq, dk, dv, w)
    return dq, dk.T, dv.T, w


def solution(mesh):
    spec = P("kv", "tp")
    return jax.shard_map(
        body, mesh=mesh, in_specs=(spec,) * 5 + (P(),), out_specs=(spec,) * 4, check_vma=False
    )
```

```python
import functools

import jax
import jax.numpy as jnp
from jax import lax
from jax.experimental import pallas as pl
from jax.experimental.pallas import tpu as pltpu
from jax.sharding import PartitionSpec as P

HEAD = 64
QB = 128
KB = 64
NSEL = 16
Z, X, TP = 8, 4, 8
TOK = 256
SEQ = 8192
GROUP = 4
SCALE = HEAD**-0.5
ORDER = (0, 1, 7, 2, 6, 3, 5, 4)
PLACE = {d: p for p, d in enumerate(ORDER)}
NEG = -1e30
PARTS = 4
SIZE = 4 // PARTS
LEAVE = (7, 5, 6, 3, 4, 1, 2, 0)
MESH = pl.DeviceIdType.MESH
F32, BF16 = jnp.float32, jnp.bfloat16
ZERO_D = 2 * NSEL
T_FWD, T_SEND, T_OWN, T_LOC, T_BLK, T_ROWS = 0, 6, 18, 20, 21, 24


def place_of(distance):
    near = jnp.where(distance < 4, 2 * distance - 1, jnp.where(distance == 4, 7, 2 * (8 - distance)))
    return jnp.where(distance == 0, 0, near)


def fill_table(table, chosen_t, z, x):
    by_row = chosen_t[...]
    lane_r = lax.broadcasted_iota(jnp.int32, by_row.shape, 1)

    def column(d, e):
        row = z * 2 * X + 2 * lax.rem(x + d, X) + e
        return jnp.sum(jnp.where(lane_r == row, by_row, 0), axis=1, keepdims=True)

    cols = [[column(d, e) for e in range(2)] for d in range(X)]
    lane = lax.broadcasted_iota(jnp.int32, (1, 128), 1)
    sub = lax.broadcasted_iota(jnp.int32, (NSEL, 128), 0)

    def row_of_place(place):
        half = (place + 1) >> 1
        d = jnp.where((place & 1) == 1, half, Z - half)
        d = jnp.where(place == 7, 4, d)
        return (z + d) & 7

    def two_used(pair, base):
        low, high = 3, 0
        for col in pair:
            rel = col - base
            ok = (rel >= 0) & (rel < 4)
            low = jnp.minimum(low, jnp.min(jnp.where(ok, rel, 3), axis=0, keepdims=True))
            high = jnp.maximum(high, jnp.max(jnp.where(ok, rel, 0), axis=0, keepdims=True))
        return low, high

    def inverse(e, block):
        hit = cols[0][e] == block
        return jnp.min(jnp.where(hit, sub + NSEL * e, ZERO_D), axis=0, keepdims=True)

    at_place = row_of_place(lane & 7) * 16
    for d in range(1, X):
        low, high = two_used(cols[d], at_place + x * 4)
        n = (d - 1) * 2
        table[T_FWD + n : T_FWD + n + 1] = low
        table[T_FWD + n + 1 : T_FWD + n + 2] = high
        base = at_place + lax.rem(x + d, X) * 4
        for s, o in enumerate(two_used(cols[0], base)):
            for e in range(2):
                m = T_SEND + ((d - 1) * 2 + s) * 2 + e
                table[m : m + 1] = inverse(e, base + o)
    mine = row_of_place((lane >> 2) & 7) * 16 + x * 4 + (lane & 3)
    for e in range(2):
        table[T_OWN + e : T_OWN + e + 1] = inverse(e, mine)
    diag = sub == (lane & (NSEL - 1))
    flat = [jnp.sum(jnp.where(diag, cols[0][e], 0), axis=0, keepdims=True) for e in range(2)]
    block = jnp.where(lane < NSEL, flat[0], flat[1])
    owner, off = block >> 2, block & 3
    place = place_of(((owner >> 2) - z) & 7)
    dx = ((owner & 3) - x) & 3
    earlier = 0
    for e in range(2):
        same = ((cols[0][e] >> 2) == owner) & ((cols[0][e] & 3) < off)
        earlier = jnp.maximum(earlier, jnp.max(jnp.where(same, 1, 0), axis=0, keepdims=True))
    loc = jnp.where(dx == 0, place * 4 + off, 32 + ((dx - 1) * Z + place) * 2 + earlier)
    table[T_LOC : T_LOC + 1] = jnp.where(owner > z * X + x, 0, loc)
    table[T_BLK : T_BLK + 1] = block


def kernel(
    chosen_h, in_h, q_h, k_h, v_h, g_h,
    dq_out, dk_out, dv_out, w_out,
    chosen_t, in_ref, q_ref, k_ref, v_ref, g_ref, tab_v, tab, kvt, xsel, in_t, xt, at, kvs, kst, qg, sg_both, sp_scr,
    dsel, dxs, rbuf, acc, zs_send, zr_buf, dqg, wp, w_send, w_recv,
    t_sem, h_sem, z_ss, z_rs, x_ss, x_rs, i_ss, i_rs, y_ss, y_rs, dq_ss, dq_rs, dx_ss, dx_rs, w_ss, w_rs, dz_ss, dz_rs,
):
    kv, tp = lax.axis_index("kv"), lax.axis_index("tp")
    z, x = kv // X, lax.rem(kv, X)

    def row(p):
        return lax.rem(z + ORDER[p], Z)

    def at_z(p):
        return (row(p) * X + x, tp)

    def at_x(d):
        return (z * X + lax.rem(x + d, X), tp)

    def at_tp(d):
        return (kv, lax.rem(tp + d, TP))

    def remote(src, dst, ss, rs, dev):
        return pltpu.make_async_remote_copy(
            src_ref=src, dst_ref=dst, send_sem=ss, recv_sem=rs, device_id=dev, device_id_type=MESH
        )

    def opposite(p):
        return PLACE[(Z - ORDER[p]) % Z]

    def column(d):
        return lax.rem(x + d, X)

    with jax.named_scope("bar"):
        barrier = pltpu.get_barrier_semaphore()
        peers = [at_z(p) for p in range(1, Z)] + [at_x(d) for d in range(1, X)] + [at_tp(d) for d in range(1, TP)]
        for dev in peers:
            pl.semaphore_signal(barrier, inc=1, device_id=dev, device_id_type=MESH)
        loads = [(k_h, k_ref), (v_h, v_ref), (chosen_h, chosen_t), (in_h, in_ref), (q_h, q_ref), (g_h, g_ref)]
        loads = [pltpu.make_async_copy(src, dst, h_sem.at[n]) for n, (src, dst) in enumerate(loads)]
        for c in loads:
            c.start()
        for c in loads[:4]:
            c.wait()
        kvt[0:4] = jnp.concatenate([k_ref[...], v_ref[...]], axis=0).T.reshape(4, KB, 128)
        in_t[...] = in_ref[...].T.reshape(X, HEAD, TOK)
        fill_table(tab_v, chosen_t, z, x)
        dsel[ZERO_D] = jnp.zeros((KB, 128), F32)
        t_copy = pltpu.make_async_copy(tab_v, tab, t_sem)
        t_copy.start()
        xt[:, 0:TOK] = in_t[x]
        for c in loads[4:]:
            c.wait()
        pl.semaphore_wait(barrier, len(peers))

    def z_keys(hop, f, up):
        here = 0 if hop in (1, 4) else PLACE[Z + 1 - hop if up else hop - 1]
        there = PLACE[Z - hop if up else hop]
        n = PARTS * there + f
        step = 4 if hop == 4 else 1 if up else Z - 1
        to = (lax.rem(z + step, Z) * X + x, tp)
        return remote(
            kvt.at[pl.ds(4 * here + SIZE * f, SIZE)], kvt.at[pl.ds(4 * there + SIZE * f, SIZE)], z_ss.at[n], z_rs.at[n], to
        )

    def z_sends(hop, up):
        if hop == 4:
            return z < Z // 2
        if up:
            return (z >= hop - 1) & (z < Z - 1)
        return lax.rem(z + hop - 1, Z) <= Z - 6

    def z_gets(hop, up):
        if up:
            return z >= hop
        return lax.rem(z + hop, Z) <= Z - 6

    HOPS = [(hop, up) for hop in range(1, 5) for up in (True, False) if up or hop < 4]
    for f in range(PARTS):
        for up in (True, False):
            pl.when(z_sends(1, up))(z_keys(1, f, up).start)

    def x_inputs(d):
        return remote(
            in_t.at[column(d)], xt.at[:, pl.ds((X - d) * TOK, TOK)], i_ss.at[d], i_rs.at[X - d], at_x(d)
        )

    def tp_inputs(d):
        return remote(xt, at.at[tp], y_ss.at[d], y_rs.at[TP - d], at_tp(d))

    def x_keys(p, d):
        mine, there = ((d - 1) * Z + p) * 2, 32 + ((X - d - 1) * Z + p) * 2
        return remote(
            xsel.at[pl.ds(mine, 2)], kvt.at[pl.ds(there, 2)],
            x_ss.at[(d - 1) * Z + p], x_rs.at[(X - d - 1) * Z + p], at_x(d),
        )

    def x_keys_in(p, d):
        there = 32 + ((d - 1) * Z + p) * 2
        n = (d - 1) * Z + p
        return remote(xsel.at[pl.ds(2 * n, 2)], kvt.at[pl.ds(there, 2)], x_ss.at[n], x_rs.at[n], at_x(d))

    def forward(p):
        four = [kvt[4 * p + o] for o in range(4)]
        for d in range(1, X):
            for s in range(2):
                o = tab[T_FWD + (d - 1) * 2 + s, p]
                low = jnp.where(o == 0, four[0], four[1])
                high = jnp.where(o == 2, four[2], four[3])
                xsel[((d - 1) * Z + p) * 2 + s] = jnp.where(o < 2, low, high)
        for d in range(1, X):
            if p > 0:
                x_keys(p, d).start()
            else:
                pl.when(column(d) > x)(x_keys(p, d).start)

    with jax.named_scope("sel"):
        t_copy.wait()
        forward(0)
        for d in range(1, X):
            x_inputs(d).start()
        for hop in (1, 2, 4, 3):
            ways = [up for up in (True, False) if (hop, up) in HOPS]
            for f in range(PARTS):
                for up in ways:
                    @pl.when(z_gets(hop, up))
                    def _(f=f, up=up):
                        z_keys(hop, f, up).wait_recv()
                        if hop < 3:
                            pl.when(z_sends(hop + 1, up))(z_keys(hop + 1, f, up).start)

            if hop == 1:
                for f in range(PARTS):
                    pl.when(z_sends(4, True))(z_keys(4, f, True).start)
            for up in ways:
                p = PLACE[Z - hop if up else hop]
                pl.when(z_gets(hop, up) & (row(p) < z))(functools.partial(forward, p))
            if hop == 1:
                for d in range(1, X):
                    x_inputs(d).wait_recv()
                for d in range(1, TP):
                    tp_inputs(d).start()
                at[tp] = xt[...]
    with jax.named_scope("xwait"):
        for p in range(1, Z):
            @pl.when(row(p) < z)
            def _(p=p):
                for d in range(1, X):
                    x_keys_in(p, d).wait_recv()
        for d in range(1, X):
            pl.when(column(d) < x)(x_keys_in(0, d).wait_recv)

    lanes = 2 * QB
    lane_t = lax.broadcasted_iota(jnp.int32, (KB, lanes), 1) % QB
    diff = lax.broadcasted_iota(jnp.int32, (KB, lanes), 0) - lane_t
    zeros = jnp.zeros((QB, HEAD), BF16)
    nt = (((1,), (1,)), ((), ()))
    nn = (((1,), (0,)), ((), ()))

    def fold(t, op):
        return op(t.reshape(KB // 8, 8, lanes), axis=0)

    def x_dq(r, hp, d):
        cols = pl.ds(hp * 2 * HEAD, 2 * HEAD)
        n = (r * 2 + hp) * X
        return remote(
            dqg.at[pl.ds(r * QB, QB), cols], dqg.at[pl.ds((X - d) * TOK + r * QB, QB), cols],
            dq_ss.at[n + d], dq_rs.at[n + X - d], at_x(d),
        )

    units = [(r, hp) for r in range(2) for hp in range(2)]
    for r, hp in units:
        scope = jax.named_scope(f"attn{r}{hp}")
        scope.__enter__()
        rows = pl.ds(r * QB, QB)
        if hp == 0:
            for j in range(NSEL):
                kvs[j * KB : (j + 1) * KB, :] = kvt[tab[T_LOC, r * NSEL + j]]
            kst[...] = kvs[...].T[:HEAD]
        first = r * 8 * QB + hp * 4 * QB
        for h in range(2):
            cols = slice((hp * 2 + h) * HEAD, (hp * 2 + h + 1) * HEAD)
            qg[first + h * QB : first + (h + 1) * QB, :] = jnp.concatenate([q_ref[rows, cols], zeros], axis=1)
            qg[first + (h + 2) * QB : first + (h + 3) * QB, :] = jnp.concatenate([zeros, g_ref[rows, cols]], axis=1)
        sg_scr = sg_both.at[hp]
        sg_scr[...] = lax.dot_general(kvs[...], qg[first : first + 4 * QB], nt, preferred_element_type=F32)
        s_lanes, g_lanes = slice(0, lanes), slice(lanes, 2 * lanes)
        ds_lanes = slice(hp * 2 * lanes, hp * 2 * lanes + lanes)
        p_lanes = slice(hp * 2 * lanes + lanes, hp * 2 * lanes + 2 * lanes)

        def mask_step(j, m):
            at_j = pl.ds(pl.multiple_of(j * KB, KB), KB)
            limit = kv * TOK + r * QB - tab[T_BLK, r * NSEL + j] * KB
            s = jnp.where(diff <= limit, sg_scr[at_j, s_lanes] * SCALE, NEG)
            sg_scr[at_j, s_lanes] = s
            return jnp.maximum(m, fold(s, jnp.max))

        m = lax.fori_loop(0, NSEL, mask_step, jnp.full((8, lanes), NEG, F32), unroll=16)
        m = jnp.max(m, axis=0, keepdims=True)

        def exp_step(j, total):
            at_j = pl.ds(pl.multiple_of(j * KB, KB), KB)
            e = jnp.exp(sg_scr[at_j, s_lanes] - m)
            sg_scr[at_j, s_lanes] = e
            return total + fold(e, jnp.sum)

        total = lax.fori_loop(0, NSEL, exp_step, jnp.zeros((8, lanes), F32), unroll=16)
        inv = 1.0 / jnp.sum(total, axis=0, keepdims=True)

        def half_step(j, dot):
            at_j = pl.ds(pl.multiple_of(j * KB, KB), KB)
            half = (sg_scr[at_j, s_lanes] * inv).astype(BF16)
            sp_scr[r, at_j, p_lanes] = half
            return dot + fold(half.astype(F32) * sg_scr[at_j, g_lanes], jnp.sum)

        dot = lax.fori_loop(0, NSEL, half_step, jnp.zeros((8, lanes), F32), unroll=16)
        dot = jnp.sum(dot, axis=0, keepdims=True)

        def grad_step(j, carry):
            at_j = pl.ds(pl.multiple_of(j * KB, KB), KB)
            grad = (sg_scr[at_j, s_lanes] * inv) * (sg_scr[at_j, g_lanes] - dot)
            sp_scr[r, at_j, ds_lanes] = grad.astype(BF16)
            return carry

        lax.fori_loop(0, NSEL, grad_step, 0, unroll=16)
        dq_t = lax.dot_general(kst[...], sp_scr[r, :, ds_lanes], nn, preferred_element_type=F32) * SCALE
        stacked = jnp.concatenate([dq_t[:, :QB], dq_t[:, QB:]], axis=0)
        dqg[rows, hp * 2 * HEAD : (hp + 1) * 2 * HEAD] = stacked.T.astype(BF16)
        for d in range(1, X):
            x_dq(r, hp, d).start()
        scope.__exit__(None, None, None)
    with jax.named_scope("dkv"):
        for r in range(2):
            dkv = lax.dot_general(
                sp_scr[r], qg[r * 8 * QB : (r + 1) * 8 * QB], nn, preferred_element_type=F32
            )
            dsel[pl.ds(r * NSEL, NSEL)] = dkv.reshape(NSEL, KB, 128)
        dq_out[...] = dqg[0:TOK, :]

    def x_grads(p, d):
        mine, there = (d - 1) * Z + p, (X - d - 1) * Z + p
        return remote(
            dxs.at[pl.ds(2 * mine, 2)], rbuf.at[pl.ds(2 * there, 2)], dx_ss.at[mine], dx_rs.at[there], at_x(d)
        )

    def x_grads_in(p, d):
        mine = (d - 1) * Z + p
        return remote(
            dxs.at[pl.ds(2 * mine, 2)], rbuf.at[pl.ds(2 * mine, 2)], dx_ss.at[mine], dx_rs.at[mine], at_x(d)
        )

    with jax.named_scope("dxsend"):
        for p in LEAVE:
            @pl.when(row(p) <= z)
            def _(p=p):
                for d in range(1, X):
                    for s in range(2):
                        t = T_SEND + ((d - 1) * 2 + s) * 2
                        dxs[((d - 1) * Z + p) * 2 + s] = (dsel[tab[t, p]] + dsel[tab[t + 1, p]]).astype(BF16)
                for d in range(1, X):
                    if p > 0:
                        x_grads(p, d).start()
                    else:
                        pl.when(column(d) < x)(x_grads(p, d).start)

    def z_weight(p):
        there = opposite(p)
        return remote(w_send.at[row(p)], w_recv.at[there], w_ss.at[p], w_rs.at[there], at_z(p))

    with jax.named_scope("wgrad"):
        for d in range(1, TP):
            tp_inputs(d).wait_recv()
        for r, hp in units:
            for d in range(1, X):
                x_dq(r, hp, d).wait_recv()
        wp[...] = lax.dot_general(
            at[...].reshape(TP * HEAD, X * TOK), dqg[...], nn, preferred_element_type=F32
        ).reshape(TP, HEAD, TOK)
        w_send[...] = wp[...].astype(BF16)
        for p in reversed(range(1, Z)):
            if p >= 5:
                z_weight(p).start()
            else:
                pl.when(z < Z // 2)(z_weight(p).start)


    def z_copy(slot, step):
        return remote(
            zs_send.at[pl.ds(4 * slot, 4)], zr_buf.at[pl.ds(4 * slot, 4)], dz_ss.at[slot], dz_rs.at[slot],
            (lax.rem(z + step + Z, Z) * X + x, tp),
        )

    wraps = (z >= Z - 2) | (z == 0)
    returns = [
        (7, z >= 4, None, None, 0, -1),
        (5, z >= 5, None, None, 1, 1),
        (6, z >= 3, 0, (z >= 3) & (z <= 6), 2, -1),
        (3, wraps, 1, wraps, 3, 2),
        (4, z >= 2, 2, (z >= 2) & (z <= 6), 4, -2),
        (1, z == 7, None, None, 5, 1),
        (2, z >= 1, None, None, 6, -1),
    ]
    arrivals = [(3, z <= 2), (4, z <= 5), (5, z == 0), (6, z <= 6)]

    def relay(p, o):
        n = p * 4 + o
        term = dsel[tab[T_OWN, n]] + dsel[tab[T_OWN + 1, n]]
        for d in range(1, X):
            mine = (d - 1) * Z + p
            t = T_FWD + (d - 1) * 2
            first = tab[t, p] == o
            used = first | (tab[t + 1, p] == o)
            if p == 0:
                used = used & (column(d) > x)
            slot = jnp.where(first, rbuf[2 * mine], rbuf[2 * mine + 1]).astype(F32)
            term += jnp.where(used, slot, 0.0)
        return term

    with jax.named_scope("relay"):
        for p, sends, added, adds, slot, step in returns:
            @pl.when(sends)
            def _(p=p, added=added, adds=adds, slot=slot, step=step):
                @pl.when(row(p) < z)
                def _():
                    for d in range(1, X):
                        x_grads_in(p, d).wait_recv()

                if added is not None:
                    pl.when(adds)(z_copy(added, 0).wait_recv)
                for o in range(4):
                    term = jnp.where(row(p) < z, relay(p, o), 0.0)
                    if added is not None:
                        term += jnp.where(adds, zr_buf[added * 4 + o].astype(F32), 0.0)
                    zs_send[slot * 4 + o] = term.astype(BF16)
                z_copy(slot, step).start()

            if slot < 4:
                pl.when(z >= Z // 2)(z_weight(4 - slot).start)

        for d in range(1, X):
            pl.when(column(d) > x)(x_grads_in(0, d).wait_recv)
        for o in range(4):
            acc[o] = relay(0, o)
    with jax.named_scope("wfin"):
        w = wp[z]
        for p in range(1, Z):
            z_weight(p).wait_recv()
        for p in range(1, Z):
            w += w_recv[p].astype(F32)
        w_out[...] = w
    with jax.named_scope("dzwait"):
        for slot, comes in arrivals:
            @pl.when(comes)
            def _(slot=slot):
                z_copy(slot, 0).wait_recv()
                acc[...] += zr_buf[4 * slot : 4 * slot + 4].astype(F32)
        both = acc[...].reshape(TOK, 128).T
        dk_out[...] = (both[:HEAD] * SCALE).astype(BF16)
        dv_out[...] = both[HEAD:].astype(BF16)
    with jax.named_scope("sentwait"):
        for hop, up in HOPS:
            for f in range(PARTS):
                pl.when(z_sends(hop, up))(z_keys(hop, f, up).wait_send)
        for p in range(1, Z):
            z_weight(p).wait_send()
            @pl.when(row(p) < z)
            def _(p=p):
                for d in range(1, X):
                    x_keys(p, d).wait_send()
                    x_grads(p, d).wait_send()
        for d in range(1, X):
            pl.when(column(d) > x)(x_keys(0, d).wait_send)
            pl.when(column(d) < x)(x_grads(0, d).wait_send)
            x_inputs(d).wait_send()
            for r, hp in units:
                x_dq(r, hp, d).wait_send()
        for d in range(1, TP):
            tp_inputs(d).wait_send()
        for p, sends, added, adds, slot, step in returns:
            pl.when(sends)(z_copy(slot, step).wait_send)


def copy_out(*refs):
    for src, dst in zip(refs[:4], refs[4:]):
        dst[...] = src[...]


def body(inputs, queries, key_vectors, value_rows_by_head, out_grad, chosen):
    dma = pltpu.SemaphoreType.DMA
    vmem = pl.BlockSpec(memory_space=pltpu.VMEM)
    dq, dk, dv, w = pl.pallas_call(
        kernel,
        out_shape=(
            pltpu.VMEM((TOK, GROUP * HEAD), BF16),
            pltpu.VMEM((HEAD, TOK), BF16),
            pltpu.VMEM((HEAD, TOK), BF16),
            pltpu.VMEM((HEAD, GROUP * HEAD), F32),
        ),
        in_specs=[pl.BlockSpec(memory_space=pl.ANY)] * 6,
        out_specs=(vmem,) * 4,
        scratch_shapes=[
            pltpu.VMEM((NSEL, SEQ // QB), jnp.int32),
            pltpu.VMEM((TOK, TOK), BF16),
            pltpu.VMEM((TOK, GROUP * HEAD), BF16),
            pltpu.VMEM((HEAD, TOK), BF16),
            pltpu.VMEM((HEAD, TOK), BF16),
            pltpu.VMEM((TOK, GROUP * HEAD), BF16),
            pltpu.VMEM((T_ROWS, 128), jnp.int32),
            pltpu.SMEM((T_ROWS, 128), jnp.int32),
            pltpu.VMEM((32 + 48, KB, 128), BF16),
            pltpu.VMEM((48, KB, 128), BF16),
            pltpu.VMEM((X, HEAD, TOK), BF16),
            pltpu.VMEM((HEAD, X * TOK), BF16),
            pltpu.VMEM((TP, HEAD, X * TOK), BF16),
            pltpu.VMEM((NSEL * KB, 128), BF16),
            pltpu.VMEM((HEAD, NSEL * KB), BF16),
            pltpu.VMEM((16 * QB, 128), BF16),
            pltpu.VMEM((2, NSEL * KB, 4 * QB), F32),
            pltpu.VMEM((2, NSEL * KB, 8 * QB), BF16),
            pltpu.VMEM((2 * NSEL + 1, KB, 128), F32),
            pltpu.VMEM((48, KB, 128), BF16),
            pltpu.VMEM((48, KB, 128), BF16),
            pltpu.VMEM((4, KB, 128), F32),
            pltpu.VMEM((28, KB, 128), BF16),
            pltpu.VMEM((28, KB, 128), BF16),
            pltpu.VMEM((X * TOK, GROUP * HEAD), BF16),
            pltpu.VMEM((TP, HEAD, TOK), F32),
            pltpu.VMEM((TP, HEAD, TOK), BF16),
            pltpu.VMEM((Z, HEAD, TOK), BF16),
            dma,
            dma((6,)),
            dma((PARTS * Z,)), dma((PARTS * Z,)),
            dma((24,)), dma((24,)),
            dma((X,)), dma((X,)),
            dma((TP,)), dma((TP,)),
            dma((4 * X,)), dma((4 * X,)),
            dma((24,)), dma((24,)),
            dma((Z,)), dma((Z,)),
            dma((Z,)), dma((Z,)),
        ],
        compiler_params=pltpu.CompilerParams(
            collective_id=0, has_side_effects=True, vmem_limit_bytes=60000 * 1024
        ),
        name="fused_backward",
    )(chosen.T, inputs, queries, key_vectors.T, value_rows_by_head.T, out_grad)
    dq, dk, dv, w = pl.pallas_call(
        copy_out,
        out_shape=tuple(jax.ShapeDtypeStruct(t.shape, t.dtype) for t in (dq, dk, dv, w)),
        in_specs=[vmem] * 4,
        out_specs=(vmem,) * 4,
        name="copy_out",
    )(*[pltpu.with_memory_space_constraint(t, pltpu.VMEM) for t in (dq, dk, dv, w)])
    return dq, dk.T, dv.T, w


def solution(mesh):
    spec = P("kv", "tp")
    return jax.shard_map(
        body, mesh=mesh, in_specs=(spec,) * 5 + (P(),), out_specs=(spec,) * 4, check_vma=False
    )
```

```python
import functools

import jax
import jax.numpy as jnp
from jax import lax
from jax.experimental import pallas as pl
from jax.experimental.pallas import tpu as pltpu
from jax.sharding import PartitionSpec as P

HEAD = 64
QB = 128
KB = 64
NSEL = 16
Z, X, TP = 8, 4, 8
TOK = 256
SEQ = 8192
GROUP = 4
SCALE = HEAD**-0.5
ORDER = (0, 1, 7, 2, 6, 3, 5, 4)
PLACE = {d: p for p, d in enumerate(ORDER)}
NEG = -1e30
PARTS = 4
SIZE = 4 // PARTS
LEAVE = (7, 5, 6, 3, 4, 1, 2, 0)
MESH = pl.DeviceIdType.MESH
F32, BF16 = jnp.float32, jnp.bfloat16
ZERO_D = 2 * NSEL
T_FWD, T_SEND, T_OWN, T_LOC, T_BLK, T_ROWS = 0, 6, 18, 20, 21, 24


def place_of(distance):
    near = jnp.where(distance < 4, 2 * distance - 1, jnp.where(distance == 4, 7, 2 * (8 - distance)))
    return jnp.where(distance == 0, 0, near)


def fill_table(table, chosen_t, z, x):
    by_row = chosen_t[...]
    lane_r = lax.broadcasted_iota(jnp.int32, by_row.shape, 1)

    def column(d, e):
        row = z * 2 * X + 2 * lax.rem(x + d, X) + e
        return jnp.sum(jnp.where(lane_r == row, by_row, 0), axis=1, keepdims=True)

    cols = [[column(d, e) for e in range(2)] for d in range(X)]
    lane = lax.broadcasted_iota(jnp.int32, (1, 128), 1)
    sub = lax.broadcasted_iota(jnp.int32, (NSEL, 128), 0)

    def row_of_place(place):
        half = (place + 1) >> 1
        d = jnp.where((place & 1) == 1, half, Z - half)
        d = jnp.where(place == 7, 4, d)
        return (z + d) & 7

    def two_used(pair, base):
        low, high = 3, 0
        for col in pair:
            rel = col - base
            ok = (rel >= 0) & (rel < 4)
            low = jnp.minimum(low, jnp.min(jnp.where(ok, rel, 3), axis=0, keepdims=True))
            high = jnp.maximum(high, jnp.max(jnp.where(ok, rel, 0), axis=0, keepdims=True))
        return low, high

    def inverse(e, block):
        hit = cols[0][e] == block
        return jnp.min(jnp.where(hit, sub + NSEL * e, ZERO_D), axis=0, keepdims=True)

    at_place = row_of_place(lane & 7) * 16
    for d in range(1, X):
        low, high = two_used(cols[d], at_place + x * 4)
        n = (d - 1) * 2
        table[T_FWD + n : T_FWD + n + 1] = low
        table[T_FWD + n + 1 : T_FWD + n + 2] = high
        base = at_place + lax.rem(x + d, X) * 4
        for s, o in enumerate(two_used(cols[0], base)):
            for e in range(2):
                m = T_SEND + ((d - 1) * 2 + s) * 2 + e
                table[m : m + 1] = inverse(e, base + o)
    mine = row_of_place((lane >> 2) & 7) * 16 + x * 4 + (lane & 3)
    for e in range(2):
        table[T_OWN + e : T_OWN + e + 1] = inverse(e, mine)
    diag = sub == (lane & (NSEL - 1))
    flat = [jnp.sum(jnp.where(diag, cols[0][e], 0), axis=0, keepdims=True) for e in range(2)]
    block = jnp.where(lane < NSEL, flat[0], flat[1])
    owner, off = block >> 2, block & 3
    place = place_of(((owner >> 2) - z) & 7)
    dx = ((owner & 3) - x) & 3
    earlier = 0
    for e in range(2):
        same = ((cols[0][e] >> 2) == owner) & ((cols[0][e] & 3) < off)
        earlier = jnp.maximum(earlier, jnp.max(jnp.where(same, 1, 0), axis=0, keepdims=True))
    loc = jnp.where(dx == 0, place * 4 + off, 32 + ((dx - 1) * Z + place) * 2 + earlier)
    table[T_LOC : T_LOC + 1] = jnp.where(owner > z * X + x, 0, loc)
    table[T_BLK : T_BLK + 1] = block


def kernel(
    chosen_h, in_h, q_h, k_h, v_h, g_h,
    dq_out, dk_out, dv_out, w_out,
    chosen_t, in_ref, q_ref, k_ref, v_ref, g_ref, tab_v, tab, kvt, xsel, in_t, xt, at, kvs, kst, qg, sg_both, sp_scr,
    dsel, dxs, rbuf, acc, zs_send, zr_buf, dqg, wp, w_send, w_recv,
    t_sem, h_sem, z_ss, z_rs, x_ss, x_rs, i_ss, i_rs, y_ss, y_rs, dq_ss, dq_rs, dx_ss, dx_rs, w_ss, w_rs, dz_ss, dz_rs,
):
    kv, tp = lax.axis_index("kv"), lax.axis_index("tp")
    z, x = kv // X, lax.rem(kv, X)

    def row(p):
        return lax.rem(z + ORDER[p], Z)

    def at_z(p):
        return (row(p) * X + x, tp)

    def at_x(d):
        return (z * X + lax.rem(x + d, X), tp)

    def at_tp(d):
        return (kv, lax.rem(tp + d, TP))

    def remote(src, dst, ss, rs, dev):
        return pltpu.make_async_remote_copy(
            src_ref=src, dst_ref=dst, send_sem=ss, recv_sem=rs, device_id=dev, device_id_type=MESH
        )

    def opposite(p):
        return PLACE[(Z - ORDER[p]) % Z]

    def column(d):
        return lax.rem(x + d, X)

    with jax.named_scope("bar"):
        barrier = pltpu.get_barrier_semaphore()
        peers = [at_z(p) for p in range(1, Z)] + [at_x(d) for d in range(1, X)] + [at_tp(d) for d in range(1, TP)]
        for dev in peers:
            pl.semaphore_signal(barrier, inc=1, device_id=dev, device_id_type=MESH)
        loads = [(k_h, k_ref), (v_h, v_ref), (chosen_h, chosen_t), (in_h, in_ref), (q_h, q_ref), (g_h, g_ref)]
        loads = [pltpu.make_async_copy(src, dst, h_sem.at[n]) for n, (src, dst) in enumerate(loads)]
        for c in loads:
            c.start()
        for c in loads[:4]:
            c.wait()
        kvt[0:4] = jnp.concatenate([k_ref[...], v_ref[...]], axis=0).T.reshape(4, KB, 128)
        in_t[...] = in_ref[...].T.reshape(X, HEAD, TOK)
        fill_table(tab_v, chosen_t, z, x)
        dsel[ZERO_D] = jnp.zeros((KB, 128), F32)
        t_copy = pltpu.make_async_copy(tab_v, tab, t_sem)
        t_copy.start()
        xt[:, 0:TOK] = in_t[x]
        for c in loads[4:]:
            c.wait()
        pl.semaphore_wait(barrier, len(peers))

    def z_keys(hop, f, up):
        here = 0 if hop in (1, 4) else PLACE[Z + 1 - hop if up else hop - 1]
        there = PLACE[Z - hop if up else hop]
        n = PARTS * there + f
        step = 4 if hop == 4 else 1 if up else Z - 1
        to = (lax.rem(z + step, Z) * X + x, tp)
        return remote(
            kvt.at[pl.ds(4 * here + SIZE * f, SIZE)], kvt.at[pl.ds(4 * there + SIZE * f, SIZE)], z_ss.at[n], z_rs.at[n], to
        )

    def z_sends(hop, up):
        if hop == 4:
            return z < Z // 2
        if up:
            return (z >= hop - 1) & (z < Z - 1)
        return lax.rem(z + hop - 1, Z) <= Z - 6

    def z_gets(hop, up):
        if up:
            return z >= hop
        return lax.rem(z + hop, Z) <= Z - 6

    HOPS = [(hop, up) for hop in range(1, 5) for up in (True, False) if up or hop < 4]
    for f in range(PARTS):
        for up in (True, False):
            pl.when(z_sends(1, up))(z_keys(1, f, up).start)

    def x_inputs(d):
        return remote(
            in_t.at[column(d)], xt.at[:, pl.ds((X - d) * TOK, TOK)], i_ss.at[d], i_rs.at[X - d], at_x(d)
        )

    def tp_inputs(d):
        return remote(xt, at.at[tp], y_ss.at[d], y_rs.at[TP - d], at_tp(d))

    def x_keys(p, d):
        mine, there = ((d - 1) * Z + p) * 2, 32 + ((X - d - 1) * Z + p) * 2
        return remote(
            xsel.at[pl.ds(mine, 2)], kvt.at[pl.ds(there, 2)],
            x_ss.at[(d - 1) * Z + p], x_rs.at[(X - d - 1) * Z + p], at_x(d),
        )

    def x_keys_in(p, d):
        there = 32 + ((d - 1) * Z + p) * 2
        n = (d - 1) * Z + p
        return remote(xsel.at[pl.ds(2 * n, 2)], kvt.at[pl.ds(there, 2)], x_ss.at[n], x_rs.at[n], at_x(d))

    def forward(p):
        four = [kvt[4 * p + o] for o in range(4)]
        for d in range(1, X):
            for s in range(2):
                o = tab[T_FWD + (d - 1) * 2 + s, p]
                low = jnp.where(o == 0, four[0], four[1])
                high = jnp.where(o == 2, four[2], four[3])
                xsel[((d - 1) * Z + p) * 2 + s] = jnp.where(o < 2, low, high)
        for d in range(1, X):
            if p > 0:
                x_keys(p, d).start()
            else:
                pl.when(column(d) > x)(x_keys(p, d).start)

    with jax.named_scope("sel"):
        t_copy.wait()
        forward(0)
        for d in range(1, X):
            x_inputs(d).start()
        for hop in (1, 2, 4, 3):
            ways = [up for up in (True, False) if (hop, up) in HOPS]
            for f in range(PARTS):
                for up in ways:
                    @pl.when(z_gets(hop, up))
                    def _(f=f, up=up):
                        z_keys(hop, f, up).wait_recv()
                        if hop < 3:
                            pl.when(z_sends(hop + 1, up))(z_keys(hop + 1, f, up).start)

            if hop == 1:
                for f in range(PARTS):
                    pl.when(z_sends(4, True))(z_keys(4, f, True).start)
            for up in ways:
                p = PLACE[Z - hop if up else hop]
                pl.when(z_gets(hop, up) & (row(p) < z))(functools.partial(forward, p))
            if hop == 1:
                for d in range(1, X):
                    x_inputs(d).wait_recv()
                for d in range(1, TP):
                    tp_inputs(d).start()
                at[tp] = xt[...]
    with jax.named_scope("xwait"):
        for p in range(1, Z):
            @pl.when(row(p) < z)
            def _(p=p):
                for d in range(1, X):
                    x_keys_in(p, d).wait_recv()
        for d in range(1, X):
            pl.when(column(d) < x)(x_keys_in(0, d).wait_recv)

    lanes = 2 * QB
    lane_t = lax.broadcasted_iota(jnp.int32, (KB, lanes), 1) % QB
    diff = lax.broadcasted_iota(jnp.int32, (KB, lanes), 0) - lane_t
    zeros = jnp.zeros((QB, HEAD), BF16)
    nt = (((1,), (1,)), ((), ()))
    nn = (((1,), (0,)), ((), ()))

    def fold(t, op):
        return op(t.reshape(KB // 8, 8, lanes), axis=0)

    def x_dq(r, hp, d):
        cols = pl.ds(hp * 2 * HEAD, 2 * HEAD)
        n = (r * 2 + hp) * X
        return remote(
            dqg.at[pl.ds(r * QB, QB), cols], dqg.at[pl.ds((X - d) * TOK + r * QB, QB), cols],
            dq_ss.at[n + d], dq_rs.at[n + X - d], at_x(d),
        )

    def key_terms(r):
        dkv = lax.dot_general(sp_scr[r], qg[r * 8 * QB : (r + 1) * 8 * QB], nn, preferred_element_type=F32)
        dsel[pl.ds(r * NSEL, NSEL)] = dkv.reshape(NSEL, KB, 128)

    units = [(r, hp) for r in range(2) for hp in range(2)]
    for r, hp in units:
        scope = jax.named_scope(f"attn{r}{hp}")
        scope.__enter__()
        rows = pl.ds(r * QB, QB)
        if hp == 0:
            for j in range(NSEL):
                kvs[j * KB : (j + 1) * KB, :] = kvt[tab[T_LOC, r * NSEL + j]]
            kst[...] = kvs[...].T[:HEAD]
        first = r * 8 * QB + hp * 4 * QB
        for h in range(2):
            cols = slice((hp * 2 + h) * HEAD, (hp * 2 + h + 1) * HEAD)
            qg[first + h * QB : first + (h + 1) * QB, :] = jnp.concatenate([q_ref[rows, cols], zeros], axis=1)
            qg[first + (h + 2) * QB : first + (h + 3) * QB, :] = jnp.concatenate([zeros, g_ref[rows, cols]], axis=1)
        sg_scr = sg_both.at[hp]
        sg_scr[...] = lax.dot_general(kvs[...], qg[first : first + 4 * QB], nt, preferred_element_type=F32)
        if (r, hp) == (1, 1):
            key_terms(0)
        s_lanes, g_lanes = slice(0, lanes), slice(lanes, 2 * lanes)
        ds_lanes = slice(hp * 2 * lanes, hp * 2 * lanes + lanes)
        p_lanes = slice(hp * 2 * lanes + lanes, hp * 2 * lanes + 2 * lanes)

        def mask_step(j, m):
            at_j = pl.ds(pl.multiple_of(j * KB, KB), KB)
            limit = kv * TOK + r * QB - tab[T_BLK, r * NSEL + j] * KB
            s = jnp.where(diff <= limit, sg_scr[at_j, s_lanes] * SCALE, NEG)
            sg_scr[at_j, s_lanes] = s
            return jnp.maximum(m, fold(s, jnp.max))

        m = lax.fori_loop(0, NSEL, mask_step, jnp.full((8, lanes), NEG, F32), unroll=16)
        m = jnp.max(m, axis=0, keepdims=True)

        def exp_step(j, total):
            at_j = pl.ds(pl.multiple_of(j * KB, KB), KB)
            e = jnp.exp(sg_scr[at_j, s_lanes] - m)
            sg_scr[at_j, s_lanes] = e
            return total + fold(e, jnp.sum)

        total = lax.fori_loop(0, NSEL, exp_step, jnp.zeros((8, lanes), F32), unroll=16)
        inv = 1.0 / jnp.sum(total, axis=0, keepdims=True)

        def half_step(j, dot):
            at_j = pl.ds(pl.multiple_of(j * KB, KB), KB)
            half = (sg_scr[at_j, s_lanes] * inv).astype(BF16)
            sp_scr[r, at_j, p_lanes] = half
            return dot + fold(half.astype(F32) * sg_scr[at_j, g_lanes], jnp.sum)

        dot = lax.fori_loop(0, NSEL, half_step, jnp.zeros((8, lanes), F32), unroll=16)
        dot = jnp.sum(dot, axis=0, keepdims=True)

        def grad_step(j, carry):
            at_j = pl.ds(pl.multiple_of(j * KB, KB), KB)
            grad = (sg_scr[at_j, s_lanes] * inv) * (sg_scr[at_j, g_lanes] - dot)
            sp_scr[r, at_j, ds_lanes] = grad.astype(BF16)
            return carry

        lax.fori_loop(0, NSEL, grad_step, 0, unroll=16)
        dq_t = lax.dot_general(kst[...], sp_scr[r, :, ds_lanes], nn, preferred_element_type=F32) * SCALE
        stacked = jnp.concatenate([dq_t[:, :QB], dq_t[:, QB:]], axis=0)
        dqg[rows, hp * 2 * HEAD : (hp + 1) * 2 * HEAD] = stacked.T.astype(BF16)
        for d in range(1, X):
            x_dq(r, hp, d).start()
        scope.__exit__(None, None, None)
    with jax.named_scope("dkv"):
        key_terms(1)
        dq_out[...] = dqg[0:TOK, :]

    def x_grads(p, d):
        mine, there = (d - 1) * Z + p, (X - d - 1) * Z + p
        return remote(
            dxs.at[pl.ds(2 * mine, 2)], rbuf.at[pl.ds(2 * there, 2)], dx_ss.at[mine], dx_rs.at[there], at_x(d)
        )

    def x_grads_in(p, d):
        mine = (d - 1) * Z + p
        return remote(
            dxs.at[pl.ds(2 * mine, 2)], rbuf.at[pl.ds(2 * mine, 2)], dx_ss.at[mine], dx_rs.at[mine], at_x(d)
        )

    with jax.named_scope("dxsend"):
        for p in LEAVE:
            @pl.when(row(p) <= z)
            def _(p=p):
                for d in range(1, X):
                    for s in range(2):
                        t = T_SEND + ((d - 1) * 2 + s) * 2
                        dxs[((d - 1) * Z + p) * 2 + s] = (dsel[tab[t, p]] + dsel[tab[t + 1, p]]).astype(BF16)
                for d in range(1, X):
                    if p > 0:
                        x_grads(p, d).start()
                    else:
                        pl.when(column(d) < x)(x_grads(p, d).start)

    def z_weight(p):
        there = opposite(p)
        return remote(w_send.at[row(p)], w_recv.at[there], w_ss.at[p], w_rs.at[there], at_z(p))

    with jax.named_scope("wgrad"):
        for d in range(1, TP):
            tp_inputs(d).wait_recv()
        for r, hp in units:
            for d in range(1, X):
                x_dq(r, hp, d).wait_recv()
        wp[...] = lax.dot_general(
            at[...].reshape(TP * HEAD, X * TOK), dqg[...], nn, preferred_element_type=F32
        ).reshape(TP, HEAD, TOK)
        w_send[...] = wp[...].astype(BF16)
        for p in reversed(range(1, Z)):
            if p >= 5:
                z_weight(p).start()
            else:
                pl.when(z < Z // 2)(z_weight(p).start)


    def z_copy(slot, step):
        return remote(
            zs_send.at[pl.ds(4 * slot, 4)], zr_buf.at[pl.ds(4 * slot, 4)], dz_ss.at[slot], dz_rs.at[slot],
            (lax.rem(z + step + Z, Z) * X + x, tp),
        )

    wraps = (z >= Z - 2) | (z == 0)
    returns = [
        (7, z >= 4, None, None, 0, -1),
        (5, z >= 5, None, None, 1, 1),
        (6, z >= 3, 0, (z >= 3) & (z <= 6), 2, -1),
        (3, wraps, 1, wraps, 3, 2),
        (4, z >= 2, 2, (z >= 2) & (z <= 6), 4, -2),
        (1, z == 7, None, None, 5, 1),
        (2, z >= 1, None, None, 6, -1),
    ]
    arrivals = [(3, z <= 2), (4, z <= 5), (5, z == 0), (6, z <= 6)]

    def relay(p, o):
        n = p * 4 + o
        term = dsel[tab[T_OWN, n]] + dsel[tab[T_OWN + 1, n]]
        for d in range(1, X):
            mine = (d - 1) * Z + p
            t = T_FWD + (d - 1) * 2
            first = tab[t, p] == o
            used = first | (tab[t + 1, p] == o)
            if p == 0:
                used = used & (column(d) > x)
            slot = jnp.where(first, rbuf[2 * mine], rbuf[2 * mine + 1]).astype(F32)
            term += jnp.where(used, slot, 0.0)
        return term

    with jax.named_scope("relay"):
        for p, sends, added, adds, slot, step in returns:
            @pl.when(sends)
            def _(p=p, added=added, adds=adds, slot=slot, step=step):
                @pl.when(row(p) < z)
                def _():
                    for d in range(1, X):
                        x_grads_in(p, d).wait_recv()

                if added is not None:
                    pl.when(adds)(z_copy(added, 0).wait_recv)
                for o in range(4):
                    term = jnp.where(row(p) < z, relay(p, o), 0.0)
                    if added is not None:
                        term += jnp.where(adds, zr_buf[added * 4 + o].astype(F32), 0.0)
                    zs_send[slot * 4 + o] = term.astype(BF16)
                z_copy(slot, step).start()

            if slot < 4:
                pl.when(z >= Z // 2)(z_weight(4 - slot).start)

        for d in range(1, X):
            pl.when(column(d) > x)(x_grads_in(0, d).wait_recv)
        for o in range(4):
            acc[o] = relay(0, o)
    with jax.named_scope("wfin"):
        w = wp[z]
        for p in range(1, Z):
            z_weight(p).wait_recv()
        for p in range(1, Z):
            w += w_recv[p].astype(F32)
        w_out[...] = w
    with jax.named_scope("dzwait"):
        for slot, comes in arrivals:
            @pl.when(comes)
            def _(slot=slot):
                z_copy(slot, 0).wait_recv()
                acc[...] += zr_buf[4 * slot : 4 * slot + 4].astype(F32)
        both = acc[...].reshape(TOK, 128).T
        dk_out[...] = (both[:HEAD] * SCALE).astype(BF16)
        dv_out[...] = both[HEAD:].astype(BF16)
    with jax.named_scope("sentwait"):
        for hop, up in HOPS:
            for f in range(PARTS):
                pl.when(z_sends(hop, up))(z_keys(hop, f, up).wait_send)
        for p in range(1, Z):
            z_weight(p).wait_send()
            @pl.when(row(p) < z)
            def _(p=p):
                for d in range(1, X):
                    x_keys(p, d).wait_send()
                    x_grads(p, d).wait_send()
        for d in range(1, X):
            pl.when(column(d) > x)(x_keys(0, d).wait_send)
            pl.when(column(d) < x)(x_grads(0, d).wait_send)
            x_inputs(d).wait_send()
            for r, hp in units:
                x_dq(r, hp, d).wait_send()
        for d in range(1, TP):
            tp_inputs(d).wait_send()
        for p, sends, added, adds, slot, step in returns:
            pl.when(sends)(z_copy(slot, step).wait_send)


def copy_out(*refs):
    for src, dst in zip(refs[:4], refs[4:]):
        dst[...] = src[...]


def body(inputs, queries, key_vectors, value_rows_by_head, out_grad, chosen):
    dma = pltpu.SemaphoreType.DMA
    vmem = pl.BlockSpec(memory_space=pltpu.VMEM)
    dq, dk, dv, w = pl.pallas_call(
        kernel,
        out_shape=(
            pltpu.VMEM((TOK, GROUP * HEAD), BF16),
            pltpu.VMEM((HEAD, TOK), BF16),
            pltpu.VMEM((HEAD, TOK), BF16),
            pltpu.VMEM((HEAD, GROUP * HEAD), F32),
        ),
        in_specs=[pl.BlockSpec(memory_space=pl.ANY)] * 6,
        out_specs=(vmem,) * 4,
        scratch_shapes=[
            pltpu.VMEM((NSEL, SEQ // QB), jnp.int32),
            pltpu.VMEM((TOK, TOK), BF16),
            pltpu.VMEM((TOK, GROUP * HEAD), BF16),
            pltpu.VMEM((HEAD, TOK), BF16),
            pltpu.VMEM((HEAD, TOK), BF16),
            pltpu.VMEM((TOK, GROUP * HEAD), BF16),
            pltpu.VMEM((T_ROWS, 128), jnp.int32),
            pltpu.SMEM((T_ROWS, 128), jnp.int32),
            pltpu.VMEM((32 + 48, KB, 128), BF16),
            pltpu.VMEM((48, KB, 128), BF16),
            pltpu.VMEM((X, HEAD, TOK), BF16),
            pltpu.VMEM((HEAD, X * TOK), BF16),
            pltpu.VMEM((TP, HEAD, X * TOK), BF16),
            pltpu.VMEM((NSEL * KB, 128), BF16),
            pltpu.VMEM((HEAD, NSEL * KB), BF16),
            pltpu.VMEM((16 * QB, 128), BF16),
            pltpu.VMEM((2, NSEL * KB, 4 * QB), F32),
            pltpu.VMEM((2, NSEL * KB, 8 * QB), BF16),
            pltpu.VMEM((2 * NSEL + 1, KB, 128), F32),
            pltpu.VMEM((48, KB, 128), BF16),
            pltpu.VMEM((48, KB, 128), BF16),
            pltpu.VMEM((4, KB, 128), F32),
            pltpu.VMEM((28, KB, 128), BF16),
            pltpu.VMEM((28, KB, 128), BF16),
            pltpu.VMEM((X * TOK, GROUP * HEAD), BF16),
            pltpu.VMEM((TP, HEAD, TOK), F32),
            pltpu.VMEM((TP, HEAD, TOK), BF16),
            pltpu.VMEM((Z, HEAD, TOK), BF16),
            dma,
            dma((6,)),
            dma((PARTS * Z,)), dma((PARTS * Z,)),
            dma((24,)), dma((24,)),
            dma((X,)), dma((X,)),
            dma((TP,)), dma((TP,)),
            dma((4 * X,)), dma((4 * X,)),
            dma((24,)), dma((24,)),
            dma((Z,)), dma((Z,)),
            dma((Z,)), dma((Z,)),
        ],
        compiler_params=pltpu.CompilerParams(
            collective_id=0, has_side_effects=True, vmem_limit_bytes=60000 * 1024
        ),
        name="fused_backward",
    )(chosen.T, inputs, queries, key_vectors.T, value_rows_by_head.T, out_grad)
    dq, dk, dv, w = pl.pallas_call(
        copy_out,
        out_shape=tuple(jax.ShapeDtypeStruct(t.shape, t.dtype) for t in (dq, dk, dv, w)),
        in_specs=[vmem] * 4,
        out_specs=(vmem,) * 4,
        name="copy_out",
    )(*[pltpu.with_memory_space_constraint(t, pltpu.VMEM) for t in (dq, dk, dv, w)])
    return dq, dk.T, dv.T, w


def solution(mesh):
    spec = P("kv", "tp")
    return jax.shard_map(
        body, mesh=mesh, in_specs=(spec,) * 5 + (P(),), out_specs=(spec,) * 4, check_vma=False
    )
```
